32 devices in a mesh: ep: 8 (over z, core), tp: 4 (over y, x).
Axes of the slice: x: 2, y: 2, z: 4, core: 2. Of those that a mesh axis runs over, the one named last changes fastest.
Arguments:
- tokens: bfloat16 [128, 2048], P('ep'), may hold values from -6 to 6
- mix_gain: float32 [2048], replicated, may hold values from 0.1 to 1.9
- gate_weight: bfloat16 [2048, 1024], P('ep', 'tp'), may hold values from -0.125 to 0.125
- inner_weight: bfloat16 [2048, 1024], P('ep', 'tp'), may hold values from -0.125 to 0.125
- write_weight: bfloat16 [2048, 512], P('ep'), may hold values from -0.125 to 0.125
- read_weight: bfloat16 [2048, 512], P('ep'), may hold values from -0.125 to 0.125
- step_weight: bfloat16 [2048, 16], P('ep'), may hold values from -0.125 to 0.125
- step_bias: float32 [16], replicated, may hold values from -2 to 1
- decay_log: float32 [16], replicated, may hold values from -1 to 1.5
- skip_scale: float32 [16], replicated, may hold values from 0.5 to 2
- inner_taps: bfloat16 [4, 1024], P(None, 'tp'), may hold values from -3 to 3
- access_taps: bfloat16 [2, 4, 512], replicated, may hold values from -3 to 3
- inner_history: bfloat16 [128, 3, 1024], P('ep', None, 'tp'), may hold values from -6 to 6
- access_history: bfloat16 [128, 2, 3, 512], P('ep'), may hold values from -6 to 6
- recurrent: float32 [128, 16, 64, 128], P('ep', 'tp'), may hold values from -3 to 3
- head_gain: float32 [1024], P('tp'), may hold values from 0.1 to 1.9
- mixer_out: bfloat16 [1024, 2048], P('tp'), may hold values from -0.1875 to 0.1875
- moe_gain: float32 [2048], replicated, may hold values from 0.1 to 1.9
- expert_ids: int32 [128, 2], P('ep'), may hold values from 0 to 7, all different within a row; in each aligned block of 16 rows (0 to 15, 16 to 31, ...) at most 8 rows name the same one
- route_scores: float32 [128, 2], P('ep'), may hold values from -6 to 6
- expert_gate: bfloat16 [8, 2048, 4096], P('ep', None, 'tp'), may hold values from -0.125 to 0.125
- expert_up: bfloat16 [8, 2048, 4096], P('ep', None, 'tp'), may hold values from -0.125 to 0.125
- expert_down: bfloat16 [8, 4096, 2048], P('ep', 'tp'), may hold values from -0.1875 to 0.1875
- blend_vector: bfloat16 [2048], replicated, may hold values from -0.125 to 0.125
- dense_gate: bfloat16 [2048, 7168], P('tp', 'ep'), may hold values from -0.125 to 0.125
- dense_up: bfloat16 [2048, 7168], P('tp', 'ep'), may hold values from -0.125 to 0.125
- dense_down: bfloat16 [7168, 2048], P('ep', 'tp'), may hold values from -0.125 to 0.125
Outputs:
- output: float32 [128, 2048], P('ep', 'tp')
- new_recurrent: float32 [128, 16, 64, 128], P('ep', 'tp')
- new_inner_history: bfloat16 [128, 3, 1024], P('ep', None, 'tp')
- new_access_history: bfloat16 [128, 2, 3, 512], P('ep')
The draws below stay inside these ranges and needn't reach their ends.
Inputs may be any that keep to these rules, and one draw needn't show every extreme that they name: `expert_ids`: each row names 2 different experts; among the rows of one device no expert is named by more than 8 rows, and in some aligned blocks of 16 rows one expert is named by exactly 8.
All inputs are finite; a program needn't handle non-finite values.
Results may differ from the reference program's by a relative error of at most 0.009.
Values may be sent and summed in bfloat16 or wider, within the bound.
A program may use at most 64 MiB of HBM per device.

```python
import math
import jax
import jax.numpy as jnp
import numpy as np
from jax import lax

D = 2048
HEADS = 16
HEAD_DIM = 64
GROUPS = 4
STATE = 128
TAPS = 4
FF = 4096
DF = 7168
TOP = 2
SEQS = 16
INNER = 1024
EXPERTS = 8
CAP = 8
TOKENS = 128
N_EP = 8


def levels(own_key, extent, split, smallest, largest):
    factor_of, own = 1.0, jax.random.fold_in(own_key, 6)
    for position, parts in split:
        heights = jnp.exp(jax.random.uniform(jax.random.fold_in(own, position), (parts,), jnp.float32, smallest / len(split), largest / len(split)))
        factor_of = factor_of * jnp.repeat(heights, extent[position] // parts).reshape([-1 if axis == position else 1 for axis in range(len(extent))])
    return factor_of


def routed_block(rng, own, number, rows, count, top, bound, skew):
    sequence = jax.random.permutation(rng, count)
    crowded, usual = shares(count, rows * top, bound, skew, True), shares(count, rows * top, bound, skew, False)
    places = jnp.arange(count)

    def named(sizes, rotation):
        used = int((sizes > 0).sum())
        fixed = max(1, used // 4)
        moved = fixed + (places - fixed + rotation * (used - fixed)) % max(1, count - fixed)
        return jnp.zeros((count,), jnp.int32).at[sequence[jnp.where(places < fixed, places, moved)]].set(jnp.asarray(sizes, jnp.int32))

    sizes = jnp.where(number % 4 == 0, named(crowded, number // 4), named(usual, number - number // 4 - 1))
    mixed = jax.random.permutation(jax.random.fold_in(own, 3), count)
    source_of, receiver = mixed[0:count // 2 * 2:2], mixed[1:count // 2 * 2:2]
    room = jnp.minimum(sizes[source_of] - 1, bound - sizes[receiver]) // 2
    room = jnp.where((source_of == sequence[0]) | (receiver == sequence[0]) | (sizes[receiver] == 0), 0, jnp.maximum(room, 0))
    moved = jax.random.randint(jax.random.fold_in(own, 4), (count // 2,), 0, 1 << 20) % (room + 1)
    sizes = sizes.at[source_of].add(-moved).at[receiver].add(moved)
    items = jnp.searchsorted(jnp.cumsum(sizes), jnp.arange(rows * top), side="right").astype(jnp.int32)
    table = items.reshape(top, rows).T
    table = table[jax.random.permutation(jax.random.fold_in(own, 1), rows)]
    rotation = jax.random.randint(jax.random.fold_in(own, 2), (rows, 1), 0, top)
    return jnp.take_along_axis(table, (jnp.arange(top)[None, :] + rotation) % top, axis=1)


def shares(number_of, total, limit, slope, full):
    loads = [(1 << 20) // math.isqrt(standing ** slope) + 1 for standing in range(1, number_of + 1)]
    largest = limit if full else min(limit, max(-(-total // number_of), total * loads[0] // sum(loads)))
    least = 1 if total - largest >= number_of - 1 else 0
    given, rest = [largest] + [least] * (number_of - 1), total - largest - least * (number_of - 1)
    while rest > 0:
        movable = [i for i in range(1, number_of) if given[i] < largest] or [i for i in range(1, number_of) if given[i] < limit]
        pool, remaining = sum([loads[i] for i in movable]), rest
        for i in movable:
            addition = min(limit - given[i], max(1, remaining * loads[i] // pool), rest)
            given[i] = given[i] + addition
            rest = rest - addition
    return np.array(given)


def scatter_about(rng, shape, deviation, bound, shards=(), dtype=jnp.bfloat16):
    array = jax.random.normal(rng, shape, jnp.float32) * deviation
    if len(shards) > 0:
        array = levels(rng, shape, shards, -0.22, 0.18) * array
    return jnp.clip(array, min=-bound, max=bound).astype(dtype)


def setup_inputs(seed: int = 0) -> dict:
    key_of = jax.random.split(jax.random.key(seed), 28)
    tokens = scatter_about(key_of[0], (TOKENS, D), 1.0, 6.0, ((0, 8),))
    mix_gain = jnp.clip(1.0 + 0.18 * jax.random.normal(key_of[1], (D,), jnp.float32), 0.1, 1.9)
    gate_weight = scatter_about(key_of[2], (D, INNER), D ** -0.5, 0.125, ((0, 8), (1, 4)))
    inner_weight = scatter_about(key_of[3], (D, INNER), D ** -0.5, 0.125, ((0, 8), (1, 4)))
    write_weight = scatter_about(key_of[4], (D, GROUPS * STATE), D ** -0.5, 0.125, ((0, 8),))
    read_weight = scatter_about(key_of[5], (D, GROUPS * STATE), D ** -0.5, 0.125, ((0, 8),))
    step_weight = scatter_about(key_of[6], (D, HEADS), D ** -0.5, 0.125, ((0, 8),))
    step_bias = jnp.clip(jax.random.uniform(key_of[7], (HEADS,), jnp.float32, -2.0, 1.0), -2.0, 1.0)
    decay_log = jnp.clip(jax.random.uniform(key_of[8], (HEADS,), jnp.float32, -1.0, 1.5), -1.0, 1.5)
    skip_scale = jnp.clip(jax.random.uniform(key_of[9], (HEADS,), jnp.float32, 0.5, 2.0), 0.5, 2.0)
    inner_taps = scatter_about(key_of[10], (TAPS, INNER), 0.5, 3.0, ((1, 4),))
    access_taps = scatter_about(key_of[11], (2, TAPS, GROUPS * STATE), 0.5, 3.0)
    inner_history = scatter_about(key_of[12], (TOKENS, TAPS - 1, INNER), 1.0, 6.0, ((0, 8), (2, 4)))
    access_history = scatter_about(key_of[13], (TOKENS, 2, TAPS - 1, GROUPS * STATE), 1.0, 6.0, ((0, 8),))
    recurrent = scatter_about(key_of[14], (TOKENS, HEADS, HEAD_DIM, STATE), 0.5, 3.0, ((0, 8), (1, 4)), jnp.float32)
    head_gain = jnp.clip(1.0 + 0.18 * jax.random.normal(key_of[15], (INNER,), jnp.float32), 0.1, 1.9)
    mixer_out = scatter_about(key_of[16], (INNER, D), INNER ** -0.5, 0.1875, ((0, 4),))
    moe_gain = jnp.clip(1.0 + 0.18 * jax.random.normal(key_of[17], (D,), jnp.float32), 0.1, 1.9)
    expert_ids_keys = jax.random.split(jax.random.fold_in(key_of[18], 1), TOKENS // SEQS)
    expert_ids_turns = jax.random.permutation(jax.random.fold_in(key_of[18], 3), TOKENS // SEQS)
    expert_ids = jax.vmap(lambda own, number: routed_block(jax.random.fold_in(key_of[18], 2), own, number, SEQS, EXPERTS, TOP, CAP, 2))(expert_ids_keys, expert_ids_turns).reshape((TOKENS, TOP))
    route_scores = scatter_about(key_of[19], (TOKENS, TOP), 1.0, 6.0, ((0, 8),), jnp.float32)
    expert_gate = scatter_about(key_of[20], (EXPERTS, D, FF), D ** -0.5, 0.125, ((0, 8), (2, 4)))
    expert_up = scatter_about(key_of[21], (EXPERTS, D, FF), D ** -0.5, 0.125, ((0, 8), (2, 4)))
    expert_down = scatter_about(key_of[22], (EXPERTS, FF, D), (FF // 4) ** -0.5, 0.1875, ((0, 8), (1, 4)))
    blend_vector = scatter_about(key_of[23], (D,), D ** -0.5, 0.125)
    dense_gate = scatter_about(key_of[24], (D, DF), D ** -0.5, 0.125, ((0, 4), (1, 8)))
    dense_up = scatter_about(key_of[25], (D, DF), D ** -0.5, 0.125, ((0, 4), (1, 8)))
    dense_down = scatter_about(key_of[26], (DF, D), (DF // 4) ** -0.5, 0.125, ((0, 8), (1, 4)))
    return dict(tokens=tokens, mix_gain=mix_gain, gate_weight=gate_weight, inner_weight=inner_weight, write_weight=write_weight, read_weight=read_weight, step_weight=step_weight, step_bias=step_bias, decay_log=decay_log, skip_scale=skip_scale, inner_taps=inner_taps, access_taps=access_taps, inner_history=inner_history, access_history=access_history, recurrent=recurrent, head_gain=head_gain, mixer_out=mixer_out, moe_gain=moe_gain, expert_ids=expert_ids, route_scores=route_scores, expert_gate=expert_gate, expert_up=expert_up, expert_down=expert_down, blend_vector=blend_vector, dense_gate=dense_gate, dense_up=dense_up, dense_down=dense_down)


EPS = 1e-06

def rms_scale(values, gain):
    mean_square = lax.optimization_barrier(jnp.mean(values * values, axis=-1, keepdims=True))
    return values * lax.rsqrt(mean_square + EPS) * gain

def reference(tokens, mix_gain, gate_weight, inner_weight, write_weight, read_weight, step_weight, step_bias, decay_log, skip_scale, inner_taps, access_taps, inner_history, access_history, recurrent, head_gain, mixer_out, moe_gain, expert_ids, route_scores, expert_gate, expert_up, expert_down, blend_vector, dense_gate, dense_up, dense_down):
    count = tokens.shape[0]
    normed = rms_scale(tokens.astype(jnp.float32), mix_gain).astype(jnp.bfloat16)
    gate_part = jnp.dot(normed, gate_weight, preferred_element_type=jnp.float32).astype(jnp.bfloat16)
    inner_part = jnp.dot(normed, inner_weight, preferred_element_type=jnp.float32).astype(jnp.bfloat16)
    write_part = jnp.dot(normed, write_weight, preferred_element_type=jnp.float32).astype(jnp.bfloat16)
    read_part = jnp.dot(normed, read_weight, preferred_element_type=jnp.float32).astype(jnp.bfloat16)
    step_raw = jnp.dot(normed, step_weight, preferred_element_type=jnp.float32)
    inner_window = jnp.concatenate([inner_history, inner_part[:, None, :]], axis=1)
    inner_conv = jax.nn.silu(lax.optimization_barrier(jnp.sum(inner_window.astype(jnp.float32) * inner_taps.astype(jnp.float32)[None], axis=1)))
    access_window = jnp.concatenate([access_history, jnp.stack([write_part, read_part], axis=1)[:, :, None, :]], axis=2)
    access_conv = jax.nn.silu(lax.optimization_barrier(jnp.sum(access_window.astype(jnp.float32) * access_taps.astype(jnp.float32)[None], axis=2)))
    per_group = HEADS // GROUPS
    write_heads = jnp.repeat(access_conv[:, 0].reshape(count, GROUPS, STATE), per_group, axis=1)
    read_heads = jnp.repeat(access_conv[:, 1].reshape(count, GROUPS, STATE), per_group, axis=1)
    step = jax.nn.softplus(step_raw + step_bias[None, :])
    decay = jnp.exp(-step * jnp.exp(decay_log)[None, :])
    inner_heads = inner_conv.reshape(count, HEADS, HEAD_DIM)
    new_recurrent = decay[:, :, None, None] * recurrent + (step[:, :, None] * inner_heads)[..., None] * write_heads[:, :, None, :]
    readout = lax.optimization_barrier(jnp.sum(new_recurrent * read_heads[:, :, None, :], axis=-1)) + skip_scale[None, :, None] * inner_heads
    gated = readout * jax.nn.silu(gate_part.astype(jnp.float32).reshape(count, HEADS, HEAD_DIM))
    head_out = rms_scale(gated, head_gain.reshape(HEADS, HEAD_DIM)).reshape(count, HEADS * HEAD_DIM).astype(jnp.bfloat16)
    mixed = jnp.dot(head_out, mixer_out, preferred_element_type=jnp.float32).astype(jnp.bfloat16)
    resid = tokens.astype(jnp.float32) + mixed.astype(jnp.float32)
    hidden = rms_scale(resid, moe_gain).astype(jnp.bfloat16)
    first = jax.nn.sigmoid(route_scores[:, 0] - route_scores[:, 1])
    weights = jnp.stack([first, 1.0 - first], axis=1).reshape(-1)
    flat_ids = expert_ids.reshape(-1)
    flat_token = (jnp.arange(count * TOP) // TOP).astype(jnp.int32)
    most = CAP * N_EP

    def one_expert(total, expert):
        chosen = flat_ids == expert
        picked = jnp.nonzero(chosen, size=most, fill_value=0)[0].astype(jnp.int32)
        valid = (jnp.arange(most) < jnp.sum(chosen.astype(jnp.int32))).astype(jnp.float32)
        rows = hidden[flat_token[picked]]
        gate_vals = jnp.dot(rows, expert_gate[expert], preferred_element_type=jnp.float32)
        up_vals = jnp.dot(rows, expert_up[expert], preferred_element_type=jnp.float32)
        act = (jax.nn.silu(gate_vals) * up_vals).astype(jnp.bfloat16)
        expert_out = jnp.dot(act, expert_down[expert], preferred_element_type=jnp.float32).astype(jnp.bfloat16)
        share = expert_out.astype(jnp.float32) * (weights[picked] * valid)[:, None]
        return (total.at[flat_token[picked]].add(share), None)
    routed, unused = lax.scan(one_expert, jnp.zeros((count, tokens.shape[1]), jnp.float32), jnp.arange(EXPERTS).astype(jnp.int32))
    dense_g = jnp.dot(hidden, dense_gate, preferred_element_type=jnp.float32)
    dense_u = jnp.dot(hidden, dense_up, preferred_element_type=jnp.float32)
    dense_act = (jax.nn.silu(dense_g) * dense_u).astype(jnp.bfloat16)
    dense_out = jnp.dot(dense_act, dense_down, preferred_element_type=jnp.float32)
    blend = jax.nn.sigmoid(jnp.dot(hidden, blend_vector, preferred_element_type=jnp.float32))
    output = resid + routed + blend[:, None] * dense_out
    return (output, new_recurrent, inner_window[:, 1:], access_window[:, :, 1:])
```

```python
import functools

import jax
import jax.numpy as jnp
from jax import lax
from jax.experimental import pallas as pl
from jax.experimental.pallas import tpu as pltpu
from jax.sharding import PartitionSpec as P

HEADS = 16
HEAD_DIM = 64
GROUPS = 4
STATE = 128
LANES = 128
TOP = 2
EPS = 1e-06
BF = jnp.bfloat16
F32 = jnp.float32


def dot(a, b):
    return jnp.dot(a, b, preferred_element_type=F32)


def silu(x):
    return x * (1.0 / (1.0 + jnp.exp(-x)))


def tile_of(extent):
    return 256 if extent % 256 == 0 else extent


def kernel(
    E, T, CAP,
    tokens_h, mix_gain_h, step_weight_h, step_bias_h, decay_log_h, skip_scale_h, inner_taps_h, access_taps_h,
    inner_past_h, access_past_h, head_gain_h, moe_gain_h, ids_h, scores_h, blend_vector_h,
    gate_w, inner_w, write_w, read_w, recurrent, mixer_w, eg_w, eu_w, ed_w, dg_w, du_w, dd_w,
    out, nrec, inner_new, access_new,
    tokens, mix_gain, step_weight, step_bias, decay_log, skip_scale, inner_taps, access_taps,
    inner_past, access_past, head_gain, moe_gain, ids, scores, blend_vector,
    gw, iw, ww, rw, rec, mw, eg, eu, ed, dg, du, dd,
    xs, xr, ps, pr, pg, pgr, rcat, ms, mr, mm, mmr, rbuf, hbuf, sel, gacc, uacc, actb, dps, dpr, dab, es, er, fs, fr,
    small_sem, load_sem, s_ep, r_ep, s_tp, r_tp, s_h, r_h, s_x, r_x,
):
    me = lax.axis_index("ep")
    mt = lax.axis_index("tp")
    S, D = tokens.shape
    C = gw.shape[1]
    DC = D // E
    DS = D // T
    U = dg.shape[1]
    FFL = eg.shape[1]
    R = E * S // T
    N = E * CAP
    M = 2 * STATE
    group = mt * (HEADS // T) // (HEADS // GROUPS)

    barrier = pltpu.get_barrier_semaphore()
    for k in range(1, E):
        pl.semaphore_signal(barrier, inc=1, device_id={"ep": lax.rem(me + k, E)},
                            device_id_type=pl.DeviceIdType.MESH)
    for k in range(1, T):
        pl.semaphore_signal(barrier, inc=1, device_id={"tp": lax.rem(mt + k, T)},
                            device_id_type=pl.DeviceIdType.MESH)

    cols = pl.ds(pl.multiple_of(group * STATE, STATE), STATE)
    small = [
        (tokens_h, tokens), (mix_gain_h, mix_gain), (ids_h, ids), (step_weight_h, step_weight),
        (scores_h, scores), (step_bias_h, step_bias), (decay_log_h, decay_log), (skip_scale_h, skip_scale),
        (inner_taps_h, inner_taps), (access_taps_h.at[:, :, cols], access_taps), (inner_past_h, inner_past),
        (access_past_h.at[:, :, :, cols], access_past), (head_gain_h, head_gain), (moe_gain_h, moe_gain),
        (blend_vector_h, blend_vector), (access_past_h.at[:, 1:3], access_new.at[:, 0:2]),
    ]
    smalls = [pltpu.make_async_copy(a, b, small_sem.at[i]) for i, (a, b) in enumerate(small)]
    pairs = [
        (gate_w, gw), (inner_w, iw), (write_w.at[:, cols], ww), (read_w.at[:, cols], rw),
        (recurrent, rec), (mixer_w, mw), (dg_w, dg), (du_w, du), (eg_w, eg), (eu_w, eu),
        (dd_w, dd), (ed_w, ed),
    ]
    loads = [pltpu.make_async_copy(a, b, load_sem.at[i]) for i, (a, b) in enumerate(pairs)]
    for c in smalls[:4]:
        c.start()
    for c in loads[:4]:
        c.start()
    for c in smalls[4:]:
        c.start()
    for c in loads[4:]:
        c.start()

    sends = []

    def remote(src, dst, send, recv, device):
        c = pltpu.make_async_remote_copy(
            src_ref=src, dst_ref=dst, send_sem=send, recv_sem=recv,
            device_id=device, device_id_type=pl.DeviceIdType.MESH)
        c.start()
        sends.append(c)
        return c

    def ep_send(phase, src_of, dst):
        got = []
        for k in range(1, E):
            to = lax.rem(me + k, E)
            got.append(remote(src_of(to), dst, s_ep.at[phase, k], r_ep.at[phase, k], {"ep": to}))
        return got

    def tp_send(phase, src_of, dst):
        got = []
        for k in range(1, T):
            to = lax.rem(mt + k, T)
            got.append(remote(src_of(to), dst, s_tp.at[phase, k], r_tp.at[phase, k], {"tp": to}))
        return got

    def arrive(copies):
        for c in copies:
            c.wait_recv()

    lane = lax.broadcasted_iota(jnp.int32, (S, LANES), 1)
    lane_f = lane.astype(F32)
    row_i = lax.broadcasted_iota(jnp.int32, (S, S), 0)
    col_i = lax.broadcasted_iota(jnp.int32, (S, S), 1)
    diagonal = row_i == col_i
    earlier = jnp.where(col_i < row_i, 1.0, 0.0)

    def column(row):
        return jnp.sum(jnp.where(diagonal, row, 0.0), axis=-1, keepdims=True)

    for c in smalls[:3]:
        c.wait()
    tok = tokens[...].astype(F32)
    scale = lax.rsqrt(jnp.mean(tok * tok, axis=-1, keepdims=True) + EPS)
    normed = (tok * scale * mix_gain[...]).astype(BF)
    names = ids[...].astype(F32)
    name_a, name_b = column(names[0:1]), column(names[1:2])
    named = jnp.where((lane_f == name_a) | (lane_f == name_b), 1.0, 0.0)
    before = dot(earlier, named)
    rank = jnp.where(named > 0.0, before, -1.0)
    for j in range(E):
        xs[j, :, 0:DC] = normed[:, j * DC:(j + 1) * DC]
        xs[j, :, DC:DC + LANES] = jnp.broadcast_to(rank[:, j:j + 1], (S, LANES)).astype(BF)
    xr[me] = xs[me]
    pl.semaphore_wait(barrier, (E - 1) + (T - 1))
    got = ep_send(0, lambda to: xs.at[to], xr.at[me])

    for c in smalls[3:15]:
        c.wait()
    ranks = scores[...]
    first = 1.0 / (1.0 + jnp.exp(column(ranks[1:2]) - column(ranks[0:1])))
    combine = jnp.where(lane_f == name_a, first, 0.0) + jnp.where(lane_f == name_b, 1.0 - first, 0.0)
    slot = lax.broadcasted_iota(jnp.int32, (S, N), 1)
    slot_rank = lax.rem(slot, CAP).astype(F32)
    mix = jnp.zeros((S, N), F32)
    for e in range(E):
        hit = (slot // CAP == e) & (slot_rank == rank[:, e:e + 1])
        mix = jnp.where(hit, combine[:, e:e + 1], mix)
    mix_hi = mix.astype(BF)
    mix_lo = (mix - mix_hi.astype(F32)).astype(BF)

    taps_k = access_taps[...].astype(F32)
    tap_rows = [jnp.concatenate([taps_k[0, k:k + 1], taps_k[1, k:k + 1]], axis=0) for k in range(4)]
    row_of = lax.broadcasted_iota(jnp.int32, (S, STATE), 0)
    past_w = jnp.zeros((S, STATE), F32)
    past_r = jnp.zeros((S, STATE), F32)
    for s in range(S):
        total = access_past[s, 0].astype(F32) * tap_rows[0]
        for k in range(1, 3):
            total = total + access_past[s, k].astype(F32) * tap_rows[k]
        past_w = jnp.where(row_of == s, total[0:1], past_w)
        past_r = jnp.where(row_of == s, total[1:2], past_r)

    for c in loads[:4]:
        c.wait()
    arrive(got)

    rows = xr[:, :, 0:DC].reshape(E * S, DC)
    step_p = lax.dot_general(
        rows, step_weight[...], (((1,), (1,)), ((), ())), preferred_element_type=F32)
    step_hi = step_p.astype(BF)
    step_lo = (step_p - step_hi.astype(F32)).astype(BF)
    ps[:, :, 0:STATE] = dot(rows, ww[...]).astype(BF).reshape(E, S, STATE)
    ps[:, :, STATE:M] = dot(rows, rw[...]).astype(BF).reshape(E, S, STATE)
    ps[:, :, M:M + LANES] = jnp.concatenate(
        [step_hi, step_lo, jnp.zeros((E * S, LANES - 2 * HEADS), BF)], axis=1).reshape(E, S, LANES)
    G = M + LANES
    ps[:, :, G:G + C] = dot(rows, iw[...]).astype(BF).reshape(E, S, C)
    pr[me] = ps[me]
    got = ep_send(1, lambda to: ps.at[to], pr.at[me])
    pg[...] = dot(rows, gw[...]).astype(BF).reshape(E, S, C)
    pgr[me] = pg[me]
    got_g = ep_send(2, lambda to: pg.at[to], pgr.at[me])

    rank_of = xr[:, :, DC:DC + LANES].reshape(E * S, LANES)[:, 0:N].astype(F32)
    wide = lax.broadcasted_iota(jnp.int32, (E * S, N), 1)
    seq = lax.broadcasted_iota(jnp.int32, (E * S, N), 0)
    chosen = (wide // CAP == seq // S) & (lax.rem(wide, CAP).astype(F32) == rank_of)
    sel[...] = jnp.transpose(jnp.where(chosen, 1.0, 0.0)).astype(BF)

    chan = lax.broadcasted_iota(jnp.int32, (S, C), 1)
    head_of = mt * (HEADS // T) + chan // HEAD_DIM

    def expand(values):
        total = jnp.zeros((S, C), F32)
        for h in range(HEADS):
            total = jnp.where(head_of == h, values[:, h:h + 1], total)
        return total

    skip = expand(skip_scale[...])
    taps = inner_taps[...].astype(F32)
    past = inner_past[0].astype(F32) * taps[0:1]
    for k in range(1, 3):
        past = past + inner_past[k].astype(F32) * taps[k:k + 1]
        inner_new[k - 1] = inner_past[k]
    rate = jnp.exp(decay_log[...])
    loads[4].wait()

    @pl.loop(0, S)
    def _(t):
        value = rec[t]
        high = value.astype(BF)
        rcat[t, :, 0:STATE] = high
        rcat[t, :, STATE:M] = (value - high.astype(F32)).astype(BF)

    arrive(got)
    proj = pr[0].astype(F32)
    for j in range(1, E):
        proj = proj + pr[j].astype(F32)
    maps = proj[:, 0:M].astype(BF)
    step_raw = proj[:, M:M + HEADS] + proj[:, M + HEADS:M + 2 * HEADS]
    inner_part = proj[:, G:G + C].astype(BF)
    inner_new[2] = inner_part
    inner = silu(past + inner_part.astype(F32) * taps[3:4])
    mm[...] = maps
    maps_f = maps.astype(F32)
    write_c = silu(past_w + maps_f[:, 0:STATE] * tap_rows[3][0:1])
    read_c = silu(past_r + maps_f[:, STATE:M] * tap_rows[3][1:2])
    read_hi = read_c.astype(BF).astype(F32)
    read_lo = read_c - read_hi
    spare = LANES - 2 * S
    upper = jnp.concatenate([read_hi, read_lo, jnp.zeros((spare, STATE), F32)], axis=0)
    lower = jnp.concatenate([read_hi, jnp.zeros((spare + S, STATE), F32)], axis=0)
    reader = jnp.concatenate([jnp.transpose(upper), jnp.transpose(lower)], axis=0).astype(BF)
    step_x = step_raw + step_bias[...]
    step = jnp.maximum(step_x, 0.0) + jnp.log1p(jnp.exp(-jnp.abs(step_x)))
    decay = expand(jnp.exp(-step * rate))
    push = expand(step) * inner
    both = jnp.sum(write_c * read_c, axis=-1, keepdims=True)
    seq_lane = lax.rem(lax.broadcasted_iota(jnp.int32, (C, LANES), 1), S)
    read_t = jnp.zeros((C, LANES), F32)
    for t in range(S):
        read_t = jnp.where(seq_lane == t, dot(rcat[t], reader), read_t)
    read_rows = jnp.transpose(read_t)
    recalled = read_rows[0:S] + read_rows[S:2 * S]
    readout = decay * recalled + push * both + skip * inner
    arrive(got_g)
    gate_sum = pgr[0].astype(F32)
    for j in range(1, E):
        gate_sum = gate_sum + pgr[j].astype(F32)
    gated = readout * silu(gate_sum.astype(BF).astype(F32))
    square = gated * gated
    norm = jnp.zeros((S, C), F32)
    for h in range(C // HEAD_DIM):
        here = chan // HEAD_DIM == h
        mean = jnp.sum(jnp.where(here, square, 0.0), axis=-1, keepdims=True) / HEAD_DIM
        norm = jnp.where(here, lax.rsqrt(mean + EPS), norm)
    head_out = (gated * norm * head_gain[...]).astype(BF)
    loads[5].wait()
    for j in range(T):
        ms[:, j * DS:(j + 1) * DS] = dot(head_out, mw[:, j * DS:(j + 1) * DS]).astype(BF)
    mr[mt] = ms[...]
    got = tp_send(0, lambda to: ms, mr.at[mt])
    mmr[mt] = mm[...]
    got_m = tp_send(1, lambda to: mm, mmr.at[mt])

    decay_t = jnp.transpose(decay)
    push_t = jnp.transpose(push)
    for t in range(S):
        nrec[t] = decay_t[:, t:t + 1] * rec[t] + push_t[:, t:t + 1] * write_c[t:t + 1]

    arrive(got)
    mixed = mr[0].astype(F32)
    for j in range(1, T):
        mixed = mixed + mr[j].astype(F32)
    resid = tok + mixed.astype(BF).astype(F32)
    scale = lax.rsqrt(jnp.mean(resid * resid, axis=-1, keepdims=True) + EPS)
    hidden = (resid * scale * moe_gain[...]).astype(BF)
    for q in range(T):
        rbuf[q] = resid[:, q * DS:(q + 1) * DS]
        hbuf[q, me] = hidden[:, q * DS:(q + 1) * DS]

    twin = me + 1 - 2 * lax.rem(me, 2)
    chips = E // 2
    pieces = []
    for j in range(T):
        q = lax.rem(mt + j, T)
        here = []
        for m in range(1, chips):
            to = lax.rem(me + 2 * m, E)
            here.append(remote(hbuf.at[q, me], hbuf.at[q, me], s_h.at[j, 2 * m], r_h.at[j, 2 * m], {"ep": to}))
        beside = remote(hbuf.at[q, me], hbuf.at[q, me], s_h.at[j, 1], r_h.at[j, 1], {"ep": twin})
        pieces.append((here, beside))

    scorer = blend_vector[...].astype(F32)
    blend = jnp.zeros((S, LANES), F32)
    for j in range(D // LANES):
        blend = blend + hidden[:, j * LANES:(j + 1) * LANES].astype(F32) * scorer[j:j + 1]
    blend = jnp.sum(blend, axis=-1, keepdims=True)
    blend = 1.0 / (1.0 + jnp.exp(-blend))

    arrive(got_m)
    smalls[15].wait()
    owners = [mmr[g * max(1, T // GROUPS)].astype(F32) for g in range(GROUPS)]
    for s in range(S):
        for g in range(GROUPS):
            pair = jnp.concatenate([owners[g][s:s + 1, 0:STATE], owners[g][s:s + 1, STATE:M]], axis=0)
            access_new[s, 2, :, g * STATE:(g + 1) * STATE] = pair.astype(BF)

    def relay(j):
        q = lax.rem(mt + j, T)
        here, beside = pieces[j]
        passed = [beside]
        for m in range(1, chips):
            here[m - 1].wait_recv()
            source = lax.rem(me + E - 2 * m, E)
            block = hbuf.at[q, source]
            passed.append(remote(block, block, s_h.at[j, 2 * m + 1], r_h.at[j, 2 * m + 1], {"ep": twin}))
        return passed

    passed = relay(0)
    got_d = None
    tile = tile_of(FFL)
    for c in loads[6:10]:
        c.wait()
    for j in range(T):
        q = lax.rem(mt + j, T)
        arrive(passed)
        here = hbuf[q].reshape(E * S, DS)
        if j == 0:
            dps[:, 0] = dot(here, dg[...]).astype(BF).reshape(T, R, U)
            dps[:, 1] = dot(here, du[...]).astype(BF).reshape(T, R, U)
            dpr[mt] = dps[mt]
            got_d = tp_send(2, lambda to: dps.at[to], dpr.at[mt])
        rows_q = pl.ds(pl.multiple_of(q * DS, DS), DS)
        picked = dot(sel[...], here).astype(BF)

        @pl.loop(0, FFL // tile)
        def _(n, picked=picked, rows_q=rows_q, j=j):
            at = pl.ds(pl.multiple_of(n * tile, tile), tile)
            g = dot(picked, eg[rows_q, at])
            u = dot(picked, eu[rows_q, at])
            if j > 0:
                g = g + gacc[:, at]
                u = u + uacc[:, at]
            if j < T - 1:
                gacc[:, at] = g
                uacc[:, at] = u
            else:
                actb[:, at] = (silu(g) * u).astype(BF)

        if j < T - 1:
            passed = relay(j + 1)

    def dense_act():
        arrive(got_d)
        dsum = dpr[0].astype(F32)
        for j in range(1, T):
            dsum = dsum + dpr[j].astype(F32)
        dab[mt] = (silu(dsum[0]) * dsum[1]).astype(BF)
        return tp_send(3, lambda to: dab.at[mt], dab.at[mt])

    loads[11].wait()
    got_a = None
    got_e = []
    dtile = tile_of(DS)
    for k in range(T - 1, -1, -1):
        to = lax.rem(mt + k, T)
        for n in range(DS // dtile):
            at = pl.ds(pl.multiple_of(to * DS + n * dtile, dtile), dtile)
            share = dot(actb[...], ed[:, at])
            for s in range(E):
                es[k, s, :, n * dtile:(n + 1) * dtile] = share[s * CAP:(s + 1) * CAP].astype(BF)
        for d in range(E - 1, -1, -1):
            owner = lax.rem(me + d, E)
            if k > 0 or d > 0:
                got_e.append(remote(
                    es.at[k, owner], er.at[k, me], s_x.at[k, d], r_x.at[k, d], {"ep": owner, "tp": to}))
            else:
                er[0, me] = es[0, me]
        if k == T - 1:
            got_a = dense_act()
    loads[10].wait()
    arrive(got_a)
    fs[...] = dot(dab[...].reshape(E * S, U), dd[...]).astype(BF).reshape(E, S, DS)
    fr[me] = fs[me]
    got = ep_send(3, lambda to: fs.at[to], fr.at[me])
    arrive(got_e)
    total = er[0].astype(F32)
    for k in range(1, T):
        total = total + er[k].astype(F32)
    outs = total.reshape(N, DS).astype(BF)
    final = rbuf[mt] + dot(mix_hi, outs) + dot(mix_lo, outs)
    arrive(got)
    dense = fr[0].astype(F32)
    for j in range(1, E):
        dense = dense + fr[j].astype(F32)
    out[...] = final + blend * dense
    for c in sends:
        c.wait_send()


def finish(out, rec, inner, access, out_o, rec_o, inner_o, access_o, sem):
    S = rec.shape[0]
    parts = 4 if S % 4 == 0 else 1
    size = S // parts
    copies = [
        pltpu.make_async_copy(rec.at[i * size:(i + 1) * size], rec_o.at[i * size:(i + 1) * size], sem.at[i])
        for i in range(parts)
    ]
    for i, (a, b) in enumerate([(out, out_o), (inner, inner_o), (access, access_o)]):
        copies.append(pltpu.make_async_copy(a, b, sem.at[parts + i]))
    for c in copies:
        c.start()
    for c in copies:
        c.wait()


def local(
    E, T,
    tokens, mix_gain, gate_weight, inner_weight, write_weight, read_weight, step_weight, step_bias,
    decay_log, skip_scale, inner_taps, access_taps, inner_history, access_history, recurrent,
    head_gain, mixer_out, moe_gain, expert_ids, route_scores, expert_gate, expert_up, expert_down,
    blend_vector, dense_gate, dense_up, dense_down,
):
    S, D = tokens.shape
    C = gate_weight.shape[1]
    DC, DS = D // E, D // T
    U = dense_gate.shape[1]
    FFL = expert_gate.shape[2]
    GS = access_taps.shape[2]
    rows = E * S
    R = rows // T
    M = 2 * STATE
    PW = M + LANES + C
    CAP = max(1, 2 * TOP * S // E)
    N = E * CAP
    vmem = pl.BlockSpec(memory_space=pltpu.VMEM)
    hbm = pl.BlockSpec(memory_space=pltpu.HBM)
    V = pltpu.VMEM
    DMA = pltpu.SemaphoreType.DMA
    shapes = (
        jax.ShapeDtypeStruct((S, DS), F32),
        jax.ShapeDtypeStruct((S, C, STATE), F32),
        jax.ShapeDtypeStruct((3, S, C), BF),
        jax.ShapeDtypeStruct((S, 3, 2, GS), BF),
    )
    held = tuple(pltpu.VMEM(x.shape, x.dtype) for x in shapes)
    operands = (
        tokens, mix_gain[None], step_weight.T, step_bias[None], decay_log[None], skip_scale[None],
        inner_taps, access_taps, inner_history.transpose(1, 0, 2), access_history.transpose(0, 2, 1, 3),
        head_gain[None], moe_gain[None], expert_ids.T, route_scores.T, blend_vector.reshape(-1, LANES),
        gate_weight, inner_weight, write_weight, read_weight,
        recurrent.reshape(S, C, STATE), mixer_out,
        expert_gate[0], expert_up[0], expert_down[0], dense_gate, dense_up, dense_down,
    )
    results = pl.pallas_call(
        functools.partial(kernel, E, T, CAP),
        name="decode_step",
        out_shape=held,
        in_specs=[hbm] * 27,
        out_specs=(vmem,) * 4,
        scratch_shapes=[
            V((S, D), BF), V((1, D), F32), V((HEADS, DC), BF), V((1, HEADS), F32), V((1, HEADS), F32),
            V((1, HEADS), F32), V((4, C), BF), V((2, 4, STATE), BF), V((3, S, C), BF), V((S, 3, 2, STATE), BF),
            V((1, C), F32), V((1, D), F32), V((TOP, S), jnp.int32), V((TOP, S), F32), V((D // LANES, LANES), BF),
            V((DC, C), BF), V((DC, C), BF), V((DC, STATE), BF), V((DC, STATE), BF),
            V((S, C, STATE), F32), V((C, D), BF),
            V((D, FFL), BF), V((D, FFL), BF), V((FFL, D), BF),
            V((DS, U), BF), V((DS, U), BF), V((U, DS), BF),
            V((E, S, DC + LANES), BF), V((E, S, DC + LANES), BF), V((E, S, PW), BF), V((E, S, PW), BF),
            V((E, S, C), BF), V((E, S, C), BF), V((S, C, M), BF),
            V((S, D), BF), V((T, S, D), BF), V((S, M), BF), V((T, S, M), BF),
            V((T, S, DS), F32), V((T, E, S, DS), BF),
            V((N, rows), BF), V((N, FFL), F32), V((N, FFL), F32), V((N, FFL), BF),
            V((T, 2, R, U), BF), V((T, 2, R, U), BF), V((T, R, U), BF),
            V((T, E, CAP, DS), BF), V((T, E, CAP, DS), BF),
            V((E, S, DS), BF), V((E, S, DS), BF),
            DMA((16,)), DMA((12,)), DMA((4, E)), DMA((4, E)), DMA((4, T)), DMA((4, T)),
            DMA((T, E)), DMA((T, E)), DMA((T, E)), DMA((T, E)),
        ],
        compiler_params=pltpu.CompilerParams(
            collective_id=0, has_side_effects=True, vmem_limit_bytes=40 * 1024 * 1024
        ),
    )(*[pltpu.with_memory_space_constraint(x, pltpu.HBM) for x in operands])
    out, new_recurrent, inner_new, access_new = pl.pallas_call(
        finish,
        name="store_results",
        out_shape=shapes,
        in_specs=[vmem] * 4,
        out_specs=(hbm,) * 4,
        scratch_shapes=[DMA((8,))],
    )(*[pltpu.with_memory_space_constraint(x, pltpu.VMEM) for x in results])
    return (
        out, new_recurrent.reshape(recurrent.shape), inner_new.transpose(1, 0, 2),
        access_new.transpose(0, 2, 1, 3),
    )


def solution(mesh):
    in_specs = (
        P("ep", None), P(), P("ep", "tp"), P("ep", "tp"), P("ep", None), P("ep", None),
        P("ep", None), P(), P(), P(), P(None, "tp"), P(), P("ep", None, "tp"),
        P("ep", None, None, None), P("ep", "tp", None, None), P("tp"), P("tp", None), P(),
        P("ep", None), P("ep", None), P("ep", None, "tp"), P("ep", None, "tp"),
        P("ep", "tp", None), P(), P("tp", "ep"), P("tp", "ep"), P("ep", "tp"),
    )
    out_specs = (
        P("ep", "tp"), P("ep", "tp", None, None), P("ep", None, "tp"), P("ep", None, None, None),
    )
    body = functools.partial(local, mesh.shape["ep"], mesh.shape["tp"])
    return jax.shard_map(body, mesh=mesh, in_specs=in_specs, out_specs=out_specs, check_vma=False)
```

```python
import functools
import math

import jax
import jax.numpy as jnp
from jax import lax
from jax.experimental import pallas as pl
from jax.experimental.pallas import tpu as pltpu
from jax.sharding import PartitionSpec as P

HEADS = 16
HEAD_DIM = 64
GROUPS = 4
STATE = 128
LANES = 128
TOP = 2
EPS = 1e-06
BF = jnp.bfloat16
F32 = jnp.float32


def dot(a, b):
    return jnp.dot(a, b, preferred_element_type=F32)


def silu(x):
    return x * (1.0 / (1.0 + jnp.exp(-x)))


def tile_of(extent):
    return 256 if extent % 256 == 0 else extent


def kernel(
    E, T, CAP,
    tokens_h, mix_gain_h, step_weight_h, step_bias_h, decay_log_h, skip_scale_h, inner_taps_h, access_taps_h,
    inner_past_h, access_past_h, head_gain_h, moe_gain_h, ids_h, scores_h, blend_vector_h,
    gate_w, inner_w, write_w, read_w, recurrent, mixer_w, eg_w, eu_w, ed_w, dg_w, du_w, dd_w,
    out, nrec, inner_new, access_new,
    tokens, mix_gain, step_weight, step_bias, decay_log, skip_scale, inner_taps, access_taps,
    inner_past, access_past, head_gain, moe_gain, ids, scores, blend_vector,
    gw, iw, ww, rw, rec, mw, eg, eu, ed, dg, du, dd,
    xs, xr, rk, rkr, ps, pr, pg, pgr, rcat, ms, mr, mm, mmr, rbuf, hbuf, sel, cs, cr, gacc, uacc, actb, dps, dpr, dab, es, er, fs, fr,
    small_sem, load_sem, s_ep, r_ep, s_tp, r_tp, s_h, r_h, s_x, r_x, s_c, r_c, s_d, r_d,
):
    me = lax.axis_index("ep")
    mt = lax.axis_index("tp")
    S, D = tokens.shape
    C = gw.shape[1]
    DC = D // E
    DS = D // T
    U = dg.shape[1]
    FFL = eg.shape[1]
    N = E * CAP
    M = 2 * STATE
    group = mt * (HEADS // T) // (HEADS // GROUPS)

    barrier = pltpu.get_barrier_semaphore()
    for k in range(1, E):
        pl.semaphore_signal(barrier, inc=1, device_id={"ep": lax.rem(me + k, E)},
                            device_id_type=pl.DeviceIdType.MESH)
    for k in range(1, T):
        pl.semaphore_signal(barrier, inc=1, device_id={"tp": lax.rem(mt + k, T)},
                            device_id_type=pl.DeviceIdType.MESH)

    cols = pl.ds(pl.multiple_of(group * STATE, STATE), STATE)
    small = [
        (tokens_h, tokens), (mix_gain_h, mix_gain), (ids_h, ids), (step_weight_h, step_weight),
        (scores_h, scores), (step_bias_h, step_bias), (decay_log_h, decay_log), (skip_scale_h, skip_scale),
        (inner_taps_h, inner_taps), (access_taps_h.at[:, :, cols], access_taps), (inner_past_h, inner_past),
        (access_past_h.at[:, :, :, cols], access_past), (head_gain_h, head_gain), (moe_gain_h, moe_gain),
        (blend_vector_h, blend_vector), (access_past_h.at[:, 1:3], access_new.at[:, 0:2]),
    ]
    smalls = [pltpu.make_async_copy(a, b, small_sem.at[i]) for i, (a, b) in enumerate(small)]
    pairs = [
        (gate_w, gw), (inner_w, iw), (write_w.at[:, cols], ww), (read_w.at[:, cols], rw),
        (recurrent, rec), (mixer_w, mw), (dg_w, dg), (du_w, du), (eg_w, eg), (eu_w, eu),
        (dd_w, dd), (ed_w, ed),
    ]
    loads = [pltpu.make_async_copy(a, b, load_sem.at[i]) for i, (a, b) in enumerate(pairs)]
    for c in smalls + loads[:4]:
        c.start()

    Z = E // 2
    z, core = me // 2, lax.rem(me, 2)
    high = 2 * z // Z
    X = math.isqrt(T) if math.isqrt(T) ** 2 == T else T
    ty, tx = mt // X, lax.rem(mt, X)
    shifts = [(dy, dx) for dy in range(T // X) for dx in range(X)]
    by_reach = sorted(shifts[1:], key=lambda o: -(o[0] > 0) - (o[1] > 0))

    def across(o, sign=1):
        return lax.rem(ty + sign * o[0] + T // X, T // X) * X + lax.rem(tx + sign * o[1] + X, X)

    def in_order(i):
        return (1 - high) * (Z - i) + high * i

    def chip_at(dz, dc):
        return lax.rem(z + dz, Z) * 2 + lax.rem(core + dc, 2)

    sends = []

    def remote(src, dst, send, recv, device):
        c = pltpu.make_async_remote_copy(
            src_ref=src, dst_ref=dst, send_sem=send, recv_sem=recv,
            device_id=device, device_id_type=pl.DeviceIdType.MESH)
        c.start()
        sends.append(c)
        return c

    def expect(src, dst, send, recv, device):
        c = pltpu.make_async_remote_copy(
            src_ref=src, dst_ref=dst, send_sem=send, recv_sem=recv,
            device_id=device, device_id_type=pl.DeviceIdType.MESH)
        sends.append(c)
        return c

    def launch(src, dst, send, recv, device):
        pltpu.make_async_remote_copy(
            src_ref=src, dst_ref=dst, send_sem=send, recv_sem=recv,
            device_id=device, device_id_type=pl.DeviceIdType.MESH).start()

    def ep_expect(phase, src, dst):
        return [
            expect(src, dst, s_ep.at[phase, k], r_ep.at[phase, k], {"ep": chip_at(0, 1)}) for k in range(1, E)
        ]

    def ep_send(phase, src_of, dst):
        for i in range(1, Z):
            dz = in_order(i)
            for dc in range(2):
                to, k = chip_at(dz, dc), 2 * dz + dc
                launch(src_of(to), dst, s_ep.at[phase, k], r_ep.at[phase, k], {"ep": to})
        to = chip_at(0, 1)
        launch(src_of(to), dst, s_ep.at[phase, 1], r_ep.at[phase, 1], {"ep": to})
        return ep_expect(phase, src_of(to), dst)

    def tp_send(phase, src_of, dst):
        got = []
        for o in by_reach:
            to, k = across(o), shifts.index(o)
            got.append(remote(src_of(to), dst, s_tp.at[phase, k], r_tp.at[phase, k], {"tp": to}))
        return got

    def arrive(copies):
        for c in copies:
            c.wait_recv()

    lane = lax.broadcasted_iota(jnp.int32, (S, LANES), 1)
    lane_f = lane.astype(F32)
    row_i = lax.broadcasted_iota(jnp.int32, (S, S), 0)
    col_i = lax.broadcasted_iota(jnp.int32, (S, S), 1)
    diagonal = row_i == col_i
    earlier = jnp.where(col_i < row_i, 1.0, 0.0)

    def column(row):
        return jnp.sum(jnp.where(diagonal, row, 0.0), axis=-1, keepdims=True)

    for c in smalls[:3]:
        c.wait()
    tok = tokens[...].astype(F32)
    scale = lax.rsqrt(jnp.mean(tok * tok, axis=-1, keepdims=True) + EPS)
    normed = (tok * scale * mix_gain[...]).astype(BF)
    names = ids[...].astype(F32)
    name_a, name_b = column(names[0:1]), column(names[1:2])
    named = jnp.where((lane_f == name_a) | (lane_f == name_b), 1.0, 0.0)
    before = dot(earlier, named)
    rank = jnp.where(named > 0.0, before, -1.0)
    for j in range(E):
        xs[j] = normed[:, j * DC:(j + 1) * DC]
    xr[me] = xs[me]
    rk[...] = rank.astype(BF)
    rkr[me] = rk[...]
    pl.semaphore_wait(barrier, (E - 1) + (T - 1))
    ep_send(0, lambda to: xs.at[to], xr.at[me])
    got_k = ep_send(4, lambda to: rk, rkr.at[me])
    for c in loads[4:6]:
        c.start()

    for c in smalls[3:15]:
        c.wait()
    ranks = scores[...]
    first = 1.0 / (1.0 + jnp.exp(column(ranks[1:2]) - column(ranks[0:1])))
    combine = jnp.where(lane_f == name_a, first, 0.0) + jnp.where(lane_f == name_b, 1.0 - first, 0.0)
    slot = lax.broadcasted_iota(jnp.int32, (S, N), 1)
    slot_rank = lax.rem(slot, CAP).astype(F32)
    mix = jnp.zeros((S, N), F32)
    hits = jnp.zeros((S, N), F32)
    for e in range(E):
        hit = (slot // CAP == e) & (slot_rank == rank[:, e:e + 1])
        mix = jnp.where(hit, combine[:, e:e + 1], mix)
        hits = jnp.where(hit, 1.0, hits)
    mix_hi = mix.astype(BF)
    mix_lo = (mix - mix_hi.astype(F32)).astype(BF)

    picker = jnp.transpose(hits).astype(BF)

    taps_k = access_taps[...].astype(F32)
    tap_rows = [jnp.concatenate([taps_k[0, k:k + 1], taps_k[1, k:k + 1]], axis=0) for k in range(4)]
    row_of = lax.broadcasted_iota(jnp.int32, (S, STATE), 0)
    past_w = jnp.zeros((S, STATE), F32)
    past_r = jnp.zeros((S, STATE), F32)
    for s in range(S):
        total = access_past[s, 0].astype(F32) * tap_rows[0]
        for k in range(1, 3):
            total = total + access_past[s, k].astype(F32) * tap_rows[k]
        past_w = jnp.where(row_of == s, total[0:1], past_w)
        past_r = jnp.where(row_of == s, total[1:2], past_r)

    for c in loads[:4]:
        c.wait()
    G = M + LANES

    def project(dz):
        chip = lax.rem(z + Z - dz, Z)
        pair = pl.ds(2 * chip, 2)
        rows = xr[pair].reshape(2 * S, DC)
        step_p = lax.dot_general(
            rows, step_weight[...], (((1,), (1,)), ((), ())), preferred_element_type=F32)
        step_hi = step_p.astype(BF)
        step_lo = (step_p - step_hi.astype(F32)).astype(BF)
        ps[pair, :, 0:STATE] = dot(rows, ww[...]).astype(BF).reshape(2, S, STATE)
        ps[pair, :, STATE:M] = dot(rows, rw[...]).astype(BF).reshape(2, S, STATE)
        ps[pair, :, M:G] = jnp.concatenate(
            [step_hi, step_lo, jnp.zeros((2 * S, LANES - 2 * HEADS), BF)], axis=1).reshape(2, S, LANES)
        ps[pair, :, G:G + C] = dot(rows, iw[...]).astype(BF).reshape(2, S, C)
        pg[pair] = dot(rows, gw[...]).astype(BF).reshape(2, S, C)

    def answer(phase, src, dst, back, dc):
        to, k = chip_at(back, dc), 2 * back + dc
        launch(src.at[to], dst.at[me], s_ep.at[phase, k], r_ep.at[phase, k], {"ep": to})

    def normed_from(dz, dc):
        k = 2 * dz + dc
        return pltpu.make_async_remote_copy(
            src_ref=xs.at[0], dst_ref=xr.at[0], send_sem=s_ep.at[0, k], recv_sem=r_ep.at[0, k],
            device_id={"ep": chip_at(0, 1)}, device_id_type=pl.DeviceIdType.MESH)

    normed_from(0, 1).wait_recv()
    project(0)
    answer(1, ps, pr, 0, 1)
    answer(2, pg, pgr, 0, 1)
    pr[me] = ps[me]
    pgr[me] = pg[me]
    for i in range(1, Z):
        dz = in_order(i)
        for dc in range(2):
            normed_from(dz, dc).wait_recv()
        project(dz)
        for dc in range(2):
            answer(1, ps, pr, Z - dz, dc)
        for dc in range(2):
            answer(2, pg, pgr, Z - dz, dc)
    got = ep_expect(1, ps.at[0], pr.at[0])
    got_g = ep_expect(2, pg.at[0], pgr.at[0])
    for c in loads[6:]:
        c.start()
    arrive(got_k)

    every = rkr[...].reshape(E * S, LANES).astype(F32)
    expert_lane = lax.broadcasted_iota(jnp.int32, (E * S, LANES), 1)
    rank_of = jnp.sum(jnp.where(expert_lane == me, every, 0.0), axis=-1, keepdims=True)
    wide = lax.broadcasted_iota(jnp.int32, (E * S, N), 1)
    seq = lax.broadcasted_iota(jnp.int32, (E * S, N), 0)
    chosen = (wide // CAP == seq // S) & (lax.rem(wide, CAP).astype(F32) == rank_of)
    sel[...] = jnp.transpose(jnp.where(chosen, 1.0, 0.0)).astype(BF)

    chan = lax.broadcasted_iota(jnp.int32, (S, C), 1)
    head_of = mt * (HEADS // T) + chan // HEAD_DIM

    def expand(values):
        total = jnp.zeros((S, C), F32)
        for h in range(HEADS):
            total = jnp.where(head_of == h, values[:, h:h + 1], total)
        return total

    skip = expand(skip_scale[...])
    taps = inner_taps[...].astype(F32)
    past = inner_past[0].astype(F32) * taps[0:1]
    for k in range(1, 3):
        past = past + inner_past[k].astype(F32) * taps[k:k + 1]
        inner_new[k - 1] = inner_past[k]
    rate = jnp.exp(decay_log[...])
    loads[4].wait()

    @pl.loop(0, S)
    def _(t):
        value = rec[t]
        high = value.astype(BF)
        rcat[t, :, 0:STATE] = high
        rcat[t, :, STATE:M] = (value - high.astype(F32)).astype(BF)

    arrive(got)
    proj = pr[0].astype(F32)
    for j in range(1, E):
        proj = proj + pr[j].astype(F32)
    maps = proj[:, 0:M].astype(BF)
    step_raw = proj[:, M:M + HEADS] + proj[:, M + HEADS:M + 2 * HEADS]
    inner_part = proj[:, G:G + C].astype(BF)
    inner_new[2] = inner_part
    inner = silu(past + inner_part.astype(F32) * taps[3:4])
    mm[...] = maps
    maps_f = maps.astype(F32)
    write_c = silu(past_w + maps_f[:, 0:STATE] * tap_rows[3][0:1])
    read_c = silu(past_r + maps_f[:, STATE:M] * tap_rows[3][1:2])
    read_hi = read_c.astype(BF).astype(F32)
    read_lo = read_c - read_hi
    spare = LANES - 2 * S
    upper = jnp.concatenate([read_hi, read_lo, jnp.zeros((spare, STATE), F32)], axis=0)
    lower = jnp.concatenate([read_hi, jnp.zeros((spare + S, STATE), F32)], axis=0)
    reader = jnp.concatenate([jnp.transpose(upper), jnp.transpose(lower)], axis=0).astype(BF)
    step_x = step_raw + step_bias[...]
    step = jnp.maximum(step_x, 0.0) + jnp.log1p(jnp.exp(-jnp.abs(step_x)))
    decay = expand(jnp.exp(-step * rate))
    push = expand(step) * inner
    both = jnp.sum(write_c * read_c, axis=-1, keepdims=True)
    seq_lane = lax.rem(lax.broadcasted_iota(jnp.int32, (C, LANES), 1), S)
    read_t = jnp.zeros((C, LANES), F32)
    for t in range(S):
        read_t = jnp.where(seq_lane == t, dot(rcat[t], reader), read_t)
    read_rows = jnp.transpose(read_t)
    recalled = read_rows[0:S] + read_rows[S:2 * S]
    readout = decay * recalled + push * both + skip * inner
    arrive(got_g)
    gate_sum = pgr[0].astype(F32)
    for j in range(1, E):
        gate_sum = gate_sum + pgr[j].astype(F32)
    gated = readout * silu(gate_sum.astype(BF).astype(F32))
    square = gated * gated
    norm = jnp.zeros((S, C), F32)
    for h in range(C // HEAD_DIM):
        here = chan // HEAD_DIM == h
        mean = jnp.sum(jnp.where(here, square, 0.0), axis=-1, keepdims=True) / HEAD_DIM
        norm = jnp.where(here, lax.rsqrt(mean + EPS), norm)
    head_out = (gated * norm * head_gain[...]).astype(BF)
    loads[5].wait()
    for j in range(T):
        ms[:, j * DS:(j + 1) * DS] = dot(head_out, mw[:, j * DS:(j + 1) * DS]).astype(BF)
    mr[mt] = ms[...]
    got = tp_send(0, lambda to: ms, mr.at[mt])
    mmr[mt] = mm[...]
    got_m = tp_send(1, lambda to: mm, mmr.at[mt])

    decay_t = jnp.transpose(decay)
    push_t = jnp.transpose(push)
    for t in range(S):
        nrec[t] = decay_t[:, t:t + 1] * rec[t] + push_t[:, t:t + 1] * write_c[t:t + 1]

    arrive(got)
    mixed = mr[0].astype(F32)
    for j in range(1, T):
        mixed = mixed + mr[j].astype(F32)
    resid = tok + mixed.astype(BF).astype(F32)
    scale = lax.rsqrt(jnp.mean(resid * resid, axis=-1, keepdims=True) + EPS)
    hidden = (resid * scale * moe_gain[...]).astype(BF)
    for q in range(T):
        rbuf[q] = resid[:, q * DS:(q + 1) * DS]
        hbuf[q, me] = hidden[:, q * DS:(q + 1) * DS]

    twin = chip_at(0, 1)
    for i in range(1, Z):
        dz = in_order(i)
        launch(hbuf.at[mt, me], hbuf.at[mt, me], s_h.at[2 * dz], r_h.at[2 * dz], {"ep": chip_at(dz, 0)})
    beside = remote(hbuf.at[mt, me], hbuf.at[mt, me], s_h.at[1], r_h.at[1], {"ep": twin})
    for q in range(T):
        chosen_q = dot(picker, hidden[:, q * DS:(q + 1) * DS])
        for e in range(E):
            cs[q, e] = chosen_q[e * CAP:(e + 1) * CAP].astype(BF)
    got_c = []
    for o in by_reach:
        q, n = across(o), shifts.index(o)
        cr[q, me] = cs[q, me]
        for i in range(1, Z + 1):
            dz = in_order(i) if i < Z else 0
            for dc in range(2):
                if i < Z or dc > 0:
                    to, k = chip_at(dz, dc), 2 * dz + dc
                    launch(cs.at[q, to], cr.at[q, me], s_c.at[n, k], r_c.at[n, k], {"ep": to})
        got_c.append([
            expect(cs.at[q, 0], cr.at[q, 0], s_c.at[n, k], r_c.at[n, k], {"ep": twin}) for k in range(1, E)
        ])

    scorer = blend_vector[...].astype(F32)
    blend = jnp.zeros((S, LANES), F32)
    for j in range(D // LANES):
        blend = blend + hidden[:, j * LANES:(j + 1) * LANES].astype(F32) * scorer[j:j + 1]
    blend = jnp.sum(blend, axis=-1, keepdims=True)
    blend = 1.0 / (1.0 + jnp.exp(-blend))

    arrive(got_m)
    smalls[15].wait()
    owners = [mmr[g * max(1, T // GROUPS)].astype(F32) for g in range(GROUPS)]
    for s in range(S):
        for g in range(GROUPS):
            pair = jnp.concatenate([owners[g][s:s + 1, 0:STATE], owners[g][s:s + 1, STATE:M]], axis=0)
            access_new[s, 2, :, g * STATE:(g + 1) * STATE] = pair.astype(BF)

    def piece(dz, dc):
        k = 2 * dz + dc
        block = hbuf.at[mt, chip_at(Z - dz, dc)]
        return pltpu.make_async_remote_copy(
            src_ref=block, dst_ref=block, send_sem=s_h.at[k], recv_sem=r_h.at[k],
            device_id={"ep": twin}, device_id_type=pl.DeviceIdType.MESH)

    def relay(i):
        dz = in_order(i)
        piece(dz, 0).wait_recv()
        block = hbuf.at[mt, chip_at(Z - dz, 0)]
        launch(block, block, s_h.at[2 * dz + 1], r_h.at[2 * dz + 1], {"ep": twin})

    def passed(i):
        piece(in_order(i), 1).wait_recv()

    Q = 2 * S // T

    def dense_part(dz):
        chip = lax.rem(z + Z - dz, Z)
        here = hbuf[mt, pl.ds(2 * chip, 2)].reshape(2 * S, DS)
        for w, weight in enumerate((dg, du)):
            part = dot(here, weight[...])
            for m in range(T):
                dps[chip, m, w] = part[m * Q:(m + 1) * Q].astype(BF)
        for o in by_reach:
            to, k = across(o), shifts.index(o)
            launch(dps.at[chip, to], dpr.at[mt, chip], s_d.at[k, dz], r_d.at[k, dz], {"tp": to})
        dpr[mt, chip] = dps[chip, mt]

    def expert_part(picked, q, first, last):
        rows_q = pl.ds(pl.multiple_of(q * DS, DS), DS)
        for n in range(FFL // tile):
            at = slice(n * tile, (n + 1) * tile)
            g = dot(picked, eg[rows_q, at])
            u = dot(picked, eu[rows_q, at])
            if not first:
                g = g + gacc[:, at]
                u = u + uacc[:, at]
            if last:
                actb[:, at] = (silu(g) * u).astype(BF)
            else:
                gacc[:, at] = g
                uacc[:, at] = u

    tile = tile_of(FFL)
    for c in loads[6:8]:
        c.wait()
    beside.wait_recv()
    dense_part(0)
    for i in range(1, Z):
        relay(i)
        if i > 1:
            passed(i - 1)
            dense_part(in_order(i - 1))
    passed(Z - 1)
    dense_part(in_order(Z - 1))
    got_d = [
        expect(dps.at[0, 0], dpr.at[0, 0], s_d.at[k, d], r_d.at[k, d], {"tp": lax.rem(mt + k, T)})
        for k in range(1, T) for d in range(Z)
    ]
    for c in loads[8:10]:
        c.wait()
    own = dot(sel[...], hbuf[mt].reshape(E * S, DS)).astype(BF)
    expert_part(own, mt, True, T == 1)
    for n, o in enumerate(by_reach):
        q = across(o)
        arrive(got_c[n])
        picked = cr[q].astype(F32).reshape(N, DS).astype(BF)
        expert_part(picked, q, False, n == len(by_reach) - 1)

    def dense_act():
        arrive(got_d)
        for chip in range(Z):
            dsum = dpr[0, chip].astype(F32)
            for j in range(1, T):
                dsum = dsum + dpr[j, chip].astype(F32)
            dab[mt, chip] = (silu(dsum[0]) * dsum[1]).astype(BF)
        return tp_send(2, lambda to: dab.at[mt], dab.at[mt])

    loads[11].wait()
    got_e = []
    got_a = None
    dtile = tile_of(DS)
    for o in by_reach + shifts[:1]:
        to, k = across(o), shifts.index(o)
        for n in range(DS // dtile):
            at = pl.ds(pl.multiple_of(to * DS + n * dtile, dtile), dtile)
            share = dot(actb[...], ed[:, at])
            for s in range(E):
                es[k, s, :, n * dtile:(n + 1) * dtile] = share[s * CAP:(s + 1) * CAP].astype(BF)
        for i in range(1, Z + 1):
            dz = in_order(i) if i < Z else 0
            for dc in range(2):
                owner, d = chip_at(dz, dc), 2 * dz + dc
                if i == Z and dc == 0 and k == 0:
                    er[0, me] = es[0, me]
                else:
                    launch(es.at[k, owner], er.at[k, me], s_x.at[k, d], r_x.at[k, d], {"ep": owner, "tp": to})
        for d in range(E):
            if k > 0 or d > 0:
                got_e.append(expect(es.at[k, 0], er.at[k, 0], s_x.at[k, d], r_x.at[k, d], {"ep": twin, "tp": to}))
        if o == by_reach[min(1, T - 2)]:
            got_a = dense_act()
    loads[10].wait()
    arrive(got_a)
    shares = dot(dab[...].astype(F32).reshape(E * S, U).astype(BF), dd[...])
    for m in range(T):
        for chip in range(Z):
            base = (m * Z + chip) * Q
            fs[2 * chip + m * Q // S, m * Q % S:m * Q % S + Q] = shares[base:base + Q].astype(BF)
    fr[me] = fs[me]
    got = ep_send(3, lambda to: fs.at[to], fr.at[me])
    arrive(got_e)
    total = er[0].astype(F32)
    for k in range(1, T):
        total = total + er[k].astype(F32)
    outs = total.reshape(N, DS).astype(BF)
    final = rbuf[mt] + dot(mix_hi, outs) + dot(mix_lo, outs)
    arrive(got)
    dense = fr[0].astype(F32)
    for j in range(1, E):
        dense = dense + fr[j].astype(F32)
    out[...] = final + blend * dense
    for k in range(2, E):
        piece(k // 2, k % 2).wait_send()
    for c in sends:
        c.wait_send()


def finish(out, rec, inner, access, out_o, rec_o, inner_o, access_o, sem):
    S = rec.shape[0]
    parts = 4 if S % 4 == 0 else 1
    size = S // parts
    copies = [
        pltpu.make_async_copy(rec.at[i * size:(i + 1) * size], rec_o.at[i * size:(i + 1) * size], sem.at[i])
        for i in range(parts)
    ]
    for i, (a, b) in enumerate([(out, out_o), (inner, inner_o), (access, access_o)]):
        copies.append(pltpu.make_async_copy(a, b, sem.at[parts + i]))
    for c in copies:
        c.start()
    for c in copies:
        c.wait()


def local(
    E, T,
    tokens, mix_gain, gate_weight, inner_weight, write_weight, read_weight, step_weight, step_bias,
    decay_log, skip_scale, inner_taps, access_taps, inner_history, access_history, recurrent,
    head_gain, mixer_out, moe_gain, expert_ids, route_scores, expert_gate, expert_up, expert_down,
    blend_vector, dense_gate, dense_up, dense_down,
):
    S, D = tokens.shape
    C = gate_weight.shape[1]
    DC, DS = D // E, D // T
    U = dense_gate.shape[1]
    FFL = expert_gate.shape[2]
    GS = access_taps.shape[2]
    rows = E * S
    Z = E // 2
    Q = 2 * S // T
    M = 2 * STATE
    PW = M + LANES + C
    CAP = max(1, 2 * TOP * S // E)
    N = E * CAP
    vmem = pl.BlockSpec(memory_space=pltpu.VMEM)
    hbm = pl.BlockSpec(memory_space=pltpu.HBM)
    V = pltpu.VMEM
    DMA = pltpu.SemaphoreType.DMA
    shapes = (
        jax.ShapeDtypeStruct((S, DS), F32),
        jax.ShapeDtypeStruct((S, C, STATE), F32),
        jax.ShapeDtypeStruct((3, S, C), BF),
        jax.ShapeDtypeStruct((S, 3, 2, GS), BF),
    )
    held = tuple(pltpu.VMEM(x.shape, x.dtype) for x in shapes)
    operands = (
        tokens, mix_gain[None], step_weight.T, step_bias[None], decay_log[None], skip_scale[None],
        inner_taps, access_taps, inner_history.transpose(1, 0, 2), access_history.transpose(0, 2, 1, 3),
        head_gain[None], moe_gain[None], expert_ids.T, route_scores.T, blend_vector.reshape(-1, LANES),
        gate_weight, inner_weight, write_weight, read_weight,
        recurrent.reshape(S, C, STATE), mixer_out,
        expert_gate[0], expert_up[0], expert_down[0], dense_gate, dense_up, dense_down,
    )
    results = pl.pallas_call(
        functools.partial(kernel, E, T, CAP),
        name="decode_step",
        out_shape=held,
        in_specs=[hbm] * 27,
        out_specs=(vmem,) * 4,
        scratch_shapes=[
            V((S, D), BF), V((1, D), F32), V((HEADS, DC), BF), V((1, HEADS), F32), V((1, HEADS), F32),
            V((1, HEADS), F32), V((4, C), BF), V((2, 4, STATE), BF), V((3, S, C), BF), V((S, 3, 2, STATE), BF),
            V((1, C), F32), V((1, D), F32), V((TOP, S), jnp.int32), V((TOP, S), F32), V((D // LANES, LANES), BF),
            V((DC, C), BF), V((DC, C), BF), V((DC, STATE), BF), V((DC, STATE), BF),
            V((S, C, STATE), F32), V((C, D), BF),
            V((D, FFL), BF), V((D, FFL), BF), V((FFL, D), BF),
            V((DS, U), BF), V((DS, U), BF), V((U, DS), BF),
            V((E, S, DC), BF), V((E, S, DC), BF), V((S, LANES), BF), V((E, S, LANES), BF), V((E, S, PW), BF), V((E, S, PW), BF),
            V((E, S, C), BF), V((E, S, C), BF), V((S, C, M), BF),
            V((S, D), BF), V((T, S, D), BF), V((S, M), BF), V((T, S, M), BF),
            V((T, S, DS), F32), V((T, E, S, DS), BF),
            V((N, rows), BF), V((T, E, CAP, DS), BF), V((T, E, CAP, DS), BF), V((N, FFL), F32), V((N, FFL), F32), V((N, FFL), BF),
            V((Z, T, 2, Q, U), BF), V((T, Z, 2, Q, U), BF), V((T, Z, Q, U), BF),
            V((T, E, CAP, DS), BF), V((T, E, CAP, DS), BF),
            V((E, S, DS), BF), V((E, S, DS), BF),
            DMA((16,)), DMA((12,)), DMA((5, E)), DMA((5, E)), DMA((4, T)), DMA((4, T)),
            DMA((E,)), DMA((E,)), DMA((T, E)), DMA((T, E)), DMA((T, E)), DMA((T, E)), DMA((T, Z)), DMA((T, Z)),
        ],
        compiler_params=pltpu.CompilerParams(
            collective_id=0, has_side_effects=True, vmem_limit_bytes=40 * 1024 * 1024
        ),
    )(*[pltpu.with_memory_space_constraint(x, pltpu.HBM) for x in operands])
    out, new_recurrent, inner_new, access_new = pl.pallas_call(
        finish,
        name="store_results",
        out_shape=shapes,
        in_specs=[vmem] * 4,
        out_specs=(hbm,) * 4,
        scratch_shapes=[DMA((8,))],
    )(*[pltpu.with_memory_space_constraint(x, pltpu.VMEM) for x in results])
    return (
        out, new_recurrent.reshape(recurrent.shape), inner_new.transpose(1, 0, 2),
        access_new.transpose(0, 2, 1, 3),
    )


def solution(mesh):
    in_specs = (
        P("ep", None), P(), P("ep", "tp"), P("ep", "tp"), P("ep", None), P("ep", None),
        P("ep", None), P(), P(), P(), P(None, "tp"), P(), P("ep", None, "tp"),
        P("ep", None, None, None), P("ep", "tp", None, None), P("tp"), P("tp", None), P(),
        P("ep", None), P("ep", None), P("ep", None, "tp"), P("ep", None, "tp"),
        P("ep", "tp", None), P(), P("tp", "ep"), P("tp", "ep"), P("ep", "tp"),
    )
    out_specs = (
        P("ep", "tp"), P("ep", "tp", None, None), P("ep", None, "tp"), P("ep", None, None, None),
    )
    body = functools.partial(local, mesh.shape["ep"], mesh.shape["tp"])
    return jax.shard_map(body, mesh=mesh, in_specs=in_specs, out_specs=out_specs, check_vma=False)
```

```python
import functools
import math

import jax
import jax.numpy as jnp
from jax import lax
from jax.experimental import pallas as pl
from jax.experimental.pallas import tpu as pltpu
from jax.sharding import PartitionSpec as P

HEADS = 16
HEAD_DIM = 64
GROUPS = 4
STATE = 128
LANES = 128
TOP = 2
EPS = 1e-06
BF = jnp.bfloat16
F32 = jnp.float32


def dot(a, b):
    return jnp.dot(a, b, preferred_element_type=F32)


def silu(x):
    return x * (1.0 / (1.0 + jnp.exp(-x)))


def tile_of(extent):
    return 256 if extent % 256 == 0 else extent


def kernel(
    E, T, CAP,
    tokens_h, mix_gain_h, step_weight_h, step_bias_h, decay_log_h, skip_scale_h, inner_taps_h, access_taps_h,
    inner_past_h, access_past_h, head_gain_h, moe_gain_h, ids_h, scores_h, blend_vector_h,
    gate_w, inner_w, write_w, read_w, recurrent, mixer_w, eg_w, eu_w, ed_w, dg_w, du_w, dd_w,
    out_k, nrec_k, inner_k, access_k,
    out, nrec, inner_new, access_new,
    tokens, mix_gain, step_weight, step_bias, decay_log, skip_scale, inner_taps, access_taps,
    inner_past, access_past, head_gain, moe_gain, ids, scores, blend_vector,
    gw, iw, ww, rw, rec, mw, eg, eu, ed, dg, du, dd,
    xs, xr, rk, rkr, ps, pr, pg, pgr, rcat, ms, mr, mm, mmr, rbuf, hbuf, sel, cs, cr, gacc, uacc, actb, dps, dpr, dab, es, er, fs, fr,
    keep_sem, small_sem, load_sem, sent, r_one, r_n, r_h, r_c, r_d, r_a, r_e,
):
    me = lax.axis_index("ep")
    mt = lax.axis_index("tp")
    S, D = tokens.shape
    C = gw.shape[1]
    DC = D // E
    DS = D // T
    U = dg.shape[1]
    FFL = eg.shape[1]
    N = E * CAP
    M = 2 * STATE
    group = mt * (HEADS // T) // (HEADS // GROUPS)

    barrier = pltpu.get_barrier_semaphore()
    for k in range(1, E):
        pl.semaphore_signal(barrier, inc=1, device_id={"ep": lax.rem(me + k, E)},
                            device_id_type=pl.DeviceIdType.MESH)
    for k in range(1, T):
        pl.semaphore_signal(barrier, inc=1, device_id={"tp": lax.rem(mt + k, T)},
                            device_id_type=pl.DeviceIdType.MESH)

    cols = pl.ds(pl.multiple_of(group * STATE, STATE), STATE)
    small = [
        (tokens_h, tokens), (mix_gain_h, mix_gain), (ids_h, ids), (step_weight_h, step_weight),
        (scores_h, scores), (step_bias_h, step_bias), (decay_log_h, decay_log), (skip_scale_h, skip_scale),
        (inner_taps_h, inner_taps), (access_taps_h.at[:, :, cols], access_taps), (inner_past_h, inner_past),
        (access_past_h.at[:, :, :, cols], access_past), (head_gain_h, head_gain), (moe_gain_h, moe_gain),
        (blend_vector_h, blend_vector), (access_past_h.at[:, 1:3], access_new.at[:, 0:2]),
    ]
    smalls = [pltpu.make_async_copy(a, b, small_sem.at[i]) for i, (a, b) in enumerate(small)]
    pairs = [
        (gate_w, gw), (inner_w, iw), (write_w.at[:, cols], ww), (read_w.at[:, cols], rw),
        (recurrent, rec), (mixer_w, mw), (dg_w, dg), (du_w, du), (eg_w, eg), (eu_w, eu),
        (dd_w, dd), (ed_w, ed),
    ]
    loads = [pltpu.make_async_copy(a, b, load_sem.at[i]) for i, (a, b) in enumerate(pairs)]
    for c in smalls + loads[:4]:
        c.start()

    Z = E // 2
    z, core = me // 2, lax.rem(me, 2)
    high = 2 * z // Z
    X = math.isqrt(T) if math.isqrt(T) ** 2 == T else T
    ty, tx = mt // X, lax.rem(mt, X)
    shifts = [(dy, dx) for dy in range(T // X) for dx in range(X)]
    by_reach = sorted(shifts[1:], key=lambda o: -(o[0] > 0) - (o[1] > 0))

    def across(o, sign=1):
        return lax.rem(ty + sign * o[0] + T // X, T // X) * X + lax.rem(tx + sign * o[1] + X, X)

    def in_order(i):
        return (1 - high) * (Z - i) + high * i

    def chip_at(dz, dc):
        return lax.rem(z + dz, Z) * 2 + lax.rem(core + dc, 2)

    keeps = [
        pltpu.make_async_copy(a, b, keep_sem.at[i])
        for i, (a, b) in enumerate([(out, out_k), (nrec, nrec_k), (inner_new, inner_k), (access_new, access_k)])
    ]
    NORM, RANK, MAPS, GATE, MIXED, GROUP, HID, PICK, PART, ACT, FAR, NEAR, DENSE = range(13)

    def copy(src, dst, kind, recv, device):
        return pltpu.make_async_remote_copy(
            src_ref=src, dst_ref=dst, send_sem=sent.at[kind], recv_sem=recv,
            device_id=device, device_id_type=pl.DeviceIdType.MESH)

    def launch(*args):
        copy(*args).start()

    def arrive(ref, recv):
        copy(ref, ref, NORM, recv, {"ep": chip_at(0, 1)}).wait_recv()

    def leave(ref, kind):
        copy(ref, ref, kind, r_one.at[0], {"ep": chip_at(0, 1)}).wait_send()

    def ep_send(kind, src_of, dst, recv):
        for i in range(1, Z):
            dz = in_order(i)
            for dc in range(2):
                to = chip_at(dz, dc)
                launch(src_of(to), dst, kind, recv(dz), {"ep": to})
        to = chip_at(0, 1)
        launch(src_of(to), dst, kind, recv(0), {"ep": to})

    def tp_send(kind, src, dst, recv):
        for o in by_reach:
            launch(src, dst, kind, recv, {"tp": across(o)})

    lane = lax.broadcasted_iota(jnp.int32, (S, LANES), 1)
    lane_f = lane.astype(F32)
    row_i = lax.broadcasted_iota(jnp.int32, (S, S), 0)
    col_i = lax.broadcasted_iota(jnp.int32, (S, S), 1)
    diagonal = row_i == col_i
    earlier = jnp.where(col_i < row_i, 1.0, 0.0)

    def column(row):
        return jnp.sum(jnp.where(diagonal, row, 0.0), axis=-1, keepdims=True)

    for c in smalls[:3]:
        c.wait()
    tok = tokens[...].astype(F32)
    scale = lax.rsqrt(jnp.mean(tok * tok, axis=-1, keepdims=True) + EPS)
    normed = (tok * scale * mix_gain[...]).astype(BF)
    names = ids[...].astype(F32)
    name_a, name_b = column(names[0:1]), column(names[1:2])
    named = jnp.where((lane_f == name_a) | (lane_f == name_b), 1.0, 0.0)
    before = dot(earlier, named)
    rank = jnp.where(named > 0.0, before, -1.0)
    for j in range(E):
        xs[j] = normed[:, j * DC:(j + 1) * DC]
    xr[me] = xs[me]
    rk[...] = rank.astype(BF)
    rkr[me] = rk[...]
    pl.semaphore_wait(barrier, (E - 1) + (T - 1))
    ep_send(NORM, lambda to: xs.at[to], xr.at[me], lambda dz: r_n.at[dz])
    ep_send(RANK, lambda to: rk, rkr.at[me], lambda dz: r_one.at[0])
    for c in loads[4:6]:
        c.start()

    for c in smalls[3:15]:
        c.wait()
    ranks = scores[...]
    first = 1.0 / (1.0 + jnp.exp(column(ranks[1:2]) - column(ranks[0:1])))
    combine = jnp.where(lane_f == name_a, first, 0.0) + jnp.where(lane_f == name_b, 1.0 - first, 0.0)
    slot = lax.broadcasted_iota(jnp.int32, (S, N), 1)
    slot_rank = lax.rem(slot, CAP).astype(F32)
    mix = jnp.zeros((S, N), F32)
    hits = jnp.zeros((S, N), F32)
    for e in range(E):
        hit = (slot // CAP == e) & (slot_rank == rank[:, e:e + 1])
        mix = jnp.where(hit, combine[:, e:e + 1], mix)
        hits = jnp.where(hit, 1.0, hits)
    mix_hi = mix.astype(BF)
    mix_lo = (mix - mix_hi.astype(F32)).astype(BF)

    picker = jnp.transpose(hits).astype(BF)

    taps_k = access_taps[...].astype(F32)
    tap_rows = [jnp.concatenate([taps_k[0, k:k + 1], taps_k[1, k:k + 1]], axis=0) for k in range(4)]
    row_of = lax.broadcasted_iota(jnp.int32, (S, STATE), 0)
    past_w = jnp.zeros((S, STATE), F32)
    past_r = jnp.zeros((S, STATE), F32)
    for s in range(S):
        total = access_past[s, 0].astype(F32) * tap_rows[0]
        for k in range(1, 3):
            total = total + access_past[s, k].astype(F32) * tap_rows[k]
        past_w = jnp.where(row_of == s, total[0:1], past_w)
        past_r = jnp.where(row_of == s, total[1:2], past_r)

    for c in loads[:4]:
        c.wait()
    G = M + LANES

    def project(dz):
        chip = lax.rem(z + Z - dz, Z)
        pair = pl.ds(2 * chip, 2)
        rows = xr[pair].reshape(2 * S, DC)
        step_p = lax.dot_general(
            rows, step_weight[...], (((1,), (1,)), ((), ())), preferred_element_type=F32)
        step_hi = step_p.astype(BF)
        step_lo = (step_p - step_hi.astype(F32)).astype(BF)
        ps[pair, :, 0:STATE] = dot(rows, ww[...]).astype(BF).reshape(2, S, STATE)
        ps[pair, :, STATE:M] = dot(rows, rw[...]).astype(BF).reshape(2, S, STATE)
        ps[pair, :, M:G] = jnp.concatenate(
            [step_hi, step_lo, jnp.zeros((2 * S, LANES - 2 * HEADS), BF)], axis=1).reshape(2, S, LANES)
        ps[pair, :, G:G + C] = dot(rows, iw[...]).astype(BF).reshape(2, S, C)
        pg[pair] = dot(rows, gw[...]).astype(BF).reshape(2, S, C)

    def answer(kind, src, dst, recv, back, dc):
        to = chip_at(back, dc)
        launch(src.at[to], dst.at[me], kind, recv, {"ep": to})

    arrive(xr.at[0], r_n.at[0])
    project(0)
    answer(MAPS, ps, pr, r_one.at[1], 0, 1)
    answer(GATE, pg, pgr, r_one.at[2], 0, 1)
    pr[me] = ps[me]
    pgr[me] = pg[me]
    for i in range(1, Z):
        dz = in_order(i)
        arrive(xr.at[0:2], r_n.at[dz])
        project(dz)
        for dc in range(2):
            answer(MAPS, ps, pr, r_one.at[1], Z - dz, dc)
        for dc in range(2):
            answer(GATE, pg, pgr, r_one.at[2], Z - dz, dc)
    for c in loads[6:]:
        c.start()
    arrive(rkr.at[0:E - 1], r_one.at[0])

    every = rkr[...].reshape(E * S, LANES).astype(F32)
    expert_lane = lax.broadcasted_iota(jnp.int32, (E * S, LANES), 1)
    rank_of = jnp.sum(jnp.where(expert_lane == me, every, 0.0), axis=-1, keepdims=True)
    wide = lax.broadcasted_iota(jnp.int32, (E * S, N), 1)
    seq = lax.broadcasted_iota(jnp.int32, (E * S, N), 0)
    chosen = (wide // CAP == seq // S) & (lax.rem(wide, CAP).astype(F32) == rank_of)
    sel[...] = jnp.transpose(jnp.where(chosen, 1.0, 0.0)).astype(BF)

    chan = lax.broadcasted_iota(jnp.int32, (S, C), 1)
    head_of = mt * (HEADS // T) + chan // HEAD_DIM

    def expand(values):
        total = jnp.zeros((S, C), F32)
        for h in range(HEADS):
            total = jnp.where(head_of == h, values[:, h:h + 1], total)
        return total

    skip = expand(skip_scale[...])
    taps = inner_taps[...].astype(F32)
    past = inner_past[0].astype(F32) * taps[0:1]
    for k in range(1, 3):
        past = past + inner_past[k].astype(F32) * taps[k:k + 1]
        inner_new[k - 1] = inner_past[k]
    rate = jnp.exp(decay_log[...])
    loads[4].wait()

    @pl.loop(0, S)
    def _(t):
        value = rec[t]
        high = value.astype(BF)
        rcat[t, :, 0:STATE] = high
        rcat[t, :, STATE:M] = (value - high.astype(F32)).astype(BF)

    arrive(pr.at[0:E - 1], r_one.at[1])
    proj = pr[0].astype(F32)
    for j in range(1, E):
        proj = proj + pr[j].astype(F32)
    maps = proj[:, 0:M].astype(BF)
    step_raw = proj[:, M:M + HEADS] + proj[:, M + HEADS:M + 2 * HEADS]
    inner_part = proj[:, G:G + C].astype(BF)
    inner_new[2] = inner_part
    inner = silu(past + inner_part.astype(F32) * taps[3:4])
    mm[...] = maps
    maps_f = maps.astype(F32)
    write_c = silu(past_w + maps_f[:, 0:STATE] * tap_rows[3][0:1])
    read_c = silu(past_r + maps_f[:, STATE:M] * tap_rows[3][1:2])
    read_hi = read_c.astype(BF).astype(F32)
    read_lo = read_c - read_hi
    spare = LANES - 2 * S
    upper = jnp.concatenate([read_hi, read_lo, jnp.zeros((spare, STATE), F32)], axis=0)
    lower = jnp.concatenate([read_hi, jnp.zeros((spare + S, STATE), F32)], axis=0)
    reader = jnp.concatenate([jnp.transpose(upper), jnp.transpose(lower)], axis=0).astype(BF)
    step_x = step_raw + step_bias[...]
    step = jnp.maximum(step_x, 0.0) + jnp.log1p(jnp.exp(-jnp.abs(step_x)))
    decay = expand(jnp.exp(-step * rate))
    push = expand(step) * inner
    both = jnp.sum(write_c * read_c, axis=-1, keepdims=True)
    seq_lane = lax.rem(lax.broadcasted_iota(jnp.int32, (C, LANES), 1), S)
    read_t = jnp.zeros((C, LANES), F32)
    for t in range(S):
        read_t = jnp.where(seq_lane == t, dot(rcat[t], reader), read_t)
    read_rows = jnp.transpose(read_t)
    recalled = read_rows[0:S] + read_rows[S:2 * S]
    readout = decay * recalled + push * both + skip * inner
    arrive(pgr.at[0:E - 1], r_one.at[2])
    gate_sum = pgr[0].astype(F32)
    for j in range(1, E):
        gate_sum = gate_sum + pgr[j].astype(F32)
    gated = readout * silu(gate_sum.astype(BF).astype(F32))
    square = gated * gated
    norm = jnp.zeros((S, C), F32)
    for h in range(C // HEAD_DIM):
        here = chan // HEAD_DIM == h
        mean = jnp.sum(jnp.where(here, square, 0.0), axis=-1, keepdims=True) / HEAD_DIM
        norm = jnp.where(here, lax.rsqrt(mean + EPS), norm)
    head_out = (gated * norm * head_gain[...]).astype(BF)
    loads[5].wait()
    for j in range(T):
        ms[:, j * DS:(j + 1) * DS] = dot(head_out, mw[:, j * DS:(j + 1) * DS]).astype(BF)
    mr[mt] = ms[...]
    tp_send(MIXED, ms, mr.at[mt], r_one.at[3])
    mmr[mt] = mm[...]
    tp_send(GROUP, mm, mmr.at[mt], r_one.at[4])

    decay_t = jnp.transpose(decay)
    push_t = jnp.transpose(push)
    for t in range(S):
        nrec[t] = decay_t[:, t:t + 1] * rec[t] + push_t[:, t:t + 1] * write_c[t:t + 1]
    keeps[1].start()
    keeps[2].start()

    arrive(mr.at[0:T - 1], r_one.at[3])
    mixed = mr[0].astype(F32)
    for j in range(1, T):
        mixed = mixed + mr[j].astype(F32)
    resid = tok + mixed.astype(BF).astype(F32)
    scale = lax.rsqrt(jnp.mean(resid * resid, axis=-1, keepdims=True) + EPS)
    hidden = (resid * scale * moe_gain[...]).astype(BF)
    for q in range(T):
        rbuf[q] = resid[:, q * DS:(q + 1) * DS]
        hbuf[q, me] = hidden[:, q * DS:(q + 1) * DS]

    twin = chip_at(0, 1)
    for i in range(1, Z):
        dz = in_order(i)
        launch(hbuf.at[mt, me], hbuf.at[mt, me], HID, r_h.at[2 * dz], {"ep": chip_at(dz, 0)})
    launch(hbuf.at[mt, me], hbuf.at[mt, me], HID, r_h.at[1], {"ep": twin})
    for q in range(T):
        chosen_q = dot(picker, hidden[:, q * DS:(q + 1) * DS])
        for e in range(E):
            cs[q, e] = chosen_q[e * CAP:(e + 1) * CAP].astype(BF)
    for o in by_reach:
        q, n = across(o), shifts.index(o)
        cr[q, me] = cs[q, me]
        for i in range(1, Z + 1):
            dz = in_order(i) if i < Z else 0
            for dc in range(2):
                if i < Z or dc > 0:
                    to = chip_at(dz, dc)
                    launch(cs.at[q, to], cr.at[q, me], PICK, r_c.at[n], {"ep": to})

    scorer = blend_vector[...].astype(F32)
    blend = jnp.zeros((S, LANES), F32)
    for j in range(D // LANES):
        blend = blend + hidden[:, j * LANES:(j + 1) * LANES].astype(F32) * scorer[j:j + 1]
    blend = jnp.sum(blend, axis=-1, keepdims=True)
    blend = 1.0 / (1.0 + jnp.exp(-blend))

    arrive(mmr.at[0:T - 1], r_one.at[4])
    smalls[15].wait()
    owners = [mmr[g * max(1, T // GROUPS)].astype(F32) for g in range(GROUPS)]
    for s in range(S):
        for g in range(GROUPS):
            pair = jnp.concatenate([owners[g][s:s + 1, 0:STATE], owners[g][s:s + 1, STATE:M]], axis=0)
            access_new[s, 2, :, g * STATE:(g + 1) * STATE] = pair.astype(BF)
    keeps[3].start()

    def relay(i):
        dz = in_order(i)
        block = hbuf.at[mt, chip_at(Z - dz, 0)]
        arrive(block, r_h.at[2 * dz])
        launch(block, block, HID, r_h.at[2 * dz + 1], {"ep": twin})

    def passed(i):
        dz = in_order(i)
        arrive(hbuf.at[mt, chip_at(Z - dz, 1)], r_h.at[2 * dz + 1])

    Q = 2 * S // T

    def dense_part(dz):
        chip = lax.rem(z + Z - dz, Z)
        here = hbuf[mt, pl.ds(2 * chip, 2)].reshape(2 * S, DS)
        for w, weight in enumerate((dg, du)):
            part = dot(here, weight[...])
            for m in range(T):
                dps[chip, m, w] = part[m * Q:(m + 1) * Q].astype(BF)
        for o in by_reach:
            to = across(o)
            launch(dps.at[chip, to], dpr.at[mt, chip], PART, r_d.at[dz], {"tp": to})
        dpr[mt, chip] = dps[chip, mt]

    def dense_act(dz):
        chip = lax.rem(z + Z - dz, Z)
        arrive(dpr.at[0:T - 1, 0], r_d.at[dz])
        dsum = dpr[0, chip].astype(F32)
        for j in range(1, T):
            dsum = dsum + dpr[j, chip].astype(F32)
        dab[mt, chip] = (silu(dsum[0]) * dsum[1]).astype(BF)
        for o in by_reach:
            launch(dab.at[mt, chip], dab.at[mt, chip], ACT, r_a.at[dz], {"tp": across(o)})

    def dense_down(dz):
        chip = lax.rem(z + Z - dz, Z)
        pair = pl.ds(2 * chip, 2)
        arrive(dab.at[0:T - 1, 0], r_a.at[dz])
        acts = dab[:, chip].astype(F32).reshape(2 * S, U).astype(BF)
        fs[pair] = dot(acts, dd[...]).astype(BF).reshape(2, S, DS)

    def expert_part(picked, q, first, last):
        rows_q = pl.ds(pl.multiple_of(q * DS, DS), DS)
        for n in range(FFL // tile):
            at = slice(n * tile, (n + 1) * tile)
            g = dot(picked, eg[rows_q, at])
            u = dot(picked, eu[rows_q, at])
            if not first:
                g = g + gacc[:, at]
                u = u + uacc[:, at]
            if last:
                actb[:, at] = (silu(g) * u).astype(BF)
            else:
                gacc[:, at] = g
                uacc[:, at] = u

    tile = tile_of(FFL)
    for c in loads[6:8]:
        c.wait()
    arrive(hbuf.at[mt, twin], r_h.at[1])
    dense_part(0)
    for i in range(1, Z):
        relay(i)
        if i > 1:
            passed(i - 1)
            dense_part(in_order(i - 1))
    passed(Z - 1)
    dense_part(in_order(Z - 1))
    for c in loads[8:10]:
        c.wait()
    own = dot(sel[...], hbuf[mt].reshape(E * S, DS)).astype(BF)
    dense_act(0)
    expert_part(own, mt, True, T == 1)
    for n, o in enumerate(by_reach):
        q = across(o)
        arrive(cr.at[q, 0:E - 1], r_c.at[shifts.index(o)])
        picked = cr[q].astype(F32).reshape(N, DS).astype(BF)
        expert_part(picked, q, False, n == len(by_reach) - 1)
        if n == 1:
            dense_act(in_order(1))

    loads[11].wait()
    dtile = tile_of(DS)
    for o in by_reach + shifts[:1]:
        to, k = across(o), shifts.index(o)
        for n in range(DS // dtile):
            at = pl.ds(pl.multiple_of(to * DS + n * dtile, dtile), dtile)
            share = dot(actb[...], ed[:, at])
            for s in range(E):
                es[k, s, :, n * dtile:(n + 1) * dtile] = share[s * CAP:(s + 1) * CAP].astype(BF)
        for i in range(1, Z + 1):
            dz = in_order(i) if i < Z else 0
            for dc in range(2):
                owner = chip_at(dz, dc)
                if i == Z and dc == 0 and k == 0:
                    er[0, me] = es[0, me]
                else:
                    launch(
                        es.at[k, owner], er.at[k, me], FAR if k > 0 else NEAR, r_e.at[min(k, 1)],
                        {"ep": owner, "tp": to})
        if o == by_reach[0]:
            dense_act(in_order(2))
    loads[10].wait()
    for i in range(3, Z):
        dense_act(in_order(i))
    dense_down(0)
    answer(DENSE, fs, fr, r_one.at[5], 0, 1)
    fr[me] = fs[me]
    for i in range(1, Z):
        dz = in_order(i)
        dense_down(dz)
        for dc in range(2):
            answer(DENSE, fs, fr, r_one.at[5], Z - dz, dc)
    arrive(er.at[0:T - 1], r_e.at[1])
    arrive(er.at[0, 0:E - 1], r_e.at[0])
    total = er[0].astype(F32)
    for k in range(1, T):
        total = total + er[k].astype(F32)
    outs = total.reshape(N, DS).astype(BF)
    final = rbuf[mt] + dot(mix_hi, outs) + dot(mix_lo, outs)
    arrive(fr.at[0:E - 1], r_one.at[5])
    dense = fr[0].astype(F32)
    for j in range(1, E):
        dense = dense + fr[j].astype(F32)
    out[...] = final + blend * dense
    keeps[0].start()
    leave(xs.at[0:E - 1], NORM)
    leave(rkr.at[0:E - 1], RANK)
    leave(ps.at[0:E - 1], MAPS)
    leave(pg.at[0:E - 1], GATE)
    leave(mr.at[0:T - 1], MIXED)
    leave(mmr.at[0:T - 1], GROUP)
    leave(hbuf.at[0, 0:E - 1], HID)
    leave(cs.at[0:T - 1, 0:E - 1], PICK)
    leave(dps.at[:, 0:T - 1], PART)
    leave(dab.at[0:T - 1], ACT)
    leave(es.at[0:T - 1], FAR)
    leave(es.at[0, 0:E - 1], NEAR)
    leave(fs.at[0:E - 1], DENSE)
    for c in keeps:
        c.wait()


def finish(out, rec, inner, access, out_o, rec_o, inner_o, access_o, sem):
    S = rec.shape[0]
    parts = 4 if S % 4 == 0 else 1
    size = S // parts
    copies = [
        pltpu.make_async_copy(rec.at[i * size:(i + 1) * size], rec_o.at[i * size:(i + 1) * size], sem.at[i])
        for i in range(parts)
    ]
    for i, (a, b) in enumerate([(out, out_o), (inner, inner_o), (access, access_o)]):
        copies.append(pltpu.make_async_copy(a, b, sem.at[parts + i]))
    for c in copies:
        c.start()
    for c in copies:
        c.wait()


def local(
    E, T,
    tokens, mix_gain, gate_weight, inner_weight, write_weight, read_weight, step_weight, step_bias,
    decay_log, skip_scale, inner_taps, access_taps, inner_history, access_history, recurrent,
    head_gain, mixer_out, moe_gain, expert_ids, route_scores, expert_gate, expert_up, expert_down,
    blend_vector, dense_gate, dense_up, dense_down,
):
    S, D = tokens.shape
    C = gate_weight.shape[1]
    DC, DS = D // E, D // T
    U = dense_gate.shape[1]
    FFL = expert_gate.shape[2]
    GS = access_taps.shape[2]
    rows = E * S
    Z = E // 2
    Q = 2 * S // T
    M = 2 * STATE
    PW = M + LANES + C
    CAP = max(1, 2 * TOP * S // E)
    N = E * CAP
    anywhere = pl.BlockSpec(memory_space=pl.ANY)
    hbm = pl.BlockSpec(memory_space=pltpu.HBM)
    V = pltpu.VMEM
    DMA = pltpu.SemaphoreType.DMA
    shapes = (
        jax.ShapeDtypeStruct((S, DS), F32),
        jax.ShapeDtypeStruct((S, C, STATE), F32),
        jax.ShapeDtypeStruct((3, S, C), BF),
        jax.ShapeDtypeStruct((S, 3, 2, GS), BF),
    )
    held = tuple(pltpu.VMEM(x.shape, x.dtype) for x in shapes)
    operands = (
        tokens, mix_gain[None], step_weight.T, step_bias[None], decay_log[None], skip_scale[None],
        inner_taps, access_taps, inner_history.transpose(1, 0, 2), access_history.transpose(0, 2, 1, 3),
        head_gain[None], moe_gain[None], expert_ids.T, route_scores.T, blend_vector.reshape(-1, LANES),
        gate_weight, inner_weight, write_weight, read_weight,
        recurrent.reshape(S, C, STATE), mixer_out,
        expert_gate[0], expert_up[0], expert_down[0], dense_gate, dense_up, dense_down,
    )
    results = pl.pallas_call(
        functools.partial(kernel, E, T, CAP),
        name="decode_step",
        out_shape=held,
        in_specs=[hbm] * 27,
        out_specs=(anywhere,) * 4,
        scratch_shapes=[
            V((S, DS), F32), V((S, C, STATE), F32), V((3, S, C), BF), V((S, 3, 2, GS), BF),
            V((S, D), BF), V((1, D), F32), V((HEADS, DC), BF), V((1, HEADS), F32), V((1, HEADS), F32),
            V((1, HEADS), F32), V((4, C), BF), V((2, 4, STATE), BF), V((3, S, C), BF), V((S, 3, 2, STATE), BF),
            V((1, C), F32), V((1, D), F32), V((TOP, S), jnp.int32), V((TOP, S), F32), V((D // LANES, LANES), BF),
            V((DC, C), BF), V((DC, C), BF), V((DC, STATE), BF), V((DC, STATE), BF),
            V((S, C, STATE), F32), V((C, D), BF),
            V((D, FFL), BF), V((D, FFL), BF), V((FFL, D), BF),
            V((DS, U), BF), V((DS, U), BF), V((U, DS), BF),
            V((E, S, DC), BF), V((E, S, DC), BF), V((S, LANES), BF), V((E, S, LANES), BF), V((E, S, PW), BF), V((E, S, PW), BF),
            V((E, S, C), BF), V((E, S, C), BF), V((S, C, M), BF),
            V((S, D), BF), V((T, S, D), BF), V((S, M), BF), V((T, S, M), BF),
            V((T, S, DS), F32), V((T, E, S, DS), BF),
            V((N, rows), BF), V((T, E, CAP, DS), BF), V((T, E, CAP, DS), BF), V((N, FFL), F32), V((N, FFL), F32), V((N, FFL), BF),
            V((Z, T, 2, Q, U), BF), V((T, Z, 2, Q, U), BF), V((T, Z, Q, U), BF),
            V((T, E, CAP, DS), BF), V((T, E, CAP, DS), BF),
            V((E, S, DS), BF), V((E, S, DS), BF),
            DMA((4,)), DMA((16,)), DMA((12,)), DMA((13,)), DMA((6,)), DMA((Z,)), DMA((E,)), DMA((T,)),
            DMA((Z,)), DMA((Z,)), DMA((2,)),
        ],
        compiler_params=pltpu.CompilerParams(
            collective_id=0, has_side_effects=True, vmem_limit_bytes=40 * 1024 * 1024
        ),
    )(*[pltpu.with_memory_space_constraint(x, pltpu.HBM) for x in operands])
    out, new_recurrent, inner_new, access_new = pl.pallas_call(
        finish,
        name="store_results",
        out_shape=shapes,
        in_specs=[anywhere] * 4,
        out_specs=(hbm,) * 4,
        scratch_shapes=[DMA((8,))],
    )(*[pltpu.with_memory_space_constraint(x, pltpu.VMEM) for x in results])
    return (
        out, new_recurrent.reshape(recurrent.shape), inner_new.transpose(1, 0, 2),
        access_new.transpose(0, 2, 1, 3),
    )


def solution(mesh):
    in_specs = (
        P("ep", None), P(), P("ep", "tp"), P("ep", "tp"), P("ep", None), P("ep", None),
        P("ep", None), P(), P(), P(), P(None, "tp"), P(), P("ep", None, "tp"),
        P("ep", None, None, None), P("ep", "tp", None, None), P("tp"), P("tp", None), P(),
        P("ep", None), P("ep", None), P("ep", None, "tp"), P("ep", None, "tp"),
        P("ep", "tp", None), P(), P("tp", "ep"), P("tp", "ep"), P("ep", "tp"),
    )
    out_specs = (
        P("ep", "tp"), P("ep", "tp", None, None), P("ep", None, "tp"), P("ep", None, None, None),
    )
    body = functools.partial(local, mesh.shape["ep"], mesh.shape["tp"])
    return jax.shard_map(body, mesh=mesh, in_specs=in_specs, out_specs=out_specs, check_vma=False)
```

```python
import functools
import math

import jax
import jax.numpy as jnp
from jax import lax
from jax.experimental import pallas as pl
from jax.experimental.pallas import tpu as pltpu
from jax.sharding import PartitionSpec as P

HEADS = 16
HEAD_DIM = 64
GROUPS = 4
STATE = 128
LANES = 128
TOP = 2
EPS = 1e-06
BF = jnp.bfloat16
F32 = jnp.float32


def dot(a, b):
    return jnp.dot(a, b, preferred_element_type=F32)


def silu(x):
    return x * (1.0 / (1.0 + jnp.exp(-x)))


def tile_of(extent):
    return 256 if extent % 256 == 0 else extent


def kernel(
    E, T, CAP,
    tokens_h, mix_gain_h, step_weight_h, step_bias_h, decay_log_h, skip_scale_h, inner_taps_h, access_taps_h,
    inner_past_h, access_past_h, head_gain_h, moe_gain_h, ids_h, scores_h, blend_vector_h,
    gate_w, inner_w, write_w, read_w, recurrent, mixer_w, eg_w, eu_w, ed_w, dg_w, du_w, dd_w,
    out_k, nrec_k, inner_k, access_k,
    out, nrec, inner_new, access_new,
    tokens, mix_gain, step_weight, step_bias, decay_log, skip_scale, inner_taps, access_taps,
    inner_past, access_past, head_gain, moe_gain, ids, scores, blend_vector,
    gw, iw, ww, rw, rec, mw, eg, eu, ed, dg, du, dd,
    xs, xr, rk, rkr, ps, pr, pg, pgr, rcat, ms, mr, mm, mmr, sc, scr, scales, hbuf, sel, cs, cr, gacc, uacc, actb, dps, dpr, dab, es, er, fs, fr,
    keep_sem, small_sem, load_sem, sent, r_one, r_n, r_h, r_c, r_d, r_a, r_e,
):
    me = lax.axis_index("ep")
    mt = lax.axis_index("tp")
    S, D = tokens.shape
    C = gw.shape[1]
    DC = D // E
    DS = D // T
    U = dg.shape[1]
    FFL = eg.shape[1]
    N = E * CAP
    M = 2 * STATE
    group = mt * (HEADS // T) // (HEADS // GROUPS)

    cols = pl.ds(pl.multiple_of(group * STATE, STATE), STATE)
    small = [
        (tokens_h, tokens), (mix_gain_h, mix_gain), (ids_h, ids), (step_weight_h, step_weight),
        (scores_h, scores), (step_bias_h, step_bias), (decay_log_h, decay_log), (skip_scale_h, skip_scale),
        (inner_taps_h, inner_taps), (access_taps_h.at[:, :, cols], access_taps), (inner_past_h, inner_past),
        (access_past_h.at[:, :, :, cols], access_past), (head_gain_h, head_gain), (moe_gain_h, moe_gain),
        (blend_vector_h, blend_vector), (access_past_h.at[:, 1:3], access_new.at[:, 0:2]),
    ]
    smalls = [pltpu.make_async_copy(a, b, small_sem.at[i]) for i, (a, b) in enumerate(small)]
    pairs = [
        (gate_w, gw), (inner_w, iw), (write_w.at[:, cols], ww), (read_w.at[:, cols], rw),
        (recurrent, rec), (mixer_w, mw), (dg_w, dg), (du_w, du), (eg_w, eg), (eu_w, eu),
        (dd_w, dd), (ed_w, ed),
    ]
    loads = [pltpu.make_async_copy(a, b, load_sem.at[i]) for i, (a, b) in enumerate(pairs)]
    for c in smalls[:3]:
        c.start()
    barrier = pltpu.get_barrier_semaphore()
    for k in range(1, E):
        pl.semaphore_signal(barrier, inc=1, device_id={"ep": lax.rem(me + k, E)},
                            device_id_type=pl.DeviceIdType.MESH)
    for k in range(1, T):
        pl.semaphore_signal(barrier, inc=1, device_id={"tp": lax.rem(mt + k, T)},
                            device_id_type=pl.DeviceIdType.MESH)

    for c in smalls[3:] + loads[:4]:
        c.start()

    Z = E // 2
    z, core = me // 2, lax.rem(me, 2)
    high = 2 * z // Z
    X = math.isqrt(T) if math.isqrt(T) ** 2 == T else T
    ty, tx = mt // X, lax.rem(mt, X)
    shifts = [(dy, dx) for dy in range(T // X) for dx in range(X)]
    by_reach = sorted(shifts[1:], key=lambda o: -(o[0] > 0) - (o[1] > 0))

    def across(o, sign=1):
        return lax.rem(ty + sign * o[0] + T // X, T // X) * X + lax.rem(tx + sign * o[1] + X, X)

    def in_order(i):
        return (1 - high) * (Z - i) + high * i

    def chip_at(dz, dc):
        return lax.rem(z + dz, Z) * 2 + lax.rem(core + dc, 2)

    keeps = [
        pltpu.make_async_copy(a, b, keep_sem.at[i])
        for i, (a, b) in enumerate([(out, out_k), (nrec, nrec_k), (inner_new, inner_k), (access_new, access_k)])
    ]
    NORM, RANK, MAPS, GATE, MIXED, GROUP, HID, PICK, PART, ACT, FAR, NEAR, DENSE, REST, SCALE = range(15)

    def copy(src, dst, kind, recv, device):
        return pltpu.make_async_remote_copy(
            src_ref=src, dst_ref=dst, send_sem=sent.at[kind], recv_sem=recv,
            device_id=device, device_id_type=pl.DeviceIdType.MESH)

    def launch(*args):
        copy(*args).start()

    def arrive(ref, recv):
        copy(ref, ref, NORM, recv, {"ep": chip_at(0, 1)}).wait_recv()

    def leave(ref, kind):
        copy(ref, ref, kind, r_one.at[0], {"ep": chip_at(0, 1)}).wait_send()

    def ep_send(kind, src_of, dst, recv):
        for i in range(1, Z):
            dz = in_order(i)
            for dc in range(2):
                to = chip_at(dz, dc)
                launch(src_of(to), dst, kind, recv(dz), {"ep": to})
        to = chip_at(0, 1)
        launch(src_of(to), dst, kind, recv(0), {"ep": to})

    def tp_send(kind, src, dst, recv):
        for o in by_reach:
            launch(src, dst, kind, recv, {"tp": across(o)})

    lane = lax.broadcasted_iota(jnp.int32, (S, LANES), 1)
    lane_f = lane.astype(F32)
    row_i = lax.broadcasted_iota(jnp.int32, (S, S), 0)
    col_i = lax.broadcasted_iota(jnp.int32, (S, S), 1)
    diagonal = row_i == col_i
    earlier = jnp.where(col_i < row_i, 1.0, 0.0)

    def column(row):
        return jnp.sum(jnp.where(diagonal, row, 0.0), axis=-1, keepdims=True)

    for c in smalls[:3]:
        c.wait()
    tok = tokens[...].astype(F32)
    scale = lax.rsqrt(jnp.mean(tok * tok, axis=-1, keepdims=True) + EPS)
    normed = (tok * scale * mix_gain[...]).astype(BF)
    for j in range(E):
        xs[j] = normed[:, j * DC:(j + 1) * DC]
    xr[me] = xs[me]
    pl.semaphore_wait(barrier, (E - 1) + (T - 1))
    ep_send(NORM, lambda to: xs.at[to], xr.at[me], lambda dz: r_n.at[dz])
    names = ids[...].astype(F32)
    name_a, name_b = column(names[0:1]), column(names[1:2])
    named = jnp.where((lane_f == name_a) | (lane_f == name_b), 1.0, 0.0)
    before = dot(earlier, named)
    rank = jnp.where(named > 0.0, before, -1.0)
    rk[...] = rank.astype(BF)
    rkr[me] = rk[...]
    ep_send(RANK, lambda to: rk, rkr.at[me], lambda dz: r_one.at[0])
    for c in loads[4:6]:
        c.start()

    for c in smalls[3:15]:
        c.wait()
    ranks = scores[...]
    first = 1.0 / (1.0 + jnp.exp(column(ranks[1:2]) - column(ranks[0:1])))
    combine = jnp.where(lane_f == name_a, first, 0.0) + jnp.where(lane_f == name_b, 1.0 - first, 0.0)
    slot = lax.broadcasted_iota(jnp.int32, (S, N), 1)
    slot_rank = lax.rem(slot, CAP).astype(F32)
    mix = jnp.zeros((S, N), F32)
    hits = jnp.zeros((S, N), F32)
    for e in range(E):
        hit = (slot // CAP == e) & (slot_rank == rank[:, e:e + 1])
        mix = jnp.where(hit, combine[:, e:e + 1], mix)
        hits = jnp.where(hit, 1.0, hits)
    mix_hi = mix.astype(BF)
    mix_lo = (mix - mix_hi.astype(F32)).astype(BF)

    picker = jnp.transpose(hits).astype(BF)

    taps_k = access_taps[...].astype(F32)
    tap_rows = [jnp.concatenate([taps_k[0, k:k + 1], taps_k[1, k:k + 1]], axis=0) for k in range(4)]
    row_of = lax.broadcasted_iota(jnp.int32, (S, STATE), 0)
    past_w = jnp.zeros((S, STATE), F32)
    past_r = jnp.zeros((S, STATE), F32)
    for s in range(S):
        total = access_past[s, 0].astype(F32) * tap_rows[0]
        for k in range(1, 3):
            total = total + access_past[s, k].astype(F32) * tap_rows[k]
        past_w = jnp.where(row_of == s, total[0:1], past_w)
        past_r = jnp.where(row_of == s, total[1:2], past_r)

    for c in loads[:4]:
        c.wait()
    G = M + LANES

    def project(dz):
        chip = lax.rem(z + Z - dz, Z)
        pair = pl.ds(2 * chip, 2)
        rows = xr[pair].reshape(2 * S, DC)
        step_p = lax.dot_general(
            rows, step_weight[...], (((1,), (1,)), ((), ())), preferred_element_type=F32)
        step_hi = step_p.astype(BF)
        step_lo = (step_p - step_hi.astype(F32)).astype(BF)
        ps[pair, :, 0:STATE] = dot(rows, ww[...]).astype(BF).reshape(2, S, STATE)
        ps[pair, :, STATE:M] = dot(rows, rw[...]).astype(BF).reshape(2, S, STATE)
        ps[pair, :, M:G] = jnp.concatenate(
            [step_hi, step_lo, jnp.zeros((2 * S, LANES - 2 * HEADS), BF)], axis=1).reshape(2, S, LANES)
        ps[pair, :, G:G + C] = dot(rows, iw[...]).astype(BF).reshape(2, S, C)
        pg[pair] = dot(rows, gw[...]).astype(BF).reshape(2, S, C)

    def answer(kind, src, dst, recv, back, dc):
        to = chip_at(back, dc)
        launch(src.at[to], dst.at[me], kind, recv, {"ep": to})

    arrive(xr.at[0], r_n.at[0])
    project(0)
    answer(MAPS, ps, pr, r_one.at[1], 0, 1)
    answer(GATE, pg, pgr, r_one.at[2], 0, 1)
    pr[me] = ps[me]
    pgr[me] = pg[me]
    for i in range(1, Z):
        dz = in_order(i)
        arrive(xr.at[0:2], r_n.at[dz])
        project(dz)
        for dc in range(2):
            answer(MAPS, ps, pr, r_one.at[1], Z - dz, dc)
        for dc in range(2):
            answer(GATE, pg, pgr, r_one.at[2], Z - dz, dc)
    for c in loads[6:]:
        c.start()
    arrive(rkr.at[0:E - 1], r_one.at[0])

    every = rkr[...].reshape(E * S, LANES).astype(F32)
    expert_lane = lax.broadcasted_iota(jnp.int32, (E * S, LANES), 1)
    rank_of = jnp.sum(jnp.where(expert_lane == me, every, 0.0), axis=-1, keepdims=True)
    wide = lax.broadcasted_iota(jnp.int32, (E * S, N), 1)
    seq = lax.broadcasted_iota(jnp.int32, (E * S, N), 0)
    chosen = (wide // CAP == seq // S) & (lax.rem(wide, CAP).astype(F32) == rank_of)
    sel[...] = jnp.transpose(jnp.where(chosen, 1.0, 0.0)).astype(BF)

    chan = lax.broadcasted_iota(jnp.int32, (S, C), 1)
    head_of = mt * (HEADS // T) + chan // HEAD_DIM

    def expand(values):
        total = jnp.zeros((S, C), F32)
        for h in range(HEADS):
            total = jnp.where(head_of == h, values[:, h:h + 1], total)
        return total

    skip = expand(skip_scale[...])
    taps = inner_taps[...].astype(F32)
    past = inner_past[0].astype(F32) * taps[0:1]
    for k in range(1, 3):
        past = past + inner_past[k].astype(F32) * taps[k:k + 1]
        inner_new[k - 1] = inner_past[k]
    rate = jnp.exp(decay_log[...])
    loads[4].wait()

    @pl.loop(0, S)
    def _(t):
        value = rec[t]
        high = value.astype(BF)
        rcat[t, :, 0:STATE] = high
        rcat[t, :, STATE:M] = (value - high.astype(F32)).astype(BF)

    arrive(pr.at[0:E - 1], r_one.at[1])
    proj = pr[0].astype(F32)
    for j in range(1, E):
        proj = proj + pr[j].astype(F32)
    maps = proj[:, 0:M].astype(BF)
    step_raw = proj[:, M:M + HEADS] + proj[:, M + HEADS:M + 2 * HEADS]
    inner_part = proj[:, G:G + C].astype(BF)
    inner_new[2] = inner_part
    inner = silu(past + inner_part.astype(F32) * taps[3:4])
    mm[...] = maps
    maps_f = maps.astype(F32)
    write_c = silu(past_w + maps_f[:, 0:STATE] * tap_rows[3][0:1])
    read_c = silu(past_r + maps_f[:, STATE:M] * tap_rows[3][1:2])
    read_hi = read_c.astype(BF).astype(F32)
    read_lo = read_c - read_hi
    reader = jnp.concatenate([
        jnp.concatenate([read_hi, read_hi], axis=1),
        jnp.concatenate([read_lo, jnp.zeros((S, STATE), F32)], axis=1)], axis=0).astype(BF)
    step_x = step_raw + step_bias[...]
    step = jnp.maximum(step_x, 0.0) + jnp.log1p(jnp.exp(-jnp.abs(step_x)))
    decay = expand(jnp.exp(-step * rate))
    push = expand(step) * inner
    both = jnp.sum(write_c * read_c, axis=-1, keepdims=True)
    seq_row = lax.rem(lax.broadcasted_iota(jnp.int32, (2 * S, C), 0), S)
    recalls = jnp.zeros((2 * S, C), F32)
    for t in range(S):
        every = lax.dot_general(reader, rcat[t], (((1,), (1,)), ((), ())), preferred_element_type=F32)
        recalls = jnp.where(seq_row == t, every, recalls)
    recalled = recalls[0:S] + recalls[S:2 * S]
    readout = decay * recalled + push * both + skip * inner
    arrive(pgr.at[0:E - 1], r_one.at[2])
    gate_sum = pgr[0].astype(F32)
    for j in range(1, E):
        gate_sum = gate_sum + pgr[j].astype(F32)
    gated = readout * silu(gate_sum.astype(BF).astype(F32))
    square = gated * gated
    norm = jnp.zeros((S, C), F32)
    for h in range(C // HEAD_DIM):
        here = chan // HEAD_DIM == h
        mean = jnp.sum(jnp.where(here, square, 0.0), axis=-1, keepdims=True) / HEAD_DIM
        norm = jnp.where(here, lax.rsqrt(mean + EPS), norm)
    head_out = (gated * norm * head_gain[...]).astype(BF)
    loads[5].wait()
    for j in range(T):
        ms[j] = dot(head_out, mw[:, j * DS:(j + 1) * DS]).astype(BF)
    for o in by_reach:
        to = across(o)
        launch(ms.at[to], mr.at[mt, to], MIXED, r_one.at[3], {"tp": to})
    for o in by_reach:
        for other in shifts:
            if other != o:
                q = across(other)
                launch(ms.at[q], mr.at[mt, q], REST, r_one.at[6], {"tp": across(o)})
    mr[mt] = ms[...]
    mmr[mt] = mm[...]
    tp_send(GROUP, mm, mmr.at[mt], r_one.at[4])

    decay_t = jnp.transpose(decay)
    push_t = jnp.transpose(push)
    for t in range(S):
        nrec[t] = decay_t[:, t:t + 1] * rec[t] + push_t[:, t:t + 1] * write_c[t:t + 1]
    keeps[1].start()
    keeps[2].start()

    arrive(mr.at[0:T - 1, 0], r_one.at[3])
    mine = pl.ds(pl.multiple_of(mt * DS, DS), DS)

    def total_of(q):
        mixed = mr[0, q].astype(F32)
        for j in range(1, T):
            mixed = mixed + mr[j, q].astype(F32)
        return mixed.astype(BF).astype(F32)

    resid_own = tokens[:, mine].astype(F32) + total_of(mt)
    hbuf[mt, me] = (resid_own * moe_gain[:, mine]).astype(BF)
    twin = chip_at(0, 1)
    for i in range(1, Z):
        dz = in_order(i)
        launch(hbuf.at[mt, me], hbuf.at[mt, me], HID, r_h.at[2 * dz], {"ep": chip_at(dz, 0)})
    launch(hbuf.at[mt, me], hbuf.at[mt, me], HID, r_h.at[1], {"ep": twin})

    arrive(mr.at[0:T - 1, 0:T - 1], r_one.at[6])
    resid = tok + jnp.concatenate([total_of(q) for q in range(T)], axis=1)
    scale = lax.rsqrt(jnp.mean(resid * resid, axis=-1, keepdims=True) + EPS)
    hidden = (resid * scale * moe_gain[...]).astype(BF)
    scale_hi = scale.astype(BF).astype(F32)
    sc[...] = jnp.where(lane < LANES // 2, scale_hi, scale - scale_hi).astype(BF)
    scr[me] = sc[...]
    ep_send(SCALE, lambda to: sc, scr.at[me], lambda dz: r_one.at[7])
    for q in range(T):
        chosen_q = dot(picker, hidden[:, q * DS:(q + 1) * DS])
        for e in range(E):
            cs[q, e] = chosen_q[e * CAP:(e + 1) * CAP].astype(BF)
    for o in by_reach:
        q, n = across(o), shifts.index(o)
        cr[q, me] = cs[q, me]
        for i in range(1, Z + 1):
            dz = in_order(i) if i < Z else 0
            for dc in range(2):
                if i < Z or dc > 0:
                    to = chip_at(dz, dc)
                    launch(cs.at[q, to], cr.at[q, me], PICK, r_c.at[n], {"ep": to})

    scorer = blend_vector[...].astype(F32)
    blend = jnp.zeros((S, LANES), F32)
    for j in range(D // LANES):
        blend = blend + hidden[:, j * LANES:(j + 1) * LANES].astype(F32) * scorer[j:j + 1]
    blend = jnp.sum(blend, axis=-1, keepdims=True)
    blend = 1.0 / (1.0 + jnp.exp(-blend))

    arrive(mmr.at[0:T - 1], r_one.at[4])
    smalls[15].wait()
    owners = [mmr[g * max(1, T // GROUPS)].astype(F32) for g in range(GROUPS)]
    for s in range(S):
        for g in range(GROUPS):
            pair = jnp.concatenate([owners[g][s:s + 1, 0:STATE], owners[g][s:s + 1, STATE:M]], axis=0)
            access_new[s, 2, :, g * STATE:(g + 1) * STATE] = pair.astype(BF)
    keeps[3].start()

    def relay(i):
        dz = in_order(i)
        block = hbuf.at[mt, chip_at(Z - dz, 0)]
        arrive(block, r_h.at[2 * dz])
        launch(block, block, HID, r_h.at[2 * dz + 1], {"ep": twin})

    def passed(i):
        dz = in_order(i)
        arrive(hbuf.at[mt, chip_at(Z - dz, 1)], r_h.at[2 * dz + 1])

    Q = 2 * S // T

    def dense_part(dz):
        chip = lax.rem(z + Z - dz, Z)
        here = hbuf[mt, pl.ds(2 * chip, 2)].reshape(2 * S, DS)
        for w, weight in enumerate((dg, du)):
            part = dot(here, weight[...])
            for m in range(T):
                dps[chip, m, w] = part[m * Q:(m + 1) * Q].astype(BF)
        for o in by_reach:
            to = across(o)
            launch(dps.at[chip, to], dpr.at[mt, chip], PART, r_d.at[dz], {"tp": to})
        dpr[mt, chip] = dps[chip, mt]

    def dense_act(dz):
        chip = lax.rem(z + Z - dz, Z)
        arrive(dpr.at[0:T - 1, 0], r_d.at[dz])
        dsum = dpr[0, chip].astype(F32)
        for j in range(1, T):
            dsum = dsum + dpr[j, chip].astype(F32)
        by = scales[chip, mt][:, 0:1]
        dab[mt, chip] = (silu(dsum[0] * by) * (dsum[1] * by)).astype(BF)
        for o in by_reach:
            launch(dab.at[mt, chip], dab.at[mt, chip], ACT, r_a.at[dz], {"tp": across(o)})

    def dense_down(dz):
        chip = lax.rem(z + Z - dz, Z)
        pair = pl.ds(2 * chip, 2)
        arrive(dab.at[0:T - 1, 0], r_a.at[dz])
        acts = dab[:, chip].astype(F32).reshape(2 * S, U).astype(BF)
        fs[pair] = dot(acts, dd[...]).astype(BF).reshape(2, S, DS)

    def expert_part(picked, q, first, last, factor=None):
        rows_q = pl.ds(pl.multiple_of(q * DS, DS), DS)
        for n in range(FFL // tile):
            at = slice(n * tile, (n + 1) * tile)
            g = dot(picked, eg[rows_q, at])
            u = dot(picked, eu[rows_q, at])
            if factor is not None:
                g, u = g * factor, u * factor
            if not first:
                g = g + gacc[:, at]
                u = u + uacc[:, at]
            if last:
                actb[:, at] = (silu(g) * u).astype(BF)
            else:
                gacc[:, at] = g
                uacc[:, at] = u

    tile = tile_of(FFL)
    for c in loads[6:8]:
        c.wait()
    arrive(hbuf.at[mt, twin], r_h.at[1])
    dense_part(0)
    for i in range(1, Z):
        relay(i)
        if i > 1:
            passed(i - 1)
            dense_part(in_order(i - 1))
    passed(Z - 1)
    dense_part(in_order(Z - 1))
    for c in loads[8:10]:
        c.wait()
    own = dot(sel[...], hbuf[mt].reshape(E * S, DS)).astype(BF)
    arrive(scr.at[0:E - 1], r_one.at[7])
    halves = scr[...].reshape(E * S, LANES)
    picked_scale = jnp.sum(dot(sel[...], halves), axis=-1, keepdims=True) * (2.0 / LANES)
    every_scale = jnp.sum(halves.astype(F32), axis=-1, keepdims=True) * (2.0 / LANES)
    scales[...] = jnp.broadcast_to(every_scale, (E * S, LANES)).reshape(Z, T, Q, LANES)
    dense_act(0)
    expert_part(own, mt, True, T == 1, picked_scale)
    for n, o in enumerate(by_reach):
        q = across(o)
        arrive(cr.at[q, 0:E - 1], r_c.at[shifts.index(o)])
        picked = cr[q].astype(F32).reshape(N, DS).astype(BF)
        expert_part(picked, q, False, n == len(by_reach) - 1)
        if n == 1:
            dense_act(in_order(1))

    loads[11].wait()
    dtile = tile_of(DS)
    for o in by_reach + shifts[:1]:
        to, k = across(o), shifts.index(o)
        for n in range(DS // dtile):
            at = pl.ds(pl.multiple_of(to * DS + n * dtile, dtile), dtile)
            share = dot(actb[...], ed[:, at])
            for s in range(E):
                es[k, s, :, n * dtile:(n + 1) * dtile] = share[s * CAP:(s + 1) * CAP].astype(BF)
        for i in range(1, Z + 1):
            dz = in_order(i) if i < Z else 0
            for dc in range(2):
                owner = chip_at(dz, dc)
                if i == Z and dc == 0 and k == 0:
                    er[0, me] = es[0, me]
                else:
                    launch(
                        es.at[k, owner], er.at[k, me], FAR if k > 0 else NEAR, r_e.at[min(k, 1)],
                        {"ep": owner, "tp": to})
        if o == by_reach[0]:
            dense_act(in_order(2))
        if o == by_reach[2]:
            dense_act(in_order(3))
    loads[10].wait()
    for i in range(4, Z):
        dense_act(in_order(i))
    dense_down(0)
    answer(DENSE, fs, fr, r_one.at[5], 0, 1)
    fr[me] = fs[me]
    for i in range(1, Z):
        dz = in_order(i)
        dense_down(dz)
        for dc in range(2):
            answer(DENSE, fs, fr, r_one.at[5], Z - dz, dc)
    arrive(er.at[0:T - 1], r_e.at[1])
    arrive(er.at[0, 0:E - 1], r_e.at[0])
    total = er[0].astype(F32)
    for k in range(1, T):
        total = total + er[k].astype(F32)
    outs = total.reshape(N, DS).astype(BF)
    final = resid_own + dot(mix_hi, outs) + dot(mix_lo, outs)
    arrive(fr.at[0:E - 1], r_one.at[5])
    dense = fr[0].astype(F32)
    for j in range(1, E):
        dense = dense + fr[j].astype(F32)
    out[...] = final + blend * dense
    keeps[0].start()
    leave(xs.at[0:E - 1], NORM)
    leave(rkr.at[0:E - 1], RANK)
    leave(ps.at[0:E - 1], MAPS)
    leave(pg.at[0:E - 1], GATE)
    leave(mr.at[0:T - 1, 0], MIXED)
    leave(mr.at[0:T - 1, 0:T - 1], REST)
    leave(scr.at[0:E - 1], SCALE)
    leave(mmr.at[0:T - 1], GROUP)
    leave(hbuf.at[0, 0:E - 1], HID)
    leave(cs.at[0:T - 1, 0:E - 1], PICK)
    leave(dps.at[:, 0:T - 1], PART)
    leave(dab.at[0:T - 1], ACT)
    leave(es.at[0:T - 1], FAR)
    leave(es.at[0, 0:E - 1], NEAR)
    leave(fs.at[0:E - 1], DENSE)
    for c in keeps:
        c.wait()


def finish(out, rec, inner, access, out_o, rec_o, inner_o, access_o, sem):
    S = rec.shape[0]
    parts = 4 if S % 4 == 0 else 1
    size = S // parts
    copies = [
        pltpu.make_async_copy(rec.at[i * size:(i + 1) * size], rec_o.at[i * size:(i + 1) * size], sem.at[i])
        for i in range(parts)
    ]
    for i, (a, b) in enumerate([(out, out_o), (inner, inner_o), (access, access_o)]):
        copies.append(pltpu.make_async_copy(a, b, sem.at[parts + i]))
    for c in copies:
        c.start()
    for c in copies:
        c.wait()


def local(
    E, T,
    tokens, mix_gain, gate_weight, inner_weight, write_weight, read_weight, step_weight, step_bias,
    decay_log, skip_scale, inner_taps, access_taps, inner_history, access_history, recurrent,
    head_gain, mixer_out, moe_gain, expert_ids, route_scores, expert_gate, expert_up, expert_down,
    blend_vector, dense_gate, dense_up, dense_down,
):
    S, D = tokens.shape
    C = gate_weight.shape[1]
    DC, DS = D // E, D // T
    U = dense_gate.shape[1]
    FFL = expert_gate.shape[2]
    GS = access_taps.shape[2]
    rows = E * S
    Z = E // 2
    Q = 2 * S // T
    M = 2 * STATE
    PW = M + LANES + C
    CAP = max(1, 2 * TOP * S // E)
    N = E * CAP
    anywhere = pl.BlockSpec(memory_space=pl.ANY)
    hbm = pl.BlockSpec(memory_space=pltpu.HBM)
    V = pltpu.VMEM
    DMA = pltpu.SemaphoreType.DMA
    shapes = (
        jax.ShapeDtypeStruct((S, DS), F32),
        jax.ShapeDtypeStruct((S, C, STATE), F32),
        jax.ShapeDtypeStruct((3, S, C), BF),
        jax.ShapeDtypeStruct((S, 3, 2, GS), BF),
    )
    held = tuple(pltpu.VMEM(x.shape, x.dtype) for x in shapes)
    operands = (
        tokens, mix_gain[None], step_weight.T, step_bias[None], decay_log[None], skip_scale[None],
        inner_taps, access_taps, inner_history.transpose(1, 0, 2), access_history.transpose(0, 2, 1, 3),
        head_gain[None], moe_gain[None], expert_ids.T, route_scores.T, blend_vector.reshape(-1, LANES),
        gate_weight, inner_weight, write_weight, read_weight,
        recurrent.reshape(S, C, STATE), mixer_out,
        expert_gate[0], expert_up[0], expert_down[0], dense_gate, dense_up, dense_down,
    )
    results = pl.pallas_call(
        functools.partial(kernel, E, T, CAP),
        name="decode_step",
        out_shape=held,
        in_specs=[hbm] * 27,
        out_specs=(anywhere,) * 4,
        scratch_shapes=[
            V((S, DS), F32), V((S, C, STATE), F32), V((3, S, C), BF), V((S, 3, 2, GS), BF),
            V((S, D), BF), V((1, D), F32), V((HEADS, DC), BF), V((1, HEADS), F32), V((1, HEADS), F32),
            V((1, HEADS), F32), V((4, C), BF), V((2, 4, STATE), BF), V((3, S, C), BF), V((S, 3, 2, STATE), BF),
            V((1, C), F32), V((1, D), F32), V((TOP, S), jnp.int32), V((TOP, S), F32), V((D // LANES, LANES), BF),
            V((DC, C), BF), V((DC, C), BF), V((DC, STATE), BF), V((DC, STATE), BF),
            V((S, C, STATE), F32), V((C, D), BF),
            V((D, FFL), BF), V((D, FFL), BF), V((FFL, D), BF),
            V((DS, U), BF), V((DS, U), BF), V((U, DS), BF),
            V((E, S, DC), BF), V((E, S, DC), BF), V((S, LANES), BF), V((E, S, LANES), BF), V((E, S, PW), BF), V((E, S, PW), BF),
            V((E, S, C), BF), V((E, S, C), BF), V((S, C, M), BF),
            V((T, S, DS), BF), V((T, T, S, DS), BF), V((S, M), BF), V((T, S, M), BF),
            V((S, LANES), BF), V((E, S, LANES), BF), V((Z, T, Q, LANES), F32), V((T, E, S, DS), BF),
            V((N, rows), BF), V((T, E, CAP, DS), BF), V((T, E, CAP, DS), BF), V((N, FFL), F32), V((N, FFL), F32), V((N, FFL), BF),
            V((Z, T, 2, Q, U), BF), V((T, Z, 2, Q, U), BF), V((T, Z, Q, U), BF),
            V((T, E, CAP, DS), BF), V((T, E, CAP, DS), BF),
            V((E, S, DS), BF), V((E, S, DS), BF),
            DMA((4,)), DMA((16,)), DMA((12,)), DMA((15,)), DMA((8,)), DMA((Z,)), DMA((E,)), DMA((T,)),
            DMA((Z,)), DMA((Z,)), DMA((2,)),
        ],
        compiler_params=pltpu.CompilerParams(
            collective_id=0, has_side_effects=True, vmem_limit_bytes=40 * 1024 * 1024
        ),
    )(*[pltpu.with_memory_space_constraint(x, pltpu.HBM) for x in operands])
    out, new_recurrent, inner_new, access_new = pl.pallas_call(
        finish,
        name="store_results",
        out_shape=shapes,
        in_specs=[anywhere] * 4,
        out_specs=(hbm,) * 4,
        scratch_shapes=[DMA((8,))],
    )(*[pltpu.with_memory_space_constraint(x, pltpu.VMEM) for x in results])
    return (
        out, new_recurrent.reshape(recurrent.shape), inner_new.transpose(1, 0, 2),
        access_new.transpose(0, 2, 1, 3),
    )


def solution(mesh):
    in_specs = (
        P("ep", None), P(), P("ep", "tp"), P("ep", "tp"), P("ep", None), P("ep", None),
        P("ep", None), P(), P(), P(), P(None, "tp"), P(), P("ep", None, "tp"),
        P("ep", None, None, None), P("ep", "tp", None, None), P("tp"), P("tp", None), P(),
        P("ep", None), P("ep", None), P("ep", None, "tp"), P("ep", None, "tp"),
        P("ep", "tp", None), P(), P("tp", "ep"), P("tp", "ep"), P("ep", "tp"),
    )
    out_specs = (
        P("ep", "tp"), P("ep", "tp", None, None), P("ep", None, "tp"), P("ep", None, None, None),
    )
    body = functools.partial(local, mesh.shape["ep"], mesh.shape["tp"])
    return jax.shard_map(body, mesh=mesh, in_specs=in_specs, out_specs=out_specs, check_vma=False)
```

```python
import functools
import math

import jax
import jax.numpy as jnp
from jax import lax
from jax.experimental import pallas as pl
from jax.experimental.pallas import tpu as pltpu
from jax.sharding import PartitionSpec as P

HEADS = 16
HEAD_DIM = 64
GROUPS = 4
STATE = 128
LANES = 128
TOP = 2
EPS = 1e-06
BF = jnp.bfloat16
F32 = jnp.float32


def dot(a, b):
    return jnp.dot(a, b, preferred_element_type=F32)


def silu(x):
    return x * (1.0 / (1.0 + jnp.exp(-x)))


def tile_of(extent):
    return 256 if extent % 256 == 0 else extent


def kernel(
    E, T, CAP,
    tokens_h, mix_gain_h, step_weight_h, step_bias_h, decay_log_h, skip_scale_h, inner_taps_h, access_taps_h,
    inner_past_h, access_past_h, head_gain_h, moe_gain_h, ids_h, scores_h, blend_vector_h,
    gate_w, inner_w, write_w, read_w, recurrent, mixer_w, eg_w, eu_w, ed_w, dg_w, du_w, dd_w,
    out_k, nrec_k, inner_k, access_k,
    out, nrec, inner_new, access_new,
    tokens, mix_gain, step_weight, step_bias, decay_log, skip_scale, inner_taps, access_taps,
    inner_past, access_past, head_gain, moe_gain, ids, scores, blend_vector,
    gw, iw, ww, rw, rec, mw, eg, eu, ed, dg, du, dd,
    xs, xr, rk, rkr, ps, pr, pg, pgr, rcat, ms, mr, mm, mmr, sc, scr, scales, hbuf, sel, cs, cr, gacc, uacc, actb, dps, dpr, dab, es, er, fs, fr,
    keep_sem, small_sem, load_sem, sent, r_one, r_n, r_m, r_h, r_c, r_d, r_a, r_e,
):
    me = lax.axis_index("ep")
    mt = lax.axis_index("tp")
    S, D = tokens.shape
    C = gw.shape[1]
    DC = D // E
    DS = D // T
    U = dg.shape[1]
    FFL = eg.shape[1]
    N = E * CAP
    M = 2 * STATE
    group = mt * (HEADS // T) // (HEADS // GROUPS)

    cols = pl.ds(pl.multiple_of(group * STATE, STATE), STATE)
    small = [
        (tokens_h, tokens), (mix_gain_h, mix_gain), (ids_h, ids), (step_weight_h, step_weight),
        (scores_h, scores), (step_bias_h, step_bias), (decay_log_h, decay_log), (skip_scale_h, skip_scale),
        (inner_taps_h, inner_taps), (access_taps_h.at[:, :, cols], access_taps), (inner_past_h, inner_past),
        (access_past_h.at[:, :, :, cols], access_past), (head_gain_h, head_gain), (moe_gain_h, moe_gain),
        (blend_vector_h, blend_vector), (access_past_h.at[:, 1:3], access_new.at[:, 0:2]),
    ]
    smalls = [pltpu.make_async_copy(a, b, small_sem.at[i]) for i, (a, b) in enumerate(small)]
    pairs = [
        (gate_w, gw), (inner_w, iw), (write_w.at[:, cols], ww), (read_w.at[:, cols], rw),
        (recurrent, rec), (mixer_w, mw), (dg_w, dg), (du_w, du), (eg_w, eg), (eu_w, eu),
        (dd_w, dd), (ed_w, ed),
    ]
    loads = [pltpu.make_async_copy(a, b, load_sem.at[i]) for i, (a, b) in enumerate(pairs)]
    for c in smalls[:3]:
        c.start()
    barrier = pltpu.get_barrier_semaphore()
    for k in range(1, E):
        pl.semaphore_signal(barrier, inc=1, device_id={"ep": lax.rem(me + k, E)},
                            device_id_type=pl.DeviceIdType.MESH)
    for k in range(1, T):
        pl.semaphore_signal(barrier, inc=1, device_id={"tp": lax.rem(mt + k, T)},
                            device_id_type=pl.DeviceIdType.MESH)

    for c in smalls[3:] + loads[:4]:
        c.start()

    Z = E // 2
    z, core = me // 2, lax.rem(me, 2)
    high = 2 * z // Z
    X = math.isqrt(T) if math.isqrt(T) ** 2 == T else T
    ty, tx = mt // X, lax.rem(mt, X)
    shifts = [(dy, dx) for dy in range(T // X) for dx in range(X)]
    by_reach = sorted(shifts[1:], key=lambda o: -(o[0] > 0) - (o[1] > 0))

    def across(o, sign=1):
        return lax.rem(ty + sign * o[0] + T // X, T // X) * X + lax.rem(tx + sign * o[1] + X, X)

    def in_order(i):
        return (1 - high) * (Z - i) + high * i

    def chip_at(dz, dc):
        return lax.rem(z + dz, Z) * 2 + lax.rem(core + dc, 2)

    keeps = [
        pltpu.make_async_copy(a, b, keep_sem.at[i])
        for i, (a, b) in enumerate([(out, out_k), (nrec, nrec_k), (inner_new, inner_k), (access_new, access_k)])
    ]
    NORM, RANK, MAPS, GATE, MIXED, GROUP, HID, PICK, PART, ACT, FAR, NEAR, DENSE, REST, SCALE = range(15)

    def copy(src, dst, kind, recv, device):
        return pltpu.make_async_remote_copy(
            src_ref=src, dst_ref=dst, send_sem=sent.at[kind], recv_sem=recv,
            device_id=device, device_id_type=pl.DeviceIdType.MESH)

    def launch(*args):
        copy(*args).start()

    def arrive(ref, recv):
        copy(ref, ref, NORM, recv, {"ep": chip_at(0, 1)}).wait_recv()

    def leave(ref, kind):
        copy(ref, ref, kind, r_one.at[0], {"ep": chip_at(0, 1)}).wait_send()

    def ep_send(kind, src_of, dst, recv):
        for i in range(1, Z):
            dz = in_order(i)
            for dc in range(2):
                to = chip_at(dz, dc)
                launch(src_of(to), dst, kind, recv(dz), {"ep": to})
        to = chip_at(0, 1)
        launch(src_of(to), dst, kind, recv(0), {"ep": to})

    def tp_send(kind, src, dst, recv):
        for o in by_reach:
            launch(src, dst, kind, recv, {"tp": across(o)})

    lane = lax.broadcasted_iota(jnp.int32, (S, LANES), 1)
    lane_f = lane.astype(F32)
    row_i = lax.broadcasted_iota(jnp.int32, (S, S), 0)
    col_i = lax.broadcasted_iota(jnp.int32, (S, S), 1)
    diagonal = row_i == col_i
    earlier = jnp.where(col_i < row_i, 1.0, 0.0)

    def column(row):
        return jnp.sum(jnp.where(diagonal, row, 0.0), axis=-1, keepdims=True)

    for c in smalls[:3]:
        c.wait()
    tok = tokens[...].astype(F32)
    scale = lax.rsqrt(jnp.mean(tok * tok, axis=-1, keepdims=True) + EPS)
    normed = (tok * scale * mix_gain[...]).astype(BF)
    for j in range(E):
        xs[j] = normed[:, j * DC:(j + 1) * DC]
    xr[me] = xs[me]
    pl.semaphore_wait(barrier, (E - 1) + (T - 1))
    ep_send(NORM, lambda to: xs.at[to], xr.at[me], lambda dz: r_n.at[dz])
    names = ids[...].astype(F32)
    name_a, name_b = column(names[0:1]), column(names[1:2])
    named = jnp.where((lane_f == name_a) | (lane_f == name_b), 1.0, 0.0)
    before = dot(earlier, named)
    rank = jnp.where(named > 0.0, before, -1.0)
    rk[...] = rank.astype(BF)
    rkr[me] = rk[...]
    ep_send(RANK, lambda to: rk, rkr.at[me], lambda dz: r_one.at[0])
    for c in loads[4:6]:
        c.start()

    for c in smalls[3:15]:
        c.wait()
    ranks = scores[...]
    first = 1.0 / (1.0 + jnp.exp(column(ranks[1:2]) - column(ranks[0:1])))
    combine = jnp.where(lane_f == name_a, first, 0.0) + jnp.where(lane_f == name_b, 1.0 - first, 0.0)
    slot = lax.broadcasted_iota(jnp.int32, (S, N), 1)
    slot_rank = lax.rem(slot, CAP).astype(F32)
    mix = jnp.zeros((S, N), F32)
    hits = jnp.zeros((S, N), F32)
    for e in range(E):
        hit = (slot // CAP == e) & (slot_rank == rank[:, e:e + 1])
        mix = jnp.where(hit, combine[:, e:e + 1], mix)
        hits = jnp.where(hit, 1.0, hits)
    mix_hi = mix.astype(BF)
    mix_lo = (mix - mix_hi.astype(F32)).astype(BF)

    picker = jnp.transpose(hits).astype(BF)

    taps_k = access_taps[...].astype(F32)
    tap_rows = [jnp.concatenate([taps_k[0, k:k + 1], taps_k[1, k:k + 1]], axis=0) for k in range(4)]
    row_of = lax.broadcasted_iota(jnp.int32, (S, STATE), 0)
    past_w = jnp.zeros((S, STATE), F32)
    past_r = jnp.zeros((S, STATE), F32)
    for s in range(S):
        total = access_past[s, 0].astype(F32) * tap_rows[0]
        for k in range(1, 3):
            total = total + access_past[s, k].astype(F32) * tap_rows[k]
        past_w = jnp.where(row_of == s, total[0:1], past_w)
        past_r = jnp.where(row_of == s, total[1:2], past_r)

    for c in loads[:4]:
        c.wait()
    G = M + LANES

    def project(dz):
        chip = lax.rem(z + Z - dz, Z)
        pair = pl.ds(2 * chip, 2)
        rows = xr[pair].reshape(2 * S, DC)
        step_p = lax.dot_general(
            rows, step_weight[...], (((1,), (1,)), ((), ())), preferred_element_type=F32)
        step_hi = step_p.astype(BF)
        step_lo = (step_p - step_hi.astype(F32)).astype(BF)
        ps[pair, :, 0:STATE] = dot(rows, ww[...]).astype(BF).reshape(2, S, STATE)
        ps[pair, :, STATE:M] = dot(rows, rw[...]).astype(BF).reshape(2, S, STATE)
        ps[pair, :, M:G] = jnp.concatenate(
            [step_hi, step_lo, jnp.zeros((2 * S, LANES - 2 * HEADS), BF)], axis=1).reshape(2, S, LANES)
        ps[pair, :, G:G + C] = dot(rows, iw[...]).astype(BF).reshape(2, S, C)
        return pair, rows

    def project_gate(pair, rows):
        pg[pair] = dot(rows, gw[...]).astype(BF).reshape(2, S, C)

    def answer(kind, src, dst, recv, back, dc):
        to = chip_at(back, dc)
        launch(src.at[to], dst.at[me], kind, recv, {"ep": to})

    arrive(xr.at[0], r_n.at[0])
    work = project(0)
    answer(MAPS, ps, pr, r_m.at[0], 0, 1)
    project_gate(*work)
    answer(GATE, pg, pgr, r_one.at[2], 0, 1)
    pr[me] = ps[me]
    pgr[me] = pg[me]
    for i in range(1, Z):
        dz = in_order(i)
        arrive(xr.at[0:2], r_n.at[dz])
        work = project(dz)
        for dc in range(2):
            answer(MAPS, ps, pr, r_m.at[Z - dz], Z - dz, dc)
        project_gate(*work)
        for dc in range(2):
            answer(GATE, pg, pgr, r_one.at[2], Z - dz, dc)
    for c in loads[6:]:
        c.start()
    arrive(rkr.at[0:E - 1], r_one.at[0])

    every = rkr[...].reshape(E * S, LANES).astype(F32)
    expert_lane = lax.broadcasted_iota(jnp.int32, (E * S, LANES), 1)
    rank_of = jnp.sum(jnp.where(expert_lane == me, every, 0.0), axis=-1, keepdims=True)
    wide = lax.broadcasted_iota(jnp.int32, (E * S, N), 1)
    seq = lax.broadcasted_iota(jnp.int32, (E * S, N), 0)
    chosen = (wide // CAP == seq // S) & (lax.rem(wide, CAP).astype(F32) == rank_of)
    sel[...] = jnp.transpose(jnp.where(chosen, 1.0, 0.0)).astype(BF)

    chan = lax.broadcasted_iota(jnp.int32, (S, C), 1)
    head_of = mt * (HEADS // T) + chan // HEAD_DIM

    def expand(values):
        total = jnp.zeros((S, C), F32)
        for h in range(HEADS):
            total = jnp.where(head_of == h, values[:, h:h + 1], total)
        return total

    skip = expand(skip_scale[...])
    taps = inner_taps[...].astype(F32)
    past = inner_past[0].astype(F32) * taps[0:1]
    for k in range(1, 3):
        past = past + inner_past[k].astype(F32) * taps[k:k + 1]
        inner_new[k - 1] = inner_past[k]
    rate = jnp.exp(decay_log[...])
    loads[4].wait()

    @pl.loop(0, S)
    def _(t):
        value = rec[t]
        rcat[t] = value.astype(BF)

    arrive(pr.at[0], r_m.at[0])
    proj = pr[me].astype(F32) + pr[chip_at(0, 1)].astype(F32)
    for i in range(1, Z):
        dz = in_order(i)
        arrive(pr.at[0:2], r_m.at[dz])
        proj = proj + pr[chip_at(Z - dz, 0)].astype(F32)
        proj = proj + pr[chip_at(Z - dz, 1)].astype(F32)
    maps = proj[:, 0:M].astype(BF)
    step_raw = proj[:, M:M + HEADS] + proj[:, M + HEADS:M + 2 * HEADS]
    inner_part = proj[:, G:G + C].astype(BF)
    inner_new[2] = inner_part
    inner = silu(past + inner_part.astype(F32) * taps[3:4])
    mm[...] = maps
    maps_f = maps.astype(F32)
    write_c = silu(past_w + maps_f[:, 0:STATE] * tap_rows[3][0:1])
    read_c = silu(past_r + maps_f[:, STATE:M] * tap_rows[3][1:2])
    read_hi = read_c.astype(BF).astype(F32)
    read_lo = read_c - read_hi
    reader = jnp.concatenate([read_hi, read_lo], axis=0).astype(BF)
    step_x = step_raw + step_bias[...]
    step = jnp.maximum(step_x, 0.0) + jnp.log1p(jnp.exp(-jnp.abs(step_x)))
    decay = expand(jnp.exp(-step * rate))
    push = expand(step) * inner
    both = jnp.sum(write_c * read_c, axis=-1, keepdims=True)
    seq_row = lax.rem(lax.broadcasted_iota(jnp.int32, (2 * S, C), 0), S)
    recalls = jnp.zeros((2 * S, C), F32)
    for t in range(S):
        every = lax.dot_general(reader, rcat[t], (((1,), (1,)), ((), ())), preferred_element_type=F32)
        recalls = jnp.where(seq_row == t, every, recalls)
    recalled = recalls[0:S] + recalls[S:2 * S]
    readout = decay * recalled + push * both + skip * inner
    arrive(pgr.at[0:E - 1], r_one.at[2])
    gate_sum = pgr[0].astype(F32)
    for j in range(1, E):
        gate_sum = gate_sum + pgr[j].astype(F32)
    gated = readout * silu(gate_sum.astype(BF).astype(F32))
    square = gated * gated
    norm = jnp.zeros((S, C), F32)
    for h in range(C // HEAD_DIM):
        here = chan // HEAD_DIM == h
        mean = jnp.sum(jnp.where(here, square, 0.0), axis=-1, keepdims=True) / HEAD_DIM
        norm = jnp.where(here, lax.rsqrt(mean + EPS), norm)
    head_out = (gated * norm * head_gain[...]).astype(BF)
    loads[5].wait()
    for o in by_reach + shifts[:1]:
        to = across(o)
        wide_to = pl.ds(pl.multiple_of(to * DS, DS), DS)
        ms[to] = dot(head_out, mw[:, wide_to]).astype(BF)
        if o != shifts[0]:
            launch(ms.at[to], mr.at[mt, to], MIXED, r_one.at[3], {"tp": to})
    for o in by_reach:
        for other in shifts:
            if other != o:
                q = across(other)
                launch(ms.at[q], mr.at[mt, q], REST, r_one.at[6], {"tp": across(o)})
    mr[mt] = ms[...]
    mmr[mt] = mm[...]
    tp_send(GROUP, mm, mmr.at[mt], r_one.at[4])

    decay_t = jnp.transpose(decay)
    push_t = jnp.transpose(push)
    for t in range(S):
        nrec[t] = decay_t[:, t:t + 1] * rec[t] + push_t[:, t:t + 1] * write_c[t:t + 1]
    keeps[1].start()
    keeps[2].start()

    arrive(mr.at[0:T - 1, 0], r_one.at[3])
    mine = pl.ds(pl.multiple_of(mt * DS, DS), DS)

    def total_of(q):
        mixed = mr[0, q].astype(F32)
        for j in range(1, T):
            mixed = mixed + mr[j, q].astype(F32)
        return mixed.astype(BF).astype(F32)

    resid_own = tokens[:, mine].astype(F32) + total_of(mt)
    hbuf[mt, me] = (resid_own * moe_gain[:, mine]).astype(BF)
    twin = chip_at(0, 1)
    for i in range(1, Z):
        dz = in_order(i)
        launch(hbuf.at[mt, me], hbuf.at[mt, me], HID, r_h.at[2 * dz], {"ep": chip_at(dz, 0)})
    launch(hbuf.at[mt, me], hbuf.at[mt, me], HID, r_h.at[1], {"ep": twin})

    Q = 2 * S // T

    def dense_part(dz):
        chip = lax.rem(z + Z - dz, Z)
        here = hbuf[mt, pl.ds(2 * chip, 2)].reshape(2 * S, DS)
        for w, weight in enumerate((dg, du)):
            part = dot(here, weight[...])
            for m in range(T):
                dps[chip, m, w] = part[m * Q:(m + 1) * Q].astype(BF)
        for o in by_reach:
            to = across(o)
            launch(dps.at[chip, to], dpr.at[mt, chip], PART, r_d.at[dz], {"tp": to})
        dpr[mt, chip] = dps[chip, mt]

    for c in loads[6:8]:
        c.wait()
    arrive(hbuf.at[mt, twin], r_h.at[1])
    dense_part(0)
    arrive(mr.at[0:T - 1, 0:T - 1], r_one.at[6])
    resid = tok + jnp.concatenate([total_of(q) for q in range(T)], axis=1)
    scale = lax.rsqrt(jnp.mean(resid * resid, axis=-1, keepdims=True) + EPS)
    hidden = (resid * scale * moe_gain[...]).astype(BF)
    scale_hi = scale.astype(BF).astype(F32)
    sc[...] = jnp.where(lane < LANES // 2, scale_hi, scale - scale_hi).astype(BF)
    scr[me] = sc[...]
    ep_send(SCALE, lambda to: sc, scr.at[me], lambda dz: r_one.at[7])
    for q in range(T):
        chosen_q = dot(picker, hidden[:, q * DS:(q + 1) * DS])
        for e in range(E):
            cs[q, e] = chosen_q[e * CAP:(e + 1) * CAP].astype(BF)
    for o in by_reach:
        q, n = across(o), shifts.index(o)
        cr[q, me] = cs[q, me]
        for i in range(1, Z + 1):
            dz = in_order(i) if i < Z else 0
            for dc in range(2):
                if i < Z or dc > 0:
                    to = chip_at(dz, dc)
                    launch(cs.at[q, to], cr.at[q, me], PICK, r_c.at[n], {"ep": to})

    def relay(i):
        dz = in_order(i)
        block = hbuf.at[mt, chip_at(Z - dz, 0)]
        arrive(block, r_h.at[2 * dz])
        launch(block, block, HID, r_h.at[2 * dz + 1], {"ep": twin})

    def passed(i):
        dz = in_order(i)
        arrive(hbuf.at[mt, chip_at(Z - dz, 1)], r_h.at[2 * dz + 1])

    def dense_act(dz):
        chip = lax.rem(z + Z - dz, Z)
        arrive(dpr.at[0:T - 1, 0], r_d.at[dz])
        dsum = dpr[0, chip].astype(F32)
        for j in range(1, T):
            dsum = dsum + dpr[j, chip].astype(F32)
        by = scales[chip, mt][:, 0:1]
        dab[mt, chip] = (silu(dsum[0] * by) * (dsum[1] * by)).astype(BF)
        for o in by_reach:
            launch(dab.at[mt, chip], dab.at[mt, chip], ACT, r_a.at[dz], {"tp": across(o)})

    def dense_down(dz):
        chip = lax.rem(z + Z - dz, Z)
        pair = pl.ds(2 * chip, 2)
        arrive(dab.at[0:T - 1, 0], r_a.at[dz])
        acts = dab[:, chip].astype(F32).reshape(2 * S, U).astype(BF)
        fs[pair] = dot(acts, dd[...]).astype(BF).reshape(2, S, DS)

    def expert_part(picked, q, first, last, factor=None):
        rows_q = pl.ds(pl.multiple_of(q * DS, DS), DS)
        for n in range(FFL // tile):
            at = slice(n * tile, (n + 1) * tile)
            g = dot(picked, eg[rows_q, at])
            u = dot(picked, eu[rows_q, at])
            if factor is not None:
                g, u = g * factor, u * factor
            if not first:
                g = g + gacc[:, at]
                u = u + uacc[:, at]
            if last:
                actb[:, at] = (silu(g) * u).astype(BF)
            else:
                gacc[:, at] = g
                uacc[:, at] = u

    tile = tile_of(FFL)
    for i in range(1, Z):
        relay(i)
        if i > 1:
            passed(i - 1)
            dense_part(in_order(i - 1))
    passed(Z - 1)
    dense_part(in_order(Z - 1))
    for c in loads[8:10]:
        c.wait()
    own = dot(sel[...], hbuf[mt].reshape(E * S, DS)).astype(BF)
    arrive(scr.at[0:E - 1], r_one.at[7])
    halves = scr[...].reshape(E * S, LANES)
    picked_scale = jnp.sum(dot(sel[...], halves), axis=-1, keepdims=True) * (2.0 / LANES)
    every_scale = jnp.sum(halves.astype(F32), axis=-1, keepdims=True) * (2.0 / LANES)
    scales[...] = jnp.broadcast_to(every_scale, (E * S, LANES)).reshape(Z, T, Q, LANES)
    dense_act(0)
    expert_part(own, mt, True, T == 1, picked_scale)
    for n, o in enumerate(by_reach):
        q = across(o)
        arrive(cr.at[q, 0:E - 1], r_c.at[shifts.index(o)])
        picked = cr[q].astype(F32).reshape(N, DS).astype(BF)
        expert_part(picked, q, False, n == len(by_reach) - 1)
        if n == 1:
            dense_act(in_order(1))

    loads[11].wait()
    dtile = tile_of(DS)
    for n_o, o in enumerate(by_reach + shifts[:1]):
        to, k = across(o), shifts.index(o)
        for n in range(DS // dtile):
            at = pl.ds(pl.multiple_of(to * DS + n * dtile, dtile), dtile)
            share = dot(actb[...], ed[:, at])
            for s in range(E):
                es[k, s, :, n * dtile:(n + 1) * dtile] = share[s * CAP:(s + 1) * CAP].astype(BF)
        for i in range(1, Z + 1):
            dz = in_order(i) if i < Z else 0
            for dc in range(2):
                owner = chip_at(dz, dc)
                if i == Z and dc == 0 and k == 0:
                    er[0, me] = es[0, me]
                else:
                    launch(
                        es.at[k, owner], er.at[k, me], FAR if k > 0 else NEAR, r_e.at[min(k, 1)],
                        {"ep": owner, "tp": to})
        if n_o == 0:
            dense_act(in_order(2))
        if n_o == 2:
            dense_act(in_order(3))
    loads[10].wait()
    for i in range(4, Z):
        dense_act(in_order(i))
    scorer = blend_vector[...].astype(F32)
    blend = jnp.zeros((S, LANES), F32)
    for j in range(D // LANES):
        blend = blend + hidden[:, j * LANES:(j + 1) * LANES].astype(F32) * scorer[j:j + 1]
    blend = jnp.sum(blend, axis=-1, keepdims=True)
    blend = 1.0 / (1.0 + jnp.exp(-blend))

    arrive(mmr.at[0:T - 1], r_one.at[4])
    smalls[15].wait()
    owners = [mmr[g * max(1, T // GROUPS)].astype(F32) for g in range(GROUPS)]
    for s in range(S):
        for g in range(GROUPS):
            pair = jnp.concatenate([owners[g][s:s + 1, 0:STATE], owners[g][s:s + 1, STATE:M]], axis=0)
            access_new[s, 2, :, g * STATE:(g + 1) * STATE] = pair.astype(BF)
    keeps[3].start()

    dense_down(0)
    answer(DENSE, fs, fr, r_one.at[5], 0, 1)
    fr[me] = fs[me]
    for i in range(1, Z):
        dz = in_order(i)
        dense_down(dz)
        for dc in range(2):
            answer(DENSE, fs, fr, r_one.at[5], Z - dz, dc)
    arrive(er.at[0:T - 1], r_e.at[1])
    arrive(er.at[0, 0:E - 1], r_e.at[0])
    total = er[0].astype(F32)
    for k in range(1, T):
        total = total + er[k].astype(F32)
    outs = total.reshape(N, DS).astype(BF)
    final = resid_own + dot(mix_hi, outs) + dot(mix_lo, outs)
    arrive(fr.at[0:E - 1], r_one.at[5])
    dense = fr[0].astype(F32)
    for j in range(1, E):
        dense = dense + fr[j].astype(F32)
    out[...] = final + blend * dense
    keeps[0].start()
    leave(xs.at[0:E - 1], NORM)
    leave(rkr.at[0:E - 1], RANK)
    leave(ps.at[0:E - 1], MAPS)
    leave(pg.at[0:E - 1], GATE)
    leave(mr.at[0:T - 1, 0], MIXED)
    leave(mr.at[0:T - 1, 0:T - 1], REST)
    leave(scr.at[0:E - 1], SCALE)
    leave(mmr.at[0:T - 1], GROUP)
    leave(hbuf.at[0, 0:E - 1], HID)
    leave(cs.at[0:T - 1, 0:E - 1], PICK)
    leave(dps.at[:, 0:T - 1], PART)
    leave(dab.at[0:T - 1], ACT)
    leave(es.at[0:T - 1], FAR)
    leave(es.at[0, 0:E - 1], NEAR)
    leave(fs.at[0:E - 1], DENSE)
    for c in keeps:
        c.wait()


def finish(out, rec, inner, access, out_o, rec_o, inner_o, access_o, sem):
    S = rec.shape[0]
    parts = 4 if S % 4 == 0 else 1
    size = S // parts
    copies = [
        pltpu.make_async_copy(rec.at[i * size:(i + 1) * size], rec_o.at[i * size:(i + 1) * size], sem.at[i])
        for i in range(parts)
    ]
    for i, (a, b) in enumerate([(out, out_o), (inner, inner_o), (access, access_o)]):
        copies.append(pltpu.make_async_copy(a, b, sem.at[parts + i]))
    for c in copies:
        c.start()
    for c in copies:
        c.wait()


def local(
    E, T,
    tokens, mix_gain, gate_weight, inner_weight, write_weight, read_weight, step_weight, step_bias,
    decay_log, skip_scale, inner_taps, access_taps, inner_history, access_history, recurrent,
    head_gain, mixer_out, moe_gain, expert_ids, route_scores, expert_gate, expert_up, expert_down,
    blend_vector, dense_gate, dense_up, dense_down,
):
    S, D = tokens.shape
    C = gate_weight.shape[1]
    DC, DS = D // E, D // T
    U = dense_gate.shape[1]
    FFL = expert_gate.shape[2]
    GS = access_taps.shape[2]
    rows = E * S
    Z = E // 2
    Q = 2 * S // T
    M = 2 * STATE
    PW = M + LANES + C
    CAP = max(1, 2 * TOP * S // E)
    N = E * CAP
    anywhere = pl.BlockSpec(memory_space=pl.ANY)
    hbm = pl.BlockSpec(memory_space=pltpu.HBM)
    V = pltpu.VMEM
    DMA = pltpu.SemaphoreType.DMA
    shapes = (
        jax.ShapeDtypeStruct((S, DS), F32),
        jax.ShapeDtypeStruct((S, C, STATE), F32),
        jax.ShapeDtypeStruct((3, S, C), BF),
        jax.ShapeDtypeStruct((S, 3, 2, GS), BF),
    )
    held = tuple(pltpu.VMEM(x.shape, x.dtype) for x in shapes)
    operands = (
        tokens, mix_gain[None], step_weight.T, step_bias[None], decay_log[None], skip_scale[None],
        inner_taps, access_taps, inner_history.transpose(1, 0, 2), access_history.transpose(0, 2, 1, 3),
        head_gain[None], moe_gain[None], expert_ids.T, route_scores.T, blend_vector.reshape(-1, LANES),
        gate_weight, inner_weight, write_weight, read_weight,
        recurrent.reshape(S, C, STATE), mixer_out,
        expert_gate[0], expert_up[0], expert_down[0], dense_gate, dense_up, dense_down,
    )
    results = pl.pallas_call(
        functools.partial(kernel, E, T, CAP),
        name="decode_step",
        out_shape=held,
        in_specs=[hbm] * 27,
        out_specs=(anywhere,) * 4,
        scratch_shapes=[
            V((S, DS), F32), V((S, C, STATE), F32), V((3, S, C), BF), V((S, 3, 2, GS), BF),
            V((S, D), BF), V((1, D), F32), V((HEADS, DC), BF), V((1, HEADS), F32), V((1, HEADS), F32),
            V((1, HEADS), F32), V((4, C), BF), V((2, 4, STATE), BF), V((3, S, C), BF), V((S, 3, 2, STATE), BF),
            V((1, C), F32), V((1, D), F32), V((TOP, S), jnp.int32), V((TOP, S), F32), V((D // LANES, LANES), BF),
            V((DC, C), BF), V((DC, C), BF), V((DC, STATE), BF), V((DC, STATE), BF),
            V((S, C, STATE), F32), V((C, D), BF),
            V((D, FFL), BF), V((D, FFL), BF), V((FFL, D), BF),
            V((DS, U), BF), V((DS, U), BF), V((U, DS), BF),
            V((E, S, DC), BF), V((E, S, DC), BF), V((S, LANES), BF), V((E, S, LANES), BF), V((E, S, PW), BF), V((E, S, PW), BF),
            V((E, S, C), BF), V((E, S, C), BF), V((S, C, STATE), BF),
            V((T, S, DS), BF), V((T, T, S, DS), BF), V((S, M), BF), V((T, S, M), BF),
            V((S, LANES), BF), V((E, S, LANES), BF), V((Z, T, Q, LANES), F32), V((T, E, S, DS), BF),
            V((N, rows), BF), V((T, E, CAP, DS), BF), V((T, E, CAP, DS), BF), V((N, FFL), F32), V((N, FFL), F32), V((N, FFL), BF),
            V((Z, T, 2, Q, U), BF), V((T, Z, 2, Q, U), BF), V((T, Z, Q, U), BF),
            V((T, E, CAP, DS), BF), V((T, E, CAP, DS), BF),
            V((E, S, DS), BF), V((E, S, DS), BF),
            DMA((4,)), DMA((16,)), DMA((12,)), DMA((15,)), DMA((8,)), DMA((Z,)), DMA((Z,)), DMA((E,)), DMA((T,)),
            DMA((Z,)), DMA((Z,)), DMA((2,)),
        ],
        compiler_params=pltpu.CompilerParams(
            collective_id=0, has_side_effects=True, vmem_limit_bytes=40 * 1024 * 1024
        ),
    )(*[pltpu.with_memory_space_constraint(x, pltpu.HBM) for x in operands])
    out, new_recurrent, inner_new, access_new = pl.pallas_call(
        finish,
        name="store_results",
        out_shape=shapes,
        in_specs=[anywhere] * 4,
        out_specs=(hbm,) * 4,
        scratch_shapes=[DMA((8,))],
    )(*[pltpu.with_memory_space_constraint(x, pltpu.VMEM) for x in results])
    return (
        out, new_recurrent.reshape(recurrent.shape), inner_new.transpose(1, 0, 2),
        access_new.transpose(0, 2, 1, 3),
    )


def solution(mesh):
    in_specs = (
        P("ep", None), P(), P("ep", "tp"), P("ep", "tp"), P("ep", None), P("ep", None),
        P("ep", None), P(), P(), P(), P(None, "tp"), P(), P("ep", None, "tp"),
        P("ep", None, None, None), P("ep", "tp", None, None), P("tp"), P("tp", None), P(),
        P("ep", None), P("ep", None), P("ep", None, "tp"), P("ep", None, "tp"),
        P("ep", "tp", None), P(), P("tp", "ep"), P("tp", "ep"), P("ep", "tp"),
    )
    out_specs = (
        P("ep", "tp"), P("ep", "tp", None, None), P("ep", None, "tp"), P("ep", None, None, None),
    )
    body = functools.partial(local, mesh.shape["ep"], mesh.shape["tp"])
    return jax.shard_map(body, mesh=mesh, in_specs=in_specs, out_specs=out_specs, check_vma=False)
```

```python
import functools
import math

import jax
import jax.numpy as jnp
from jax import lax
from jax.experimental import pallas as pl
from jax.experimental.pallas import tpu as pltpu
from jax.sharding import PartitionSpec as P

HEADS = 16
HEAD_DIM = 64
GROUPS = 4
STATE = 128
LANES = 128
TOP = 2
EPS = 1e-06
BF = jnp.bfloat16
F32 = jnp.float32


def dot(a, b):
    return jnp.dot(a, b, preferred_element_type=F32)


def silu(x):
    return x * (1.0 / (1.0 + jnp.exp(-x)))


def tile_of(extent):
    return 256 if extent % 256 == 0 else extent


def kernel(
    E, T, CAP,
    tokens_h, mix_gain_h, step_weight_h, step_bias_h, decay_log_h, skip_scale_h, inner_taps_h, access_taps_h,
    inner_past_h, access_past_h, head_gain_h, moe_gain_h, ids_h, scores_h, blend_vector_h,
    gate_w, inner_w, write_w, read_w, recurrent, mixer_w, eg_w, eu_w, ed_w, dg_w, du_w, dd_w,
    out_k, nrec_k, inner_k, access_k,
    out, nrec, inner_new, access_new,
    tokens, mix_gain, step_weight, step_bias, decay_log, skip_scale, inner_taps, access_taps,
    inner_past, access_past, head_gain, moe_gain, ids, scores, blend_vector,
    gw, iw, ww, rw, rec, mw, eg, eu, ed, dg, du, dd,
    xs, xr, rk, rkr, ps, pr, pg, pgr, rcat, ms, mr, mm, mmr, sc, scr, scales, hbuf, sel, cs, cr, gacc, uacc, actb, dps, dpr, dab, es, er, fs, fr,
    keep_sem, small_sem, load_sem, sent, r_one, r_n, r_m, r_h, r_c, r_d, r_a, r_e,
):
    me = lax.axis_index("ep")
    mt = lax.axis_index("tp")
    S, D = tokens.shape
    C = gw.shape[1]
    DC = D // E
    DS = D // T
    U = dg.shape[1]
    FFL = eg.shape[1]
    N = E * CAP
    M = 2 * STATE
    group = mt * (HEADS // T) // (HEADS // GROUPS)

    cols = pl.ds(pl.multiple_of(group * STATE, STATE), STATE)
    small = [
        (tokens_h, tokens), (mix_gain_h, mix_gain), (ids_h, ids), (step_weight_h, step_weight),
        (scores_h, scores), (step_bias_h, step_bias), (decay_log_h, decay_log), (skip_scale_h, skip_scale),
        (inner_taps_h, inner_taps), (access_taps_h.at[:, :, cols], access_taps), (inner_past_h, inner_past),
        (access_past_h.at[:, :, :, cols], access_past), (head_gain_h, head_gain), (moe_gain_h, moe_gain),
        (blend_vector_h, blend_vector), (access_past_h.at[:, 1:3], access_new.at[:, 0:2]),
    ]
    smalls = [pltpu.make_async_copy(a, b, small_sem.at[i]) for i, (a, b) in enumerate(small)]
    pairs = [
        (gate_w, gw), (inner_w, iw), (write_w.at[:, cols], ww), (read_w.at[:, cols], rw),
        (recurrent, rec), (mixer_w, mw), (dg_w, dg), (du_w, du), (eg_w, eg), (eu_w, eu),
        (dd_w, dd), (ed_w, ed),
    ]
    loads = [pltpu.make_async_copy(a, b, load_sem.at[i]) for i, (a, b) in enumerate(pairs)]
    for c in smalls[:3]:
        c.start()
    barrier = pltpu.get_barrier_semaphore()
    for k in range(1, E):
        pl.semaphore_signal(barrier, inc=1, device_id={"ep": lax.rem(me + k, E)},
                            device_id_type=pl.DeviceIdType.MESH)
    for k in range(1, T):
        pl.semaphore_signal(barrier, inc=1, device_id={"tp": lax.rem(mt + k, T)},
                            device_id_type=pl.DeviceIdType.MESH)

    for c in smalls[3:] + loads[:4]:
        c.start()

    Z = E // 2
    z, core = me // 2, lax.rem(me, 2)
    high = 2 * z // Z
    X = math.isqrt(T) if math.isqrt(T) ** 2 == T else T
    ty, tx = mt // X, lax.rem(mt, X)
    shifts = [(dy, dx) for dy in range(T // X) for dx in range(X)]
    by_reach = sorted(shifts[1:], key=lambda o: -(o[0] > 0) - (o[1] > 0))

    def across(o, sign=1):
        return lax.rem(ty + sign * o[0] + T // X, T // X) * X + lax.rem(tx + sign * o[1] + X, X)

    def in_order(i):
        return (1 - high) * (Z - i) + high * i

    def chip_at(dz, dc):
        return lax.rem(z + dz, Z) * 2 + lax.rem(core + dc, 2)

    keeps = [
        pltpu.make_async_copy(a, b, keep_sem.at[i])
        for i, (a, b) in enumerate([(out, out_k), (nrec, nrec_k), (inner_new, inner_k), (access_new, access_k)])
    ]
    NORM, RANK, MAPS, GATE, MIXED, GROUP, HID, PICK, PART, ACT, FAR, SCALE = range(12)
    REST, NEAR, DENSE = MIXED, PICK, HID

    def copy(src, dst, kind, recv, device):
        return pltpu.make_async_remote_copy(
            src_ref=src, dst_ref=dst, send_sem=sent.at[kind], recv_sem=recv,
            device_id=device, device_id_type=pl.DeviceIdType.MESH)

    def launch(*args):
        copy(*args).start()

    def arrive(ref, recv):
        copy(ref, ref, NORM, recv, {"ep": chip_at(0, 1)}).wait_recv()

    def leave(ref, kind):
        copy(ref, ref, kind, r_one.at[0], {"ep": chip_at(0, 1)}).wait_send()

    def ep_send(kind, src_of, dst, recv):
        for i in range(1, Z):
            dz = in_order(i)
            for dc in range(2):
                to = chip_at(dz, dc)
                launch(src_of(to), dst, kind, recv(dz), {"ep": to})
        to = chip_at(0, 1)
        launch(src_of(to), dst, kind, recv(0), {"ep": to})

    def tp_send(kind, src, dst, recv):
        for o in by_reach:
            launch(src, dst, kind, recv, {"tp": across(o)})

    lane = lax.broadcasted_iota(jnp.int32, (S, LANES), 1)
    lane_f = lane.astype(F32)
    row_i = lax.broadcasted_iota(jnp.int32, (S, S), 0)
    col_i = lax.broadcasted_iota(jnp.int32, (S, S), 1)
    diagonal = row_i == col_i
    earlier = jnp.where(col_i < row_i, 1.0, 0.0)

    def column(row):
        return jnp.sum(jnp.where(diagonal, row, 0.0), axis=-1, keepdims=True)

    for c in smalls[:3]:
        c.wait()
    tok = tokens[...].astype(F32)
    scale = lax.rsqrt(jnp.mean(tok * tok, axis=-1, keepdims=True) + EPS)
    normed = (tok * scale * mix_gain[...]).astype(BF)
    for j in range(E):
        xs[j] = normed[:, j * DC:(j + 1) * DC]
    xr[me] = xs[me]
    pl.semaphore_wait(barrier, (E - 1) + (T - 1))
    ep_send(NORM, lambda to: xs.at[to], xr.at[me], lambda dz: r_n.at[dz])
    names = ids[...].astype(F32)
    name_a, name_b = column(names[0:1]), column(names[1:2])
    named = jnp.where((lane_f == name_a) | (lane_f == name_b), 1.0, 0.0)
    before = dot(earlier, named)
    rank = jnp.where(named > 0.0, before, -1.0)
    rk[...] = rank.astype(BF)
    rkr[me] = rk[...]
    ep_send(RANK, lambda to: rk, rkr.at[me], lambda dz: r_one.at[0])
    for c in loads[4:6]:
        c.start()

    for c in smalls[3:15]:
        c.wait()
    ranks = scores[...]
    first = 1.0 / (1.0 + jnp.exp(column(ranks[1:2]) - column(ranks[0:1])))
    combine = jnp.where(lane_f == name_a, first, 0.0) + jnp.where(lane_f == name_b, 1.0 - first, 0.0)
    slot = lax.broadcasted_iota(jnp.int32, (S, N), 1)
    slot_rank = lax.rem(slot, CAP).astype(F32)
    mix = jnp.zeros((S, N), F32)
    hits = jnp.zeros((S, N), F32)
    for e in range(E):
        hit = (slot // CAP == e) & (slot_rank == rank[:, e:e + 1])
        mix = jnp.where(hit, combine[:, e:e + 1], mix)
        hits = jnp.where(hit, 1.0, hits)
    mix_hi = mix.astype(BF)
    mix_lo = (mix - mix_hi.astype(F32)).astype(BF)

    picker = jnp.transpose(hits).astype(BF)

    taps_k = access_taps[...].astype(F32)
    tap_rows = [jnp.concatenate([taps_k[0, k:k + 1], taps_k[1, k:k + 1]], axis=0) for k in range(4)]
    row_of = lax.broadcasted_iota(jnp.int32, (S, STATE), 0)
    past_w = jnp.zeros((S, STATE), F32)
    past_r = jnp.zeros((S, STATE), F32)
    for s in range(S):
        total = access_past[s, 0].astype(F32) * tap_rows[0]
        for k in range(1, 3):
            total = total + access_past[s, k].astype(F32) * tap_rows[k]
        past_w = jnp.where(row_of == s, total[0:1], past_w)
        past_r = jnp.where(row_of == s, total[1:2], past_r)

    for c in loads[:4]:
        c.wait()
    G = M + LANES

    def project(dz):
        chip = lax.rem(z + Z - dz, Z)
        pair = pl.ds(2 * chip, 2)
        rows = xr[pair].reshape(2 * S, DC)
        step_p = lax.dot_general(
            rows, step_weight[...], (((1,), (1,)), ((), ())), preferred_element_type=F32)
        step_hi = step_p.astype(BF)
        step_lo = (step_p - step_hi.astype(F32)).astype(BF)
        ps[pair, :, 0:STATE] = dot(rows, ww[...]).astype(BF).reshape(2, S, STATE)
        ps[pair, :, STATE:M] = dot(rows, rw[...]).astype(BF).reshape(2, S, STATE)
        ps[pair, :, M:G] = jnp.concatenate(
            [step_hi, step_lo, jnp.zeros((2 * S, LANES - 2 * HEADS), BF)], axis=1).reshape(2, S, LANES)
        ps[pair, :, G:G + C] = dot(rows, iw[...]).astype(BF).reshape(2, S, C)
        return pair, rows

    def project_gate(pair, rows):
        pg[pair] = dot(rows, gw[...]).astype(BF).reshape(2, S, C)

    def answer(kind, src, dst, recv, back, dc):
        to = chip_at(back, dc)
        launch(src.at[to], dst.at[me], kind, recv, {"ep": to})

    arrive(xr.at[0], r_n.at[0])
    work = project(0)
    answer(MAPS, ps, pr, r_m.at[0], 0, 1)
    project_gate(*work)
    answer(GATE, pg, pgr, r_one.at[2], 0, 1)
    pr[me] = ps[me]
    pgr[me] = pg[me]
    for i in range(1, Z):
        dz = in_order(i)
        arrive(xr.at[0:2], r_n.at[dz])
        work = project(dz)
        for dc in range(2):
            answer(MAPS, ps, pr, r_m.at[Z - dz], Z - dz, dc)
        project_gate(*work)
        for dc in range(2):
            answer(GATE, pg, pgr, r_one.at[2], Z - dz, dc)
    for c in loads[6:]:
        c.start()
    arrive(rkr.at[0:E - 1], r_one.at[0])

    every = rkr[...].reshape(E * S, LANES).astype(F32)
    expert_lane = lax.broadcasted_iota(jnp.int32, (E * S, LANES), 1)
    rank_of = jnp.sum(jnp.where(expert_lane == me, every, 0.0), axis=-1, keepdims=True)
    wide = lax.broadcasted_iota(jnp.int32, (E * S, N), 1)
    seq = lax.broadcasted_iota(jnp.int32, (E * S, N), 0)
    chosen = (wide // CAP == seq // S) & (lax.rem(wide, CAP).astype(F32) == rank_of)
    sel[...] = jnp.transpose(jnp.where(chosen, 1.0, 0.0)).astype(BF)

    chan = lax.broadcasted_iota(jnp.int32, (S, C), 1)
    head_of = mt * (HEADS // T) + chan // HEAD_DIM

    def expand(values):
        total = jnp.zeros((S, C), F32)
        for h in range(HEADS):
            total = jnp.where(head_of == h, values[:, h:h + 1], total)
        return total

    skip = expand(skip_scale[...])
    taps = inner_taps[...].astype(F32)
    past = inner_past[0].astype(F32) * taps[0:1]
    for k in range(1, 3):
        past = past + inner_past[k].astype(F32) * taps[k:k + 1]
        inner_new[k - 1] = inner_past[k]
    rate = jnp.exp(decay_log[...])
    loads[4].wait()

    @pl.loop(0, S)
    def _(t):
        value = rec[t]
        rcat[t] = value.astype(BF)

    arrive(pr.at[0], r_m.at[0])
    proj = pr[me].astype(F32) + pr[chip_at(0, 1)].astype(F32)
    for i in range(1, Z):
        dz = in_order(i)
        arrive(pr.at[0:2], r_m.at[dz])
        proj = proj + pr[chip_at(Z - dz, 0)].astype(F32)
        proj = proj + pr[chip_at(Z - dz, 1)].astype(F32)
    maps = proj[:, 0:M].astype(BF)
    step_raw = proj[:, M:M + HEADS] + proj[:, M + HEADS:M + 2 * HEADS]
    inner_part = proj[:, G:G + C].astype(BF)
    inner_new[2] = inner_part
    inner = silu(past + inner_part.astype(F32) * taps[3:4])
    mm[...] = maps
    maps_f = maps.astype(F32)
    write_c = silu(past_w + maps_f[:, 0:STATE] * tap_rows[3][0:1])
    read_c = silu(past_r + maps_f[:, STATE:M] * tap_rows[3][1:2])
    read_hi = read_c.astype(BF).astype(F32)
    read_lo = read_c - read_hi
    reader = jnp.concatenate([read_hi, read_lo], axis=0).astype(BF)
    step_x = step_raw + step_bias[...]
    step = jnp.maximum(step_x, 0.0) + jnp.log1p(jnp.exp(-jnp.abs(step_x)))
    decay = expand(jnp.exp(-step * rate))
    push = expand(step) * inner
    both = jnp.sum(write_c * read_c, axis=-1, keepdims=True)
    seq_row = lax.rem(lax.broadcasted_iota(jnp.int32, (2 * S, C), 0), S)
    recalls = jnp.zeros((2 * S, C), F32)
    for t in range(S):
        every = lax.dot_general(reader, rcat[t], (((1,), (1,)), ((), ())), preferred_element_type=F32)
        recalls = jnp.where(seq_row == t, every, recalls)
    recalled = recalls[0:S] + recalls[S:2 * S]
    readout = decay * recalled + push * both + skip * inner
    arrive(pgr.at[0:E - 1], r_one.at[2])
    gate_sum = pgr[0].astype(F32)
    for j in range(1, E):
        gate_sum = gate_sum + pgr[j].astype(F32)
    gated = readout * silu(gate_sum.astype(BF).astype(F32))
    square = gated * gated
    norm = jnp.zeros((S, C), F32)
    for h in range(C // HEAD_DIM):
        here = chan // HEAD_DIM == h
        mean = jnp.sum(jnp.where(here, square, 0.0), axis=-1, keepdims=True) / HEAD_DIM
        norm = jnp.where(here, lax.rsqrt(mean + EPS), norm)
    head_out = (gated * norm * head_gain[...]).astype(BF)
    loads[5].wait()
    for o in by_reach + shifts[:1]:
        to = across(o)
        wide_to = pl.ds(pl.multiple_of(to * DS, DS), DS)
        ms[to] = dot(head_out, mw[:, wide_to]).astype(BF)
        if o != shifts[0]:
            launch(ms.at[to], mr.at[mt, to], MIXED, r_one.at[3], {"tp": to})
    for o in by_reach:
        for other in shifts:
            if other != o:
                q = across(other)
                launch(ms.at[q], mr.at[mt, q], REST, r_one.at[6], {"tp": across(o)})
    mr[mt] = ms[...]
    mmr[mt] = mm[...]
    tp_send(GROUP, mm, mmr.at[mt], r_one.at[4])

    arrive(mr.at[0:T - 1, 0], r_one.at[3])
    mine = pl.ds(pl.multiple_of(mt * DS, DS), DS)

    def total_of(q):
        mixed = mr[0, q].astype(F32)
        for j in range(1, T):
            mixed = mixed + mr[j, q].astype(F32)
        return mixed.astype(BF).astype(F32)

    resid_own = tokens[:, mine].astype(F32) + total_of(mt)
    hbuf[mt, me] = (resid_own * moe_gain[:, mine]).astype(BF)
    twin = chip_at(0, 1)
    for i in range(1, Z):
        dz = in_order(i)
        launch(hbuf.at[mt, me], hbuf.at[mt, me], HID, r_h.at[2 * dz], {"ep": chip_at(dz, 0)})
    launch(hbuf.at[mt, me], hbuf.at[mt, me], HID, r_h.at[1], {"ep": twin})
    decay_t = jnp.transpose(decay)
    push_t = jnp.transpose(push)
    for t in range(S):
        nrec[t] = decay_t[:, t:t + 1] * rec[t] + push_t[:, t:t + 1] * write_c[t:t + 1]
    keeps[1].start()
    keeps[2].start()


    Q = 2 * S // T

    def dense_part(dz):
        chip = lax.rem(z + Z - dz, Z)
        here = hbuf[mt, pl.ds(2 * chip, 2)].reshape(2 * S, DS)
        for w, weight in enumerate((dg, du)):
            part = dot(here, weight[...])
            for m in range(T):
                dps[chip, m, w] = part[m * Q:(m + 1) * Q].astype(BF)
        for o in by_reach:
            to = across(o)
            launch(dps.at[chip, to], dpr.at[mt, chip], PART, r_d.at[dz], {"tp": to})
        dpr[mt, chip] = dps[chip, mt]

    for c in loads[6:8]:
        c.wait()
    arrive(hbuf.at[mt, twin], r_h.at[1])
    dense_part(0)
    arrive(mr.at[0:T - 1, 0:T - 1], r_one.at[6])
    resid = tok + jnp.concatenate([total_of(q) for q in range(T)], axis=1)
    scale = lax.rsqrt(jnp.mean(resid * resid, axis=-1, keepdims=True) + EPS)
    hidden = (resid * scale * moe_gain[...]).astype(BF)
    scale_hi = scale.astype(BF).astype(F32)
    sc[...] = jnp.where(lane < LANES // 2, scale_hi, scale - scale_hi).astype(BF)
    scr[me] = sc[...]
    ep_send(SCALE, lambda to: sc, scr.at[me], lambda dz: r_one.at[7])
    for q in range(T):
        chosen_q = dot(picker, hidden[:, q * DS:(q + 1) * DS])
        for e in range(E):
            cs[q, e] = chosen_q[e * CAP:(e + 1) * CAP].astype(BF)
    for o in by_reach:
        q, n = across(o), shifts.index(o)
        cr[q, me] = cs[q, me]
        for i in range(1, Z + 1):
            dz = in_order(i) if i < Z else 0
            for dc in range(2):
                if i < Z or dc > 0:
                    to = chip_at(dz, dc)
                    launch(cs.at[q, to], cr.at[q, me], PICK, r_c.at[n], {"ep": to})

    def relay(i):
        dz = in_order(i)
        block = hbuf.at[mt, chip_at(Z - dz, 0)]
        arrive(block, r_h.at[2 * dz])
        launch(block, block, HID, r_h.at[2 * dz + 1], {"ep": twin})

    def passed(i):
        dz = in_order(i)
        arrive(hbuf.at[mt, chip_at(Z - dz, 1)], r_h.at[2 * dz + 1])

    def dense_act(dz):
        chip = lax.rem(z + Z - dz, Z)
        arrive(dpr.at[0:T - 1, 0], r_d.at[dz])
        dsum = dpr[0, chip].astype(F32)
        for j in range(1, T):
            dsum = dsum + dpr[j, chip].astype(F32)
        by = scales[chip, mt][:, 0:1]
        dab[mt, chip] = (silu(dsum[0] * by) * (dsum[1] * by)).astype(BF)
        for o in by_reach:
            launch(dab.at[mt, chip], dab.at[mt, chip], ACT, r_a.at[dz], {"tp": across(o)})

    def dense_down(dz):
        chip = lax.rem(z + Z - dz, Z)
        pair = pl.ds(2 * chip, 2)
        arrive(dab.at[0:T - 1, 0], r_a.at[dz])
        acts = dab[:, chip].astype(F32).reshape(2 * S, U).astype(BF)
        fs[pair] = dot(acts, dd[...]).astype(BF).reshape(2, S, DS)

    def expert_part(picked, q, first, last, factor=None):
        rows_q = pl.ds(pl.multiple_of(q * DS, DS), DS)
        for n in range(FFL // tile):
            at = slice(n * tile, (n + 1) * tile)
            g = dot(picked, eg[rows_q, at])
            u = dot(picked, eu[rows_q, at])
            if factor is not None:
                g, u = g * factor, u * factor
            if not first:
                g = g + gacc[:, at]
                u = u + uacc[:, at]
            if last:
                actb[:, at] = (silu(g) * u).astype(BF)
            else:
                gacc[:, at] = g
                uacc[:, at] = u

    tile = tile_of(FFL)
    for i in range(1, Z):
        relay(i)
        if i > 1:
            passed(i - 1)
            dense_part(in_order(i - 1))
    passed(Z - 1)
    dense_part(in_order(Z - 1))
    for c in loads[8:10]:
        c.wait()
    own = dot(sel[...], hbuf[mt].reshape(E * S, DS)).astype(BF)
    arrive(scr.at[0:E - 1], r_one.at[7])
    halves = scr[...].reshape(E * S, LANES)
    picked_scale = jnp.sum(dot(sel[...], halves), axis=-1, keepdims=True) * (2.0 / LANES)
    every_scale = jnp.sum(halves.astype(F32), axis=-1, keepdims=True) * (2.0 / LANES)
    scales[...] = jnp.broadcast_to(every_scale, (E * S, LANES)).reshape(Z, T, Q, LANES)
    dense_act(0)
    expert_part(own, mt, True, T == 1, picked_scale)
    for n, o in enumerate(by_reach):
        q = across(o)
        arrive(cr.at[q, 0:E - 1], r_c.at[shifts.index(o)])
        picked = cr[q].astype(F32).reshape(N, DS).astype(BF)
        expert_part(picked, q, False, n == len(by_reach) - 1)
        if n == 1:
            dense_act(in_order(1))

    loads[11].wait()
    dtile = tile_of(DS)
    for n_o, o in enumerate(by_reach + shifts[:1]):
        to, k = across(o), shifts.index(o)
        for n in range(DS // dtile):
            at = pl.ds(pl.multiple_of(to * DS + n * dtile, dtile), dtile)
            share = dot(actb[...], ed[:, at])
            for s in range(E):
                es[k, s, :, n * dtile:(n + 1) * dtile] = share[s * CAP:(s + 1) * CAP].astype(BF)
        for i in range(1, Z + 1):
            dz = in_order(i) if i < Z else 0
            for dc in range(2):
                owner = chip_at(dz, dc)
                if i == Z and dc == 0 and k == 0:
                    er[0, me] = es[0, me]
                else:
                    launch(
                        es.at[k, owner], er.at[k, me], FAR if k > 0 else NEAR, r_e.at[min(k, 1)],
                        {"ep": owner, "tp": to})
        if n_o == 0:
            dense_act(in_order(2))
        if n_o == 2:
            dense_act(in_order(3))
    loads[10].wait()
    for i in range(4, Z):
        dense_act(in_order(i))
    scorer = blend_vector[...].astype(F32)
    blend = jnp.zeros((S, LANES), F32)
    for j in range(D // LANES):
        blend = blend + hidden[:, j * LANES:(j + 1) * LANES].astype(F32) * scorer[j:j + 1]
    blend = jnp.sum(blend, axis=-1, keepdims=True)
    blend = 1.0 / (1.0 + jnp.exp(-blend))

    arrive(mmr.at[0:T - 1], r_one.at[4])
    smalls[15].wait()
    owners = [mmr[g * max(1, T // GROUPS)].astype(F32) for g in range(GROUPS)]
    for s in range(S):
        for g in range(GROUPS):
            pair = jnp.concatenate([owners[g][s:s + 1, 0:STATE], owners[g][s:s + 1, STATE:M]], axis=0)
            access_new[s, 2, :, g * STATE:(g + 1) * STATE] = pair.astype(BF)
    keeps[3].start()

    dense_down(0)
    answer(DENSE, fs, fr, r_one.at[5], 0, 1)
    fr[me] = fs[me]
    for i in range(1, Z):
        dz = in_order(i)
        dense_down(dz)
        for dc in range(2):
            answer(DENSE, fs, fr, r_one.at[5], Z - dz, dc)
    arrive(er.at[0:T - 1], r_e.at[1])
    arrive(er.at[0, 0:E - 1], r_e.at[0])
    total = er[0].astype(F32)
    for k in range(1, T):
        total = total + er[k].astype(F32)
    outs = total.reshape(N, DS).astype(BF)
    final = resid_own + dot(mix_hi, outs) + dot(mix_lo, outs)
    arrive(fr.at[0:E - 1], r_one.at[5])
    dense = fr[0].astype(F32)
    for j in range(1, E):
        dense = dense + fr[j].astype(F32)
    out[...] = final + blend * dense
    keeps[0].start()
    leave(xs.at[0:E - 1], NORM)
    leave(rkr.at[0:E - 1], RANK)
    leave(ps.at[0:E - 1], MAPS)
    leave(pg.at[0:E - 1], GATE)
    leave(mr.at[0:T - 1, 0:T], MIXED)
    leave(scr.at[0:E - 1], SCALE)
    leave(mmr.at[0:T - 1], GROUP)
    leave(hbuf.at[0:2, 0:E - 1], HID)
    leave(cs.at[0:T, 0:E - 1], PICK)
    leave(dps.at[:, 0:T - 1], PART)
    leave(dab.at[0:T - 1], ACT)
    leave(es.at[0:T - 1], FAR)
    for c in keeps:
        c.wait()


def finish(out, rec, inner, access, out_o, rec_o, inner_o, access_o, sem):
    S = rec.shape[0]
    parts = 4 if S % 4 == 0 else 1
    size = S // parts
    copies = [
        pltpu.make_async_copy(rec.at[i * size:(i + 1) * size], rec_o.at[i * size:(i + 1) * size], sem.at[i])
        for i in range(parts)
    ]
    for i, (a, b) in enumerate([(out, out_o), (inner, inner_o), (access, access_o)]):
        copies.append(pltpu.make_async_copy(a, b, sem.at[parts + i]))
    for c in copies:
        c.start()
    for c in copies:
        c.wait()


def local(
    E, T,
    tokens, mix_gain, gate_weight, inner_weight, write_weight, read_weight, step_weight, step_bias,
    decay_log, skip_scale, inner_taps, access_taps, inner_history, access_history, recurrent,
    head_gain, mixer_out, moe_gain, expert_ids, route_scores, expert_gate, expert_up, expert_down,
    blend_vector, dense_gate, dense_up, dense_down,
):
    S, D = tokens.shape
    C = gate_weight.shape[1]
    DC, DS = D // E, D // T
    U = dense_gate.shape[1]
    FFL = expert_gate.shape[2]
    GS = access_taps.shape[2]
    rows = E * S
    Z = E // 2
    Q = 2 * S // T
    M = 2 * STATE
    PW = M + LANES + C
    CAP = max(1, 2 * TOP * S // E)
    N = E * CAP
    anywhere = pl.BlockSpec(memory_space=pl.ANY)
    hbm = pl.BlockSpec(memory_space=pltpu.HBM)
    V = pltpu.VMEM
    DMA = pltpu.SemaphoreType.DMA
    shapes = (
        jax.ShapeDtypeStruct((S, DS), F32),
        jax.ShapeDtypeStruct((S, C, STATE), F32),
        jax.ShapeDtypeStruct((3, S, C), BF),
        jax.ShapeDtypeStruct((S, 3, 2, GS), BF),
    )
    held = tuple(pltpu.VMEM(x.shape, x.dtype) for x in shapes)
    operands = (
        tokens, mix_gain[None], step_weight.T, step_bias[None], decay_log[None], skip_scale[None],
        inner_taps, access_taps, inner_history.transpose(1, 0, 2), access_history.transpose(0, 2, 1, 3),
        head_gain[None], moe_gain[None], expert_ids.T, route_scores.T, blend_vector.reshape(-1, LANES),
        gate_weight, inner_weight, write_weight, read_weight,
        recurrent.reshape(S, C, STATE), mixer_out,
        expert_gate[0], expert_up[0], expert_down[0], dense_gate, dense_up, dense_down,
    )
    results = pl.pallas_call(
        functools.partial(kernel, E, T, CAP),
        name="decode_step",
        out_shape=held,
        in_specs=[hbm] * 27,
        out_specs=(anywhere,) * 4,
        scratch_shapes=[
            V((S, DS), F32), V((S, C, STATE), F32), V((3, S, C), BF), V((S, 3, 2, GS), BF),
            V((S, D), BF), V((1, D), F32), V((HEADS, DC), BF), V((1, HEADS), F32), V((1, HEADS), F32),
            V((1, HEADS), F32), V((4, C), BF), V((2, 4, STATE), BF), V((3, S, C), BF), V((S, 3, 2, STATE), BF),
            V((1, C), F32), V((1, D), F32), V((TOP, S), jnp.int32), V((TOP, S), F32), V((D // LANES, LANES), BF),
            V((DC, C), BF), V((DC, C), BF), V((DC, STATE), BF), V((DC, STATE), BF),
            V((S, C, STATE), F32), V((C, D), BF),
            V((D, FFL), BF), V((D, FFL), BF), V((FFL, D), BF),
            V((DS, U), BF), V((DS, U), BF), V((U, DS), BF),
            V((E, S, DC), BF), V((E, S, DC), BF), V((S, LANES), BF), V((E, S, LANES), BF), V((E, S, PW), BF), V((E, S, PW), BF),
            V((E, S, C), BF), V((E, S, C), BF), V((S, C, STATE), BF),
            V((T, S, DS), BF), V((T, T, S, DS), BF), V((S, M), BF), V((T, S, M), BF),
            V((S, LANES), BF), V((E, S, LANES), BF), V((Z, T, Q, LANES), F32), V((T, E, S, DS), BF),
            V((N, rows), BF), V((T, E, CAP, DS), BF), V((T, E, CAP, DS), BF), V((N, FFL), F32), V((N, FFL), F32), V((N, FFL), BF),
            V((Z, T, 2, Q, U), BF), V((T, Z, 2, Q, U), BF), V((T, Z, Q, U), BF),
            V((T, E, CAP, DS), BF), V((T, E, CAP, DS), BF),
            V((E, S, DS), BF), V((E, S, DS), BF),
            DMA((4,)), DMA((16,)), DMA((12,)), DMA((12,)), DMA((8,)), DMA((Z,)), DMA((Z,)), DMA((E,)), DMA((T,)),
            DMA((Z,)), DMA((Z,)), DMA((2,)),
        ],
        compiler_params=pltpu.CompilerParams(
            collective_id=0, has_side_effects=True, vmem_limit_bytes=40 * 1024 * 1024
        ),
    )(*[pltpu.with_memory_space_constraint(x, pltpu.HBM) for x in operands])
    out, new_recurrent, inner_new, access_new = pl.pallas_call(
        finish,
        name="store_results",
        out_shape=shapes,
        in_specs=[anywhere] * 4,
        out_specs=(hbm,) * 4,
        scratch_shapes=[DMA((8,))],
    )(*[pltpu.with_memory_space_constraint(x, pltpu.VMEM) for x in results])
    return (
        out, new_recurrent.reshape(recurrent.shape), inner_new.transpose(1, 0, 2),
        access_new.transpose(0, 2, 1, 3),
    )


def solution(mesh):
    in_specs = (
        P("ep", None), P(), P("ep", "tp"), P("ep", "tp"), P("ep", None), P("ep", None),
        P("ep", None), P(), P(), P(), P(None, "tp"), P(), P("ep", None, "tp"),
        P("ep", None, None, None), P("ep", "tp", None, None), P("tp"), P("tp", None), P(),
        P("ep", None), P("ep", None), P("ep", None, "tp"), P("ep", None, "tp"),
        P("ep", "tp", None), P(), P("tp", "ep"), P("tp", "ep"), P("ep", "tp"),
    )
    out_specs = (
        P("ep", "tp"), P("ep", "tp", None, None), P("ep", None, "tp"), P("ep", None, None, None),
    )
    body = functools.partial(local, mesh.shape["ep"], mesh.shape["tp"])
    return jax.shard_map(body, mesh=mesh, in_specs=in_specs, out_specs=out_specs, check_vma=False)
```
